32 devices in a mesh: grp: 2 (over x), ep: 16 (over z, y, core).
Axes of the slice: x: 2, y: 2, z: 4, core: 2. Of those that a mesh axis runs over, the one named last changes fastest.
Arguments:
- hidden: bfloat16 [96, 2048], P(('grp', 'ep')), parts along dimension 0, may hold values from -6 to 6
- conv_window: bfloat16 [96, 3, 6144], P(('grp', 'ep')), parts along dimension 0, may hold values from -6 to 6
- ssm_state: float32 [96, 64, 64, 128], P(('grp', 'ep')), parts along dimension 0, may hold values from -1.75 to 1.75
- gate_proj: bfloat16 [2048, 4096], P(None, 'ep'), may hold values from -0.125 to 0.125
- input_proj: bfloat16 [2048, 4096], P(None, 'ep'), may hold values from -0.125 to 0.125
- write_proj: bfloat16 [2048, 1024], P(None, 'ep'), may hold values from -0.125 to 0.125
- read_proj: bfloat16 [2048, 1024], P(None, 'ep'), may hold values from -0.125 to 0.125
- step_proj: bfloat16 [2048, 64], replicated, may hold values from -0.125 to 0.125
- step_bias: float32 [64], replicated, may hold values from -2 to 1
- decay_log: float32 [64], replicated, may hold values from -2.3 to 1.4
- decay_shift: float32 [96, 64], P(('grp', 'ep')), parts along dimension 0, may hold values from -0.7 to 0
- skip_scale: float32 [64], replicated, may hold values from -4 to 4
- conv_taps: bfloat16 [4, 6144], replicated, may hold values from -3 to 3
- conv_bias: float32 [6144], replicated, may hold values from -3 to 3
- mix_gain: float32 [2048], replicated, may hold values from 0.1 to 1.9
- group_gain: float32 [4096], replicated, may hold values from 0.1 to 1.9
- out_proj: bfloat16 [4096, 2048], P(None, 'ep'), may hold values from -0.09375 to 0.09375
- ffn_gain: float32 [2048], replicated, may hold values from 0.1 to 1.9
- router: bfloat16 [2048, 16], replicated, may hold values from -0.125 to 0.125
- expert_ids: int32 [96, 6], P(('grp', 'ep')), parts along dimension 0, may hold values from 0 to 15, all different within a row; in each aligned block of 3 rows (0 to 2, 3 to 5, ...) at most 2 rows name the same one
- expert_gate: bfloat16 [16, 2048, 512], P('ep'), may hold values from -0.125 to 0.125
- expert_up: bfloat16 [16, 2048, 512], P('ep'), may hold values from -0.125 to 0.125
- expert_down: bfloat16 [16, 512, 2048], P('ep'), may hold values from -0.25 to 0.25
- shared_gate: bfloat16 [2048, 512], P('ep'), may hold values from -0.125 to 0.125
- shared_up: bfloat16 [2048, 512], P('ep'), may hold values from -0.125 to 0.125
- shared_down: bfloat16 [512, 2048], replicated, may hold values from -0.25 to 0.25
Outputs:
- layer_out: bfloat16 [96, 2048], P(('grp', 'ep')), parts along dimension 0
- next_state: float32 [96, 64, 64, 128], P(('grp', 'ep')), parts along dimension 0
- next_window: bfloat16 [96, 3, 6144], P(('grp', 'ep')), parts along dimension 0
The draws below stay inside these ranges and needn't reach their ends.
There are 2 independent parts, one for each index of `grp`. The reference program is written for one: setup_inputs(seed, part) draws one part's arguments, and reference() takes and returns one part's arrays. A program takes and returns all parts, laid end to end along the dimension named above; an argument that names none is the same for every part. Nothing has to cross between parts.
Inputs may be any that keep to these rules, and one draw needn't show every extreme that they name: `expert_ids`: each row names 6 different experts; in the rows of one device no expert is named by more than 2 rows, and in every draw some device's rows name some expert exactly 2 times.
All inputs are finite; a program needn't handle non-finite values.
Results may differ from the reference program's by a relative error of at most 0.019.
Values may be sent and summed in bfloat16 or wider, within the bound.
A program may use at most 128 MiB of HBM per device.

```python
import math
import jax
import jax.numpy as jnp
import numpy as np
from jax import lax

D = 2048
INNER = 4096
HEAD_DIM = 64
GROUPS = 8
STATE = 128
CONV = 4
EFF = 512
SFF = 512
TOP_K = 6
SEQ_DEV = 3
CAP = 2
HEADS = 64
CONV_DIM = 6144
EXPERTS = 16
SEQS = 48


def block_levels(own_key, extent, shards, low, largest):
    loudness, own = 1.0, jax.random.fold_in(own_key, 6)
    for dim, shards_of in shards:
        draws = jnp.exp(jax.random.uniform(jax.random.fold_in(own, dim), (shards_of,), jnp.float32, low / len(shards), largest / len(shards)))
        loudness = loudness * jnp.repeat(draws, extent[dim] // shards_of).reshape([-1 if axis == dim else 1 for axis in range(len(extent))])
    return loudness


def routed_block(rng, own, number, rows, amount, top, limit, slope):
    order = jax.random.permutation(rng, amount)
    packed, ordinary = shares(amount, rows * top, limit, slope, True), shares(amount, rows * top, limit, slope, False)
    places = jnp.arange(amount)

    def named(lengths, offset_by):
        used = int((lengths > 0).sum())
        fixed = max(1, used // 4)
        passed = fixed + (places - fixed + offset_by * (used - fixed)) % max(1, amount - fixed)
        return jnp.zeros((amount,), jnp.int32).at[order[jnp.where(places < fixed, places, passed)]].set(jnp.asarray(lengths, jnp.int32))

    lengths = jnp.where(number % 4 == 0, named(packed, number // 4), named(ordinary, number - number // 4 - 1))
    mixed = jax.random.permutation(jax.random.fold_in(own, 3), amount)
    source_of, sink = mixed[0:amount // 2 * 2:2], mixed[1:amount // 2 * 2:2]
    slack = jnp.minimum(lengths[source_of] - 1, limit - lengths[sink]) // 2
    slack = jnp.where((source_of == order[0]) | (sink == order[0]) | (lengths[sink] == 0), 0, jnp.maximum(slack, 0))
    passed = jax.random.randint(jax.random.fold_in(own, 4), (amount // 2,), 0, 1 << 20) % (slack + 1)
    lengths = lengths.at[source_of].add(-passed).at[sink].add(passed)
    labels = jnp.searchsorted(jnp.cumsum(lengths), jnp.arange(rows * top), side="right").astype(jnp.int32)
    listing = labels.reshape(top, rows).T
    listing = listing[jax.random.permutation(jax.random.fold_in(own, 1), rows)]
    offset_by = jax.random.randint(jax.random.fold_in(own, 2), (rows, 1), 0, top)
    return jnp.take_along_axis(listing, (jnp.arange(top)[None, :] + offset_by) % top, axis=1)


def shares(count, total, most, lean, full):
    portions = [(1 << 20) // math.isqrt(grade ** lean) + 1 for grade in range(1, count + 1)]
    largest = most if full else min(most, max(-(-total // count), total * portions[0] // sum(portions)))
    least = 1 if total - largest >= count - 1 else 0
    given, rest = [largest] + [least] * (count - 1), total - largest - least * (count - 1)
    while rest > 0:
        free = [i for i in range(1, count) if given[i] < largest] or [i for i in range(1, count) if given[i] < most]
        pool, budget = sum([portions[i] for i in free]), rest
        for i in free:
            addition = min(most - given[i], max(1, budget * portions[i] // pool), rest)
            given[i] = given[i] + addition
            rest = rest - addition
    return np.array(given)


def gaussian(key, extent, deviation, most, pieces=(), held_as=jnp.bfloat16):
    values = deviation * jax.random.normal(key, extent, jnp.float32)
    if pieces:
        values = values * block_levels(key, extent, pieces, -0.22, 0.18)
    return jnp.clip(values, -most, most).astype(held_as)


def setup_inputs(seed: int = 0, part: int = 0) -> dict:
    seeds = jax.random.split(jax.random.key(seed), 27)
    part_keys = jax.random.split(jax.random.fold_in(seeds[26], part), 27)
    hidden = gaussian(part_keys[0], (SEQS, D), 1.0, 6.0, ((0, 16),))
    conv_window = gaussian(part_keys[1], (SEQS, CONV - 1, CONV_DIM), 1.0, 6.0, ((0, 16),))
    ssm_state = gaussian(part_keys[2], (SEQS, HEADS, HEAD_DIM, STATE), 0.3, 1.75, ((0, 16),), jnp.float32)
    gate_proj = gaussian(seeds[3], (D, INNER), D ** -0.5, 0.125, ((1, 16),))
    input_proj = gaussian(seeds[4], (D, INNER), D ** -0.5, 0.125, ((1, 16),))
    write_proj = gaussian(seeds[5], (D, GROUPS * STATE), D ** -0.5, 0.125, ((1, 16),))
    read_proj = gaussian(seeds[6], (D, GROUPS * STATE), D ** -0.5, 0.125, ((1, 16),))
    step_proj = gaussian(seeds[7], (D, HEADS), D ** -0.5, 0.125)
    step_bias = jnp.clip(jax.random.uniform(seeds[8], (HEADS,), jnp.float32, -2.0, 1.0), -2.0, 1.0)
    decay_log = jnp.clip(jax.random.uniform(seeds[9], (HEADS,), jnp.float32, -2.3, 1.4), -2.3, 1.4)
    decay_shift = jnp.clip(-0.7 + 0.7 * jax.random.uniform(part_keys[10], (SEQS, HEADS), jnp.float32) ** block_levels(part_keys[10], (SEQS, HEADS), ((0, 16),), -0.2, 0.2), -0.7, 0.0)
    skip_scale = gaussian(seeds[11], (HEADS,), 1.0, 4.0, (), jnp.float32)
    conv_taps = gaussian(seeds[12], (CONV, CONV_DIM), CONV ** -0.5, 3.0)
    conv_bias = gaussian(seeds[13], (CONV_DIM,), 0.5, 3.0, (), jnp.float32)
    mix_gain = jnp.clip(1.0 + 0.18 * jax.random.normal(seeds[14], (D,), jnp.float32), 0.1, 1.9)
    group_gain = jnp.clip(1.0 + 0.18 * jax.random.normal(seeds[15], (INNER,), jnp.float32), 0.1, 1.9)
    out_proj = gaussian(seeds[16], (INNER, D), INNER ** -0.5, 0.09375, ((1, 16),))
    ffn_gain = jnp.clip(1.0 + 0.18 * jax.random.normal(seeds[17], (D,), jnp.float32), 0.1, 1.9)
    router = gaussian(seeds[18], (D, EXPERTS), D ** -0.5, 0.125)
    expert_ids_keys = jax.random.split(jax.random.fold_in(part_keys[19], 1), SEQS // SEQ_DEV)
    expert_ids_turns = jax.random.permutation(jax.random.fold_in(part_keys[19], 3), SEQS // SEQ_DEV)
    expert_ids = jax.vmap(lambda own, number: routed_block(jax.random.fold_in(part_keys[19], 2), own, number, SEQ_DEV, EXPERTS, TOP_K, CAP, 2))(expert_ids_keys, expert_ids_turns).reshape((SEQS, TOP_K))
    expert_gate = gaussian(seeds[20], (EXPERTS, D, EFF), D ** -0.5, 0.125, ((0, 16),))
    expert_up = gaussian(seeds[21], (EXPERTS, D, EFF), D ** -0.5, 0.125, ((0, 16),))
    expert_down = gaussian(seeds[22], (EXPERTS, EFF, D), EFF ** -0.5, 0.25, ((0, 16),))
    shared_gate = gaussian(seeds[23], (D, SFF), D ** -0.5, 0.125, ((0, 16),))
    shared_up = gaussian(seeds[24], (D, SFF), D ** -0.5, 0.125, ((0, 16),))
    shared_down = gaussian(seeds[25], (SFF, D), SFF ** -0.5, 0.25)
    return {"hidden": hidden, "conv_window": conv_window, "ssm_state": ssm_state, "gate_proj": gate_proj, "input_proj": input_proj, "write_proj": write_proj, "read_proj": read_proj, "step_proj": step_proj, "step_bias": step_bias, "decay_log": decay_log, "decay_shift": decay_shift, "skip_scale": skip_scale, "conv_taps": conv_taps, "conv_bias": conv_bias, "mix_gain": mix_gain, "group_gain": group_gain, "out_proj": out_proj, "ffn_gain": ffn_gain, "router": router, "expert_ids": expert_ids, "expert_gate": expert_gate, "expert_up": expert_up, "expert_down": expert_down, "shared_gate": shared_gate, "shared_up": shared_up, "shared_down": shared_down}


epsilon = 1e-06
routed_scale = 2.5

def row_scale(values):
    return lax.rsqrt(lax.optimization_barrier(jnp.mean(values * values, axis=-1, keepdims=True)) + epsilon)

def matmul(left, right):
    return jnp.dot(left, right, preferred_element_type=jnp.float32)

def reference(hidden, conv_window, ssm_state, gate_proj, input_proj, write_proj, read_proj, step_proj, step_bias, decay_log, decay_shift, skip_scale, conv_taps, conv_bias, mix_gain, group_gain, out_proj, ffn_gain, router, expert_ids, expert_gate, expert_up, expert_down, shared_gate, shared_up, shared_down):
    batch_rows = hidden.shape[0]
    head_count = step_bias.shape[0]
    per_group = head_count // GROUPS
    inner_width = gate_proj.shape[1]
    state_span = GROUPS * STATE
    hidden_wide = hidden.astype(jnp.float32)
    normed = (hidden_wide * row_scale(hidden_wide) * mix_gain).astype(jnp.bfloat16)
    gate_rows = matmul(normed, gate_proj).astype(jnp.bfloat16)
    input_rows = matmul(normed, input_proj).astype(jnp.bfloat16)
    write_rows = matmul(normed, write_proj).astype(jnp.bfloat16)
    read_rows = matmul(normed, read_proj).astype(jnp.bfloat16)
    step_raw = matmul(normed, step_proj)
    fresh_row = jnp.concatenate([input_rows, write_rows, read_rows], axis=1)
    window = jnp.concatenate([conv_window, fresh_row[:, None, :]], axis=1)
    convolved = jax.nn.silu(lax.optimization_barrier(jnp.sum(window.astype(jnp.float32) * conv_taps.astype(jnp.float32)[None], axis=1)) + conv_bias)
    head_input = convolved[:, :inner_width].reshape(batch_rows, GROUPS, per_group, HEAD_DIM)
    write_vec = convolved[:, inner_width:inner_width + state_span].reshape(batch_rows, GROUPS, STATE)
    read_vec = convolved[:, inner_width + state_span:].reshape(batch_rows, GROUPS, STATE)
    step_size = jax.nn.softplus(step_raw + step_bias)
    decay_rate = jnp.exp(decay_shift - step_size * jnp.exp(decay_log)).reshape(batch_rows, GROUPS, per_group)
    step_group = step_size.reshape(batch_rows, GROUPS, per_group)
    carried = ssm_state.reshape(batch_rows, GROUPS, per_group, HEAD_DIM, STATE)
    next_state = decay_rate[..., None, None] * carried + (step_group[..., None] * head_input)[..., None] * write_vec[:, :, None, None, :]
    mixed_out = jnp.einsum('sgepn,sgn->sgep', next_state, read_vec, precision=lax.Precision.HIGHEST)
    mixed_out = mixed_out + skip_scale.reshape(GROUPS, per_group)[None, :, :, None] * head_input
    mixed_out = mixed_out.reshape(batch_rows, inner_width).astype(jnp.bfloat16)
    gated_out = mixed_out.astype(jnp.float32) * jax.nn.silu(gate_rows.astype(jnp.float32))
    blocks = gated_out.reshape(batch_rows, GROUPS, -1)
    gated_out = ((blocks * row_scale(blocks)).reshape(batch_rows, inner_width) * group_gain).astype(jnp.bfloat16)
    resid = (hidden_wide + matmul(gated_out, out_proj)).astype(jnp.bfloat16)
    resid_wide = resid.astype(jnp.float32)
    norm_scale = row_scale(resid_wide)
    routed_in = (resid_wide * norm_scale * ffn_gain).astype(jnp.bfloat16)
    shared_in = (resid_wide * ffn_gain).astype(jnp.bfloat16)
    scores = jax.nn.sigmoid(matmul(routed_in, router))
    picked = jnp.take_along_axis(scores, expert_ids, axis=1)
    weights = routed_scale * picked / lax.optimization_barrier(jnp.sum(picked, axis=1, keepdims=True))

    def add_expert(running, inputs):
        weight_gate, weight_up, weight_down, index = inputs
        expert_hidden = (jax.nn.silu(matmul(routed_in, weight_gate)) * matmul(routed_in, weight_up)).astype(jnp.bfloat16)
        result = matmul(expert_hidden, weight_down).astype(jnp.bfloat16)
        coefficient = lax.optimization_barrier(jnp.sum(jnp.where(expert_ids == index, weights, 0.0), axis=1))
        return (running + coefficient[:, None] * result.astype(jnp.float32), None)
    routed, _ = lax.scan(add_expert, jnp.zeros((batch_rows, hidden.shape[1]), jnp.float32), (expert_gate, expert_up, expert_down, jnp.arange(expert_gate.shape[0], dtype=jnp.int32)))
    shared_hidden = (jax.nn.silu(norm_scale * matmul(shared_in, shared_gate)) * (norm_scale * matmul(shared_in, shared_up))).astype(jnp.bfloat16)
    layer_out = (resid_wide + routed + matmul(shared_hidden, shared_down)).astype(jnp.bfloat16)
    return (layer_out, next_state.reshape(ssm_state.shape), window[:, 1:])
```

```python
import functools
import typing

import jax
import jax.numpy as jnp
from jax import lax
from jax.experimental import pallas as pl
from jax.experimental.pallas import tpu as pltpu
from jax.sharding import PartitionSpec as P

HEAD_DIM = 64
GROUPS = 8
STATE = 128


epsilon = 1e-06
routed_scale = 2.5


def row_scale(values):
    return lax.rsqrt(jnp.mean(values * values, axis=-1, keepdims=True) + epsilon)


def matmul(left, right):
    return jnp.dot(left, right, preferred_element_type=jnp.float32)


def expert_result(rows_in, weight_gate, weight_up, weight_down):
    expert_hidden = (jax.nn.silu(matmul(rows_in, weight_gate)) * matmul(rows_in, weight_up)).astype(
        jnp.bfloat16
    )
    return matmul(expert_hidden, weight_down).astype(jnp.bfloat16)


def exchange_kernel(n, spread, source, landed, send_sem, recv_sem, own_sem):
    me = lax.axis_index("ep")
    barrier = pltpu.get_barrier_semaphore()
    for step in range(1, n):
        pl.semaphore_signal(
            barrier, inc=1, device_id={"ep": lax.rem(me + step, n)}, device_id_type=pl.DeviceIdType.MESH
        )
    own = pltpu.make_async_copy(source if spread else source.at[me], landed.at[me], own_sem)
    own.start()
    pl.semaphore_wait(barrier, n - 1)
    copies = []
    for step in range(1, n):
        target = lax.rem(me + step, n)
        copy = pltpu.make_async_remote_copy(
            src_ref=source if spread else source.at[target],
            dst_ref=landed.at[me],
            send_sem=send_sem.at[step],
            recv_sem=recv_sem.at[step],
            device_id={"ep": target},
            device_id_type=pl.DeviceIdType.MESH,
        )
        copy.start()
        copies.append(copy)
    own.wait()
    for copy in copies:
        copy.wait()


def send(source, shape, spread, ident):
    n = shape[0]
    return pl.pallas_call(
        functools.partial(exchange_kernel, n, spread),
        out_shape=jax.ShapeDtypeStruct(shape, source.dtype),
        in_specs=[pl.BlockSpec(memory_space=pltpu.VMEM)],
        out_specs=pl.BlockSpec(memory_space=pltpu.VMEM),
        scratch_shapes=[
            pltpu.SemaphoreType.DMA((n,)),
            pltpu.SemaphoreType.DMA((n,)),
            pltpu.SemaphoreType.DMA,
        ],
        compiler_params=pltpu.CompilerParams(collective_id=ident, has_side_effects=True),
    )(source)


def exchange(blocks, ident):
    return send(blocks, blocks.shape, False, ident)


def gather(block, ident):
    return send(block, (lax.axis_size("ep"),) + block.shape, True, ident)


def transposed(left, right):
    return lax.dot_general(left, right, (((1,), (1,)), ((), ())), preferred_element_type=jnp.float32)


def state_kernel(per_group, decay, inputs, write, read, carried, updated, mixed):
    row, part = pl.program_id(0), pl.program_id(1)
    heads = carried.shape[1]
    scaled = inputs[0, 0]
    lane = lax.broadcasted_iota(jnp.int32, scaled.shape, 1)
    total = jnp.zeros(scaled.shape, jnp.float32)
    entries = carried.shape[3]
    head_dim = carried.shape[2]
    for group in range(heads // per_group):
        write_row = write[0, 0, group : group + 1]
        spread = jnp.broadcast_to(read[0, 0, group : group + 1], (entries, entries))
        spread_high = spread.astype(jnp.bfloat16)
        spread_low = (spread - spread_high.astype(jnp.float32)).astype(jnp.bfloat16)
        pieces = []
        for head in range(group * per_group, (group + 1) * per_group):
            fresh = (
                carried[0, head] * decay[row, part * heads + head]
                + scaled[:, head : head + 1] * write_row
            )
            updated[0, head] = fresh
            pieces.append(fresh)
        stacked = jnp.concatenate(pieces, axis=0)
        high = stacked.astype(jnp.bfloat16)
        low = (stacked - high.astype(jnp.float32)).astype(jnp.bfloat16)
        columns = transposed(high, spread_high) + transposed(low, spread_high) + transposed(high, spread_low)
        for place in range(per_group):
            head = group * per_group + place
            column = columns[place * head_dim : (place + 1) * head_dim, :heads]
            total = jnp.where(lane == head, column, total)
    mixed[0, 0] = total


def state_step(state, decay_rate, scaled, write_vec, read_vec):
    rows, head_count, head_dim, entries = state.shape
    groups = write_vec.shape[1]
    parts = 2
    heads = head_count // parts
    inputs = scaled.reshape(rows, parts, heads, head_dim).transpose(0, 1, 3, 2)
    vec_shape = (rows, parts, groups // parts, entries)
    part_spec = lambda *dims: pl.BlockSpec((1, 1) + dims, lambda row, part: (row, part, 0, 0))
    state_spec = pl.BlockSpec((1, heads, head_dim, entries), lambda row, part: (row, part, 0, 0))
    next_state, mixed = pl.pallas_call(
        functools.partial(state_kernel, head_count // groups),
        grid=(rows, parts),
        out_shape=(
            jax.ShapeDtypeStruct(state.shape, jnp.float32),
            jax.ShapeDtypeStruct(inputs.shape, jnp.float32),
        ),
        in_specs=[
            pl.BlockSpec(memory_space=pltpu.SMEM),
            part_spec(head_dim, heads),
            part_spec(groups // parts, entries),
            part_spec(groups // parts, entries),
            state_spec,
        ],
        out_specs=(state_spec, part_spec(head_dim, heads)),
    )(decay_rate, inputs, write_vec.reshape(vec_shape), read_vec.reshape(vec_shape), state)
    return next_state, mixed.transpose(0, 1, 3, 2).reshape(rows, head_count, head_dim)


def shards(
    hidden,
    conv_window,
    ssm_state,
    gate_proj,
    input_proj,
    write_proj,
    read_proj,
    step_proj,
    step_bias,
    decay_log,
    decay_shift,
    skip_scale,
    conv_taps,
    conv_bias,
    mix_gain,
    group_gain,
    out_proj,
    ffn_gain,
    router,
    expert_ids,
    expert_gate,
    expert_up,
    expert_down,
    shared_gate,
    shared_up,
    shared_down,
):
    local_rows = hidden.shape[0]
    device_index = lax.axis_index("ep")
    width = hidden.shape[1]
    first_row = device_index * local_rows
    gathered = gather(hidden, 0).reshape(-1, width)
    gathered_wide = gathered.astype(jnp.float32)
    normed = (gathered_wide * row_scale(gathered_wide) * mix_gain).astype(jnp.bfloat16)
    parts = [matmul(normed, proj).astype(jnp.bfloat16) for proj in (gate_proj, input_proj, write_proj, read_proj)]
    outbound = jnp.concatenate(parts, axis=1)
    arrived = exchange(outbound.reshape(-1, local_rows, outbound.shape[1]), 1)
    rows, offset = [], 0
    for part in parts:
        piece = arrived[:, :, offset : offset + part.shape[1]]
        rows.append(piece.transpose(1, 0, 2).reshape(local_rows, -1))
        offset += part.shape[1]
    gate_rows, input_rows, write_rows, read_rows = rows
    hidden_wide = hidden.astype(jnp.float32)
    normed_local = (hidden_wide * row_scale(hidden_wide) * mix_gain).astype(jnp.bfloat16)
    step_raw = matmul(normed_local, step_proj)
    inner_width = gate_rows.shape[1]
    state_span = GROUPS * STATE
    head_count = step_bias.shape[0]
    fresh_row = jnp.concatenate([input_rows, write_rows, read_rows], axis=1)
    window = jnp.concatenate([conv_window, fresh_row[:, None, :]], axis=1)
    convolved = jax.nn.silu(
        jnp.sum(window.astype(jnp.float32) * conv_taps.astype(jnp.float32)[None], axis=1)
        + conv_bias
    )
    head_input = convolved[:, :inner_width].reshape(local_rows, head_count, HEAD_DIM)
    write_vec = convolved[:, inner_width : inner_width + state_span].reshape(
        local_rows, GROUPS, STATE
    )
    read_vec = convolved[:, inner_width + state_span :].reshape(local_rows, GROUPS, STATE)
    step_size = jax.nn.softplus(step_raw + step_bias)
    decay_rate = jnp.exp(decay_shift - step_size * jnp.exp(decay_log))
    next_state, mixed_out = state_step(
        ssm_state, decay_rate, step_size[:, :, None] * head_input, write_vec, read_vec
    )
    mixed_out = mixed_out + skip_scale[None, :, None] * head_input
    mixed_out = mixed_out.reshape(local_rows, inner_width).astype(jnp.bfloat16)
    gated_out = mixed_out.astype(jnp.float32) * jax.nn.silu(gate_rows.astype(jnp.float32))
    blocks = gated_out.reshape(local_rows, GROUPS, -1)
    gated_out = ((blocks * row_scale(blocks)).reshape(local_rows, inner_width) * group_gain).astype(
        jnp.bfloat16
    )
    col_width = out_proj.shape[1]
    resid_cols = lax.dynamic_slice_in_dim(gathered_wide, device_index * col_width, col_width, 1)
    resid_part = (
        resid_cols + matmul(gather(gated_out, 2).reshape(-1, inner_width), out_proj)
    ).astype(jnp.bfloat16)
    resid_all = gather(resid_part, 3).transpose(1, 0, 2).reshape(-1, width)
    gain_part = lax.dynamic_slice_in_dim(ffn_gain, device_index * col_width, col_width, 0)
    shared_part = (resid_part.astype(jnp.float32) * gain_part).astype(jnp.bfloat16)
    shared_pre = jnp.concatenate(
        [matmul(shared_part, shared_gate), matmul(shared_part, shared_up)], axis=1
    ).astype(jnp.bfloat16)
    resid_all_wide = resid_all.astype(jnp.float32)
    scale_all = row_scale(resid_all_wide)
    routed_all = (resid_all_wide * scale_all * ffn_gain).astype(jnp.bfloat16)
    result = expert_result(routed_all, expert_gate[0], expert_up[0], expert_down[0])
    back = exchange(
        jnp.concatenate([result, shared_pre], axis=1).reshape(
            -1, local_rows, width + shared_pre.shape[1]
        ),
        4,
    ).astype(jnp.float32)
    resid_wide = lax.dynamic_slice_in_dim(resid_all_wide, first_row, local_rows, 0)
    norm_scale = lax.dynamic_slice_in_dim(scale_all, first_row, local_rows, 0)
    routed_in = lax.dynamic_slice_in_dim(routed_all, first_row, local_rows, 0)
    scores = jax.nn.sigmoid(matmul(routed_in, router))
    chosen = jnp.any(
        expert_ids[:, :, None] == jnp.arange(router.shape[1], dtype=jnp.int32)[None, None, :], axis=1
    )
    scores = jnp.where(chosen, scores, 0.0)
    weights = routed_scale * scores / jnp.sum(scores, axis=1, keepdims=True)
    routed = jnp.sum(back[:, :, :width] * weights.T[:, :, None], axis=0)
    shared_sum = jnp.sum(back[:, :, width:], axis=0)
    hidden_units = shared_down.shape[0]
    shared_hidden = (
        jax.nn.silu(norm_scale * shared_sum[:, :hidden_units])
        * (norm_scale * shared_sum[:, hidden_units:])
    ).astype(jnp.bfloat16)
    layer_out = (resid_wide + routed + matmul(shared_hidden, shared_down)).astype(jnp.bfloat16)
    return (layer_out, next_state, window[:, 1:])


def dot_t(left, right):
    return lax.dot_general(left, right, (((1,), (1,)), ((), ())), preferred_element_type=jnp.float32)


def dot_0(left, right):
    return lax.dot_general(left, right, (((0,), (0,)), ((), ())), preferred_element_type=jnp.float32)


def silu(v):
    return v / (1.0 + jnp.exp(-v))


def split2(v):
    high = v.astype(jnp.bfloat16)
    return high, (v - high.astype(jnp.float32)).astype(jnp.bfloat16)


class Args(typing.NamedTuple):
    hidden: typing.Any
    conv_window: typing.Any
    ssm_state: typing.Any
    gate_proj: typing.Any
    input_proj: typing.Any
    write_t: typing.Any
    read_t: typing.Any
    step_t: typing.Any
    step_bias: typing.Any
    decay_log: typing.Any
    decay_shift: typing.Any
    skip_scale: typing.Any
    conv_taps: typing.Any
    conv_bias: typing.Any
    mix_gain: typing.Any
    group_gain: typing.Any
    out_proj: typing.Any
    ffn_gain: typing.Any
    router_t: typing.Any
    expert_ids: typing.Any
    expert_gate: typing.Any
    expert_up: typing.Any
    expert_down: typing.Any
    shared_gate: typing.Any
    shared_up: typing.Any
    shared_down: typing.Any


def layer_kernel(n, rows, *refs):
    count = len(Args._fields)
    hbm = Args(*refs[:count])
    layer_out, next_state, next_window = refs[count : count + 3]
    vm = Args(*refs[count + 3 : 2 * count + 3])
    (
        src1, land1, src2, land2, src3, land3, src4, land4, src5, land5, src6, land6,
        fold1, fold3, fold5, x_all, x_low, p_all, extra, g_all, g_low, h_all, flag0, flag2, part48,
        acc_gate, acc_up, base, cols, y_all, fresh, xv, wv, rv, step_x, skip_x,
        decay_col, decayed, window, slots, served_f, in_sem, send_sem, recv_sem, pass_send, pass_recv,
    ) = refs[2 * count + 3 :]
    me = lax.axis_index("ep")
    f32, bf16 = jnp.float32, jnp.bfloat16
    width = vm.hidden.shape[1]
    inner = cols.shape[1]
    total = n * rows
    heads = hbm.step_bias.shape[1]
    head_dim = inner // heads
    groups = GROUPS
    per_group = heads // groups
    span = inner // groups
    state = STATE
    gate_cols = hbm.gate_proj.shape[1]
    vec_cols = hbm.write_t.shape[0]
    col_width = hbm.out_proj.shape[1]
    shared_units = hbm.shared_gate.shape[1]

    def flipped(value):
        other = me
        bit = 1
        while bit < n:
            if value & bit:
                other = other + bit - 2 * bit * lax.rem(me // bit, 2)
            bit *= 2
        return other

    far_first = tuple(range(n - 1, 0, -1))
    partner = flipped(1)

    barrier = pltpu.get_barrier_semaphore()
    for step in far_first:
        pl.semaphore_signal(
            barrier, inc=1, device_id={"ep": flipped(step)}, device_id_type=pl.DeviceIdType.MESH
        )
    loads = Args(
        *[pltpu.make_async_copy(there, here, in_sem.at[at]) for at, (there, here) in enumerate(zip(hbm, vm))]
    )
    for one in (
        loads.hidden,
        loads.mix_gain,
        loads.expert_ids,
        loads.gate_proj,
        loads.input_proj,
        loads.write_t,
        loads.read_t,
        loads.step_t,
        loads.step_bias,
        loads.decay_log,
        loads.decay_shift,
        loads.skip_scale,
        loads.conv_window,
        loads.conv_taps,
        loads.conv_bias,
        loads.ssm_state,
        loads.group_gain,
        loads.out_proj,
        loads.shared_gate,
        loads.shared_up,
        loads.ffn_gain,
        loads.expert_gate,
        loads.expert_up,
        loads.expert_down,
        loads.router_t,
        loads.shared_down,
    ):
        one.start()

    def need(*these):
        for one in these:
            one.wait()

    def remote(source, target_ref, sends, arrives, target):
        return pltpu.make_async_remote_copy(
            src_ref=source,
            dst_ref=target_ref,
            send_sem=sends,
            recv_sem=arrives,
            device_id={"ep": target},
            device_id_type=pl.DeviceIdType.MESH,
        )

    sent = []

    def begin(one):
        one.start()
        sent.append(one)
        return one

    def spread(phase, source, landed):
        steps = far_first[:: 2] if n % 2 else tuple(range(n - 2, 0, -2))
        out = {}
        for step in steps:
            out[step] = begin(
                remote(source, landed.at[me], send_sem.at[phase, step], recv_sem.at[phase, step], flipped(step))
            )
        out[0] = begin(remote(source, landed.at[me], pass_send.at[phase, 0], pass_recv.at[phase, 0], partner))
        return out

    def collect(phase, landed, out, take):
        passed = [(partner, out[0])]
        for step in range(2, n, 2):
            out[step].wait_recv()
            owner = flipped(step)
            block = landed.at[owner]
            passed.append(
                (
                    flipped(step + 1),
                    begin(remote(block, block, pass_send.at[phase, step], pass_recv.at[phase, step], partner)),
                )
            )
            take(owner)
        for owner, one in passed:
            one.wait_recv()
            take(owner)

    def scatter(phase, source, landed):
        return {
            step: begin(
                remote(
                    source.at[flipped(step)], landed.at[me], send_sem.at[phase, step], recv_sem.at[phase, me],
                    flipped(step),
                )
            )
            for step in far_first
        }

    def arrived(phase, source, landed, place):
        @pl.when(me != place)
        def _():
            remote(
                source, landed.at[place], send_sem.at[phase, 0], recv_sem.at[phase, place], place
            ).wait_recv()

    def folded(value, buffer):
        wide = buffer.shape[1]
        rest = wide // rows
        buffer[0:rows] = value[:, :wide]
        for row in range(rows):
            buffer[rows : rows + 1, row * rest : (row + 1) * rest] = value[row : row + 1, wide:]
        return buffer[...].astype(bf16)

    def unfolded(landed, owner, target):
        piece = landed[owner].astype(f32)
        wide = piece.shape[1]
        rest = wide // rows
        target[owner, 0:rows, :wide] = piece[0:rows]
        for row in range(rows):
            target[owner, row : row + 1, wide:] = piece[rows : rows + 1, row * rest : (row + 1) * rest]

    need(loads.hidden, loads.mix_gain, loads.expert_ids)
    own = vm.hidden[...].astype(f32)
    scale = lax.rsqrt(jnp.mean(own * own, axis=-1, keepdims=True) + epsilon)
    normed = (own * scale * vm.mix_gain[...]).astype(bf16)
    packed = folded(normed.astype(f32), fold1)
    src1[...] = packed
    land1[me] = packed
    pl.semaphore_wait(barrier, n - 1)
    rows1 = spread(0, src1, land1)

    lane = lax.broadcasted_iota(jnp.int32, (rows, 128), 1)
    ids = vm.expert_ids[...]
    chosen = jnp.zeros((rows, 128), f32)
    for k in range(ids.shape[1]):
        chosen = jnp.where(lane == ids[:, k : k + 1], 1.0, chosen)
    for place in range(n):
        for row in range(rows):
            extra[place, rows : rows + 1, row * col_width : (row + 1) * col_width] = own[
                row : row + 1, place * col_width : (place + 1) * col_width
            ]
        extra[place, rows : rows + 1, rows * col_width : rows * col_width + 128] = chosen[0:1]
        extra[place, rows : rows + 1, rows * col_width + 128 : rows * col_width + 256] = chosen[2:3]
    need(loads.step_t, loads.step_bias, loads.decay_log, loads.decay_shift, loads.skip_scale)
    raw = dot_t(normed, vm.step_t[...]) + vm.step_bias[...]
    step_size = jnp.maximum(raw, 0.0) + jnp.log1p(jnp.exp(-jnp.abs(raw)))
    decay = jnp.exp(vm.decay_shift[...] - step_size * jnp.exp(vm.decay_log[...]))
    skip = vm.skip_scale[...]
    low_half = lax.broadcasted_iota(jnp.int32, (rows, 128), 1) < head_dim
    for pair in range(heads // 2):
        at = slice(pair * 128, (pair + 1) * 128)
        first = jnp.broadcast_to(step_size[:, 2 * pair : 2 * pair + 1], (rows, 128))
        second = jnp.broadcast_to(step_size[:, 2 * pair + 1 : 2 * pair + 2], (rows, 128))
        step_x[:, at] = jnp.where(low_half, first, second)
        first = jnp.broadcast_to(skip[:, 2 * pair : 2 * pair + 1], (1, 128))
        second = jnp.broadcast_to(skip[:, 2 * pair + 1 : 2 * pair + 2], (1, 128))
        skip_x[:, at] = jnp.where(low_half[0:1], first, second)
    for row in range(rows):
        spread_row = jnp.broadcast_to(jnp.concatenate([decay[row : row + 1]] * 2, axis=1), (128, 128))
        turned = spread_row.T
        for group in range(groups):
            decay_col[row * groups + group] = turned[group * per_group : (group + 1) * per_group]

    need(loads.conv_window, loads.conv_taps, loads.conv_bias)
    taps = vm.conv_taps[...].astype(f32)
    for row in range(rows):
        old = vm.conv_window[row].astype(f32)
        base[row : row + 1] = (
            jnp.sum(old * taps[:3], axis=0, keepdims=True) + vm.conv_bias[...]
        )
        window[row, 0:2] = old[1:3]

    unfolded(land1, me, x_all)
    collect(0, land1, rows1, lambda owner: unfolded(land1, owner, x_all))
    need(loads.gate_proj, loads.input_proj, loads.write_t, loads.read_t)
    x_low[...] = x_all[...].reshape(x_low.shape).astype(bf16)
    p_all[:, :gate_cols] = matmul(x_low[...], vm.gate_proj[...])
    p_all[:, gate_cols : 2 * gate_cols] = matmul(x_low[...], vm.input_proj[...])
    p_all[:, 2 * gate_cols : 2 * gate_cols + vec_cols] = dot_t(x_low[...], vm.write_t[...])
    p_all[:, 2 * gate_cols + vec_cols :] = dot_t(x_low[...], vm.read_t[...])
    own_part = lax.broadcasted_iota(jnp.int32, extra.shape[1:], 0) < rows
    for place in range(n):
        src2[place] = jnp.where(own_part, p_all[8 * place : 8 * place + rows + 1], extra[place]).astype(bf16)
    scatter(1, src2, land2)
    land2[me] = src2[me]

    need(loads.ssm_state)

    def decay_group(at, carry):
        columns = decay_col[at]
        for head in range(per_group):
            part = slice(head * head_dim, (head + 1) * head_dim)
            value = vm.ssm_state[at, part] * columns[head : head + 1]
            next_state[at, part] = value
            decayed[at, part] = value.astype(bf16)
        return carry

    lax.fori_loop(0, rows * groups, decay_group, 0)

    need(loads.group_gain)
    half = vec_cols
    for place in range(0, n, 2):
        last = []
        for one in (place, place + 1):
            arrived(1, src2.at[0], land2, one)
            whole = land2[one].astype(f32)
            piece = whole[0:rows]
            at = slice(one * gate_cols, (one + 1) * gate_cols)
            cols[:, at] = piece[:, :gate_cols]
            fresh[:, at] = piece[:, gate_cols : 2 * gate_cols]
            last.append(piece[:, 2 * gate_cols :])
            for row in range(rows):
                h_all[8 * one + row : 8 * one + row + 1] = whole[
                    rows : rows + 1, row * col_width : (row + 1) * col_width
                ]
            flag0[one : one + 1] = whole[rows : rows + 1, rows * col_width : rows * col_width + 128]
            flag2[one : one + 1] = whole[rows : rows + 1, rows * col_width + 128 : rows * col_width + 256]
        low = lax.broadcasted_iota(jnp.int32, last[0].shape, 1) < half
        at = slice(inner + place * half, inner + (place + 2) * half)
        fresh[:, at] = jnp.where(low, last[0], pltpu.roll(last[1], half, 1))
        at = slice(at.start + groups * state, at.stop + groups * state)
        fresh[:, at] = jnp.where(low, pltpu.roll(last[0], half, 1), last[1])
    convolved = silu(base[...] + fresh[...] * taps[3:4])
    head_input = convolved[:, :inner]
    xv[...] = head_input
    for group in range(groups):
        at = slice(inner + group * state, inner + (group + 1) * state)
        write = convolved[:, at]
        read = convolved[:, at.start + groups * state : at.stop + groups * state]
        wv[group] = write
        rv[group] = read
    for group in range(groups):
        read = rv[group]
        high, low = split2(read)
        for row in range(rows):
            left = jnp.concatenate([high[row : row + 1], low[row : row + 1]], axis=0)
            both = dot_t(left, decayed[row * groups + group])
            y_all[row : row + 1, group * span : (group + 1) * span] = both[0:1] + both[1:2]
    for group in range(groups):
        at = slice(group * span, (group + 1) * span)
        overlap = jnp.sum(wv[group] * rv[group], axis=1, keepdims=True)
        mixed = y_all[:, at] + xv[:, at] * (step_x[:, at] * overlap + skip_x[:, at])
        mixed = mixed.astype(bf16).astype(f32) * silu(cols[:, at])
        mixed = mixed * lax.rsqrt(jnp.mean(mixed * mixed, axis=-1, keepdims=True) + epsilon)
        y_all[:, at] = mixed * vm.group_gain[:, at]
    packed = folded(y_all[...], fold3)
    src3[...] = packed
    land3[me] = packed
    rows3 = spread(2, src3, land3)

    for group in range(groups):
        at = slice(group * span, (group + 1) * span)
        high, low = split2(xv[:, at] * step_x[:, at])
        left = jnp.concatenate([high.astype(f32), low.astype(f32), high.astype(f32)], axis=0).astype(bf16)
        w_high, w_low = split2(wv[group])
        right = jnp.concatenate([w_high.astype(f32), w_high.astype(f32), w_low.astype(f32)], axis=0)
        owner = lax.rem(lax.broadcasted_iota(jnp.int32, right.shape, 0), rows)
        for row in range(rows):
            picked = jnp.where(owner == row, right, 0.0).astype(bf16)
            place = row * groups + group
            next_state[place] = next_state[place] + dot_0(left, picked)
    for row in range(rows):
        window[row, 2:3] = fresh[row : row + 1]
        next_window[row] = window[row].astype(bf16)

    slot_row = lax.broadcasted_iota(jnp.int32, (2 * n, total), 0)
    slot_lane = lax.broadcasted_iota(jnp.int32, (2 * n, total), 1)
    first_row = (slot_row // 2) * rows
    even = slot_row % 2 == 0
    outer = jnp.where(even, first_row, first_row + 2)
    whose = lax.broadcasted_iota(jnp.int32, (2 * n, n), 1) == lax.broadcasted_iota(jnp.int32, (2 * n, n), 0) // 2
    whose = jnp.where(whose, 1.0, 0.0).astype(bf16)
    even_row = lax.broadcasted_iota(jnp.int32, (2 * n, 128), 0) % 2 == 0
    flag = jnp.where(
        even_row, matmul(whose, flag0[...].astype(bf16)), matmul(whose, flag2[...].astype(bf16))
    )
    flag = jnp.where(lax.broadcasted_iota(jnp.int32, flag.shape, 1) == me, flag, 0.0)
    flag = jnp.sum(flag, axis=1, keepdims=True)
    source_row = jnp.where(flag > 0.5, outer, first_row + 1)
    select = jnp.where(slot_lane == source_row, 1.0, 0.0).astype(bf16)

    unfolded(land3, me, g_all)
    collect(2, land3, rows3, lambda owner: unfolded(land3, owner, g_all))
    need(loads.out_proj, loads.shared_gate, loads.shared_up, loads.ffn_gain)
    g_low[...] = g_all[...].reshape(g_low.shape).astype(bf16)
    resid_f = h_all[...] + matmul(g_low[...], vm.out_proj[...])
    for place in range(n):
        part48[place * rows : (place + 1) * rows] = resid_f[8 * place : 8 * place + rows]
    resid_part = part48[...].astype(bf16)
    src4[...] = resid_part
    land4[me] = resid_part
    rows4 = spread(3, src4, land4)
    gain_part = vm.ffn_gain[:, pl.ds(pl.multiple_of(me * col_width, col_width), col_width)]
    shared_part = (resid_part.astype(f32) * gain_part).astype(bf16)
    slots[:, :shared_units] = matmul(shared_part, vm.shared_gate[...])
    slots[:, shared_units:] = matmul(shared_part, vm.shared_up[...])
    for place in range(n):
        src5[place] = folded(slots[place * rows : (place + 1) * rows], fold5.at[place])
    scatter(4, src5, land5)
    land5[me] = src5[me]

    need(loads.expert_gate, loads.expert_up, loads.expert_down)
    acc_gate[...] = jnp.zeros_like(acc_gate)
    acc_up[...] = jnp.zeros_like(acc_up)
    squares = [jnp.zeros((total, col_width), f32)]

    def add_block(owner):
        piece = land4[owner].astype(f32)
        squares[0] = squares[0] + piece * piece
        at = pl.ds(pl.multiple_of(owner * col_width, col_width), col_width)
        scaled = (piece * vm.ffn_gain[:, at]).astype(bf16)
        acc_gate[...] += matmul(scaled, vm.expert_gate[at])
        acc_up[...] += matmul(scaled, vm.expert_up[at])

    add_block(me)
    collect(3, land4, rows4, add_block)
    scale_all = lax.rsqrt(jnp.sum(squares[0], axis=1, keepdims=True) / width + epsilon)
    hidden_units = (silu(acc_gate[...] * scale_all) * (acc_up[...] * scale_all)).astype(bf16)
    served = matmul(select, hidden_units).astype(bf16)
    served_f[...] = matmul(served, vm.expert_down[...])
    for place in range(n):
        src6[place] = served_f[2 * place : 2 * place + 2].astype(bf16)
    scatter(5, src6, land6)
    land6[me] = src6[me]

    need(loads.router_t, loads.shared_down)
    own_row = lax.broadcasted_iota(jnp.int32, (rows, total), 0) + me * rows
    pick = jnp.where(lax.broadcasted_iota(jnp.int32, (rows, total), 1) == own_row, 1.0, 0.0).astype(bf16)
    for place in range(n):
        at = slice(place * col_width, (place + 1) * col_width)
        y_all[:, at] = matmul(pick, land4[place])
    resid_own = y_all[:, :width]
    norm_scale = lax.rsqrt(jnp.mean(resid_own * resid_own, axis=-1, keepdims=True) + epsilon)
    routed_own = (resid_own * norm_scale * vm.ffn_gain[...]).astype(bf16)
    scores = 1.0 / (1.0 + jnp.exp(-dot_t(routed_own, vm.router_t[...])))
    kept = chosen[:, :n]
    scores = jnp.where(kept > 0.5, scores, 0.0)
    weights = routed_scale * scores / jnp.sum(scores, axis=1, keepdims=True)
    outer_w = jnp.concatenate([weights[0:1], weights[2:3]], axis=0)
    middle = weights[1:2]
    inner_w = jnp.concatenate([middle * (1.0 - kept[0:1]), middle * kept[0:1]], axis=0)
    shared = jnp.zeros(fold5.shape[1:], f32)
    for place in range(n):
        arrived(4, src5.at[0], land5, place)
        shared = shared + land5[place].astype(f32)
    wide = shared.shape[1]
    rest = wide // rows
    cols[:, :wide] = shared[0:rows]
    for row in range(rows):
        cols[row : row + 1, wide : wide + rest] = shared[rows : rows + 1, row * rest : (row + 1) * rest]
    shared = cols[:, : wide + rest] * norm_scale
    shared_hidden = (silu(shared[:, :shared_units]) * shared[:, shared_units:]).astype(bf16)
    start = resid_own + matmul(shared_hidden, vm.shared_down[...])
    y_all[:, :width] = start
    ends = jnp.zeros((2, width), f32)
    mid = jnp.zeros((2, width), f32)
    for place in range(n):
        arrived(5, src6.at[0], land6, place)
        piece = land6[place].astype(f32)
        ends = ends + piece * outer_w[:, place : place + 1]
        mid = mid + piece * inner_w[:, place : place + 1]
    xv[0:1, :width] = ends[0:1]
    xv[1:2, :width] = mid[0:1] + mid[1:2]
    xv[2:3, :width] = ends[1:2]
    layer_out[...] = (y_all[:, :width] + xv[:, :width]).astype(bf16)
    for one in sent:
        one.wait_send()


def store_kernel(layer_out, next_state, next_window, layer_hbm, state_hbm, window_hbm, sems):
    pieces = [(layer_out, layer_hbm), (next_window, window_hbm)]
    pieces += [(next_state.at[at], state_hbm.at[at]) for at in range(next_state.shape[0])]
    copies = [pltpu.make_async_copy(a, b, sems.at[at]) for at, (a, b) in enumerate(pieces)]
    for one in copies:
        one.start()
    for one in copies:
        one.wait()


def one_kernel(*args):
    named = Args(*args)
    n = lax.axis_size("ep")
    rows, width = named.hidden.shape
    inner = named.gate_proj.shape[1] * n
    total = n * rows
    heads = named.step_bias.shape[0]
    flat = lambda one: one.reshape(1, -1)
    named = named._replace(
        write_t=named.write_t.T,
        read_t=named.read_t.T,
        step_t=named.step_t.T,
        router_t=named.router_t.T,
        step_bias=flat(named.step_bias),
        decay_log=flat(named.decay_log),
        skip_scale=flat(named.skip_scale),
        conv_bias=flat(named.conv_bias),
        mix_gain=flat(named.mix_gain),
        group_gain=flat(named.group_gain),
        ffn_gain=flat(named.ffn_gain),
        expert_gate=named.expert_gate[0],
        expert_up=named.expert_up[0],
        expert_down=named.expert_down[0],
    )
    state_shape = named.ssm_state.shape
    span = inner // GROUPS
    named = named._replace(ssm_state=named.ssm_state.reshape(rows * GROUPS, span, STATE))
    conv_dim = named.conv_bias.shape[1]
    cols = 2 * named.gate_proj.shape[1] + 2 * named.write_t.shape[0]
    col_width = named.out_proj.shape[1]
    shared_units = named.shared_gate.shape[1]
    bf16, f32 = jnp.bfloat16, jnp.float32
    V = pltpu.VMEM
    scratch = [V(one.shape, one.dtype) for one in named]
    units = 2 * shared_units
    scratch += [
        V((4, width * 3 // 4), bf16), V((n, 4, width * 3 // 4), bf16),
        V((n, 4, cols), bf16), V((n, 4, cols), bf16),
        V((4, inner * 3 // 4), bf16), V((n, 4, inner * 3 // 4), bf16),
        V((total, col_width), bf16), V((n, total, col_width), bf16),
        V((n, 4, units * 3 // 4), bf16), V((n, 4, units * 3 // 4), bf16),
        V((n, 2, width), bf16), V((n, 2, width), bf16),
        V((4, width * 3 // 4), f32), V((4, inner * 3 // 4), f32), V((n, 4, units * 3 // 4), f32),
        V((n, 8, width), f32), V((n * 8, width), bf16), V((n * 8, cols), f32), V((n, 4, cols), f32),
        V((n, 8, inner), f32), V((n * 8, inner), bf16), V((n * 8, col_width), f32),
        V((n, 128), f32), V((n, 128), f32), V((total, col_width), f32),
        V((total, shared_units), f32), V((total, shared_units), f32),
        V((rows, conv_dim), f32), V((rows, inner), f32), V((rows, inner), f32), V((rows, conv_dim), f32),
        V((rows, inner), f32), V((GROUPS, rows, STATE), f32), V((GROUPS, rows, STATE), f32),
        V((rows, inner), f32), V((1, inner), f32),
        V((rows * GROUPS, heads // GROUPS, 128), f32), V((rows * GROUPS, span, STATE), bf16),
        V((rows, 3, conv_dim), f32), V((total, units), f32), V((2 * n, width), f32),
        pltpu.SemaphoreType.DMA((len(named),)),
        pltpu.SemaphoreType.DMA((6, n)),
        pltpu.SemaphoreType.DMA((6, n)),
        pltpu.SemaphoreType.DMA((6, n)),
        pltpu.SemaphoreType.DMA((6, n)),
    ]
    layer_out, next_state, next_window = pl.pallas_call(
        functools.partial(layer_kernel, n, rows),
        out_shape=(
            pltpu.VMEM((rows, width), bf16),
            pltpu.VMEM(named.ssm_state.shape, f32),
            pltpu.VMEM(named.conv_window.shape, bf16),
        ),
        in_specs=[pl.BlockSpec(memory_space=pltpu.HBM)] * len(named),
        out_specs=tuple(pl.BlockSpec(memory_space=pltpu.VMEM) for _ in range(3)),
        scratch_shapes=scratch,
        compiler_params=pltpu.CompilerParams(
            collective_id=0, has_side_effects=True, vmem_limit_bytes=36 * 1024 * 1024
        ),
    )(*[pltpu.with_memory_space_constraint(one, pltpu.HBM) for one in named])
    outs = (layer_out, next_state, next_window)
    layer_out, next_state, next_window = pl.pallas_call(
        store_kernel,
        out_shape=tuple(jax.ShapeDtypeStruct(one.shape, one.dtype) for one in outs),
        in_specs=[pl.BlockSpec(memory_space=pltpu.VMEM)] * 3,
        out_specs=tuple(pl.BlockSpec(memory_space=pltpu.HBM) for _ in range(3)),
        scratch_shapes=[pltpu.SemaphoreType.DMA((2 + named.ssm_state.shape[0],))],
        compiler_params=pltpu.CompilerParams(vmem_limit_bytes=1024 * 1024),
    )(*outs)
    return layer_out, next_state.reshape(state_shape), next_window


def fits(args):
    named = Args(*args)
    n = lax.axis_size("ep")
    return (
        named.hidden.shape[0] == 3
        and n & (n - 1) == 0
        and 2 <= n <= 128
        and named.hidden.shape[1] % 512 == 0
        and 2 * named.gate_proj.shape[1] + 128 == 3 * 128 + 256
        and named.expert_gate.shape[2] == named.shared_gate.shape[1]
        and named.shared_gate.shape[1] % 256 == 0
        and named.hidden.shape[1] <= named.group_gain.shape[0]
        and named.out_proj.shape[1] == 128
        and named.gate_proj.shape[1] % 128 == 0
        and named.write_t.shape[1] == 64
        and named.expert_gate.shape[0] == 1
        and named.router_t.shape[1] == n
        and HEAD_DIM * 2 == 128
    )


def body(*args):
    return one_kernel(*args) if fits(args) else shards(*args)


def solution(mesh):
    placed = (
        P(("grp", "ep"), None),
        P(("grp", "ep"), None, None),
        P(("grp", "ep"), None, None, None),
        P(None, "ep"),
        P(None, "ep"),
        P(None, "ep"),
        P(None, "ep"),
        P(),
        P(),
        P(),
        P(("grp", "ep"), None),
        P(),
        P(),
        P(),
        P(),
        P(),
        P(None, "ep"),
        P(),
        P(),
        P(("grp", "ep"), None),
        P("ep", None, None),
        P("ep", None, None),
        P("ep", None, None),
        P("ep", None),
        P("ep", None),
        P(),
    )
    return jax.shard_map(
        body,
        mesh=mesh,
        in_specs=placed,
        out_specs=(
            P(("grp", "ep"), None),
            P(("grp", "ep"), None, None, None),
            P(("grp", "ep"), None, None),
        ),
        check_vma=False,
    )
```

```python
import functools
import typing

import jax
import jax.numpy as jnp
from jax import lax
from jax.experimental import pallas as pl
from jax.experimental.pallas import tpu as pltpu
from jax.sharding import PartitionSpec as P

HEAD_DIM = 64
GROUPS = 8
STATE = 128


epsilon = 1e-06
routed_scale = 2.5


def row_scale(values):
    return lax.rsqrt(jnp.mean(values * values, axis=-1, keepdims=True) + epsilon)


def matmul(left, right):
    return jnp.dot(left, right, preferred_element_type=jnp.float32)


def expert_result(rows_in, weight_gate, weight_up, weight_down):
    expert_hidden = (jax.nn.silu(matmul(rows_in, weight_gate)) * matmul(rows_in, weight_up)).astype(
        jnp.bfloat16
    )
    return matmul(expert_hidden, weight_down).astype(jnp.bfloat16)


def exchange_kernel(n, spread, source, landed, send_sem, recv_sem, own_sem):
    me = lax.axis_index("ep")
    barrier = pltpu.get_barrier_semaphore()
    for step in range(1, n):
        pl.semaphore_signal(
            barrier, inc=1, device_id={"ep": lax.rem(me + step, n)}, device_id_type=pl.DeviceIdType.MESH
        )
    own = pltpu.make_async_copy(source if spread else source.at[me], landed.at[me], own_sem)
    own.start()
    pl.semaphore_wait(barrier, n - 1)
    copies = []
    for step in range(1, n):
        target = lax.rem(me + step, n)
        copy = pltpu.make_async_remote_copy(
            src_ref=source if spread else source.at[target],
            dst_ref=landed.at[me],
            send_sem=send_sem.at[step],
            recv_sem=recv_sem.at[step],
            device_id={"ep": target},
            device_id_type=pl.DeviceIdType.MESH,
        )
        copy.start()
        copies.append(copy)
    own.wait()
    for copy in copies:
        copy.wait()


def send(source, shape, spread, ident):
    n = shape[0]
    return pl.pallas_call(
        functools.partial(exchange_kernel, n, spread),
        out_shape=jax.ShapeDtypeStruct(shape, source.dtype),
        in_specs=[pl.BlockSpec(memory_space=pltpu.VMEM)],
        out_specs=pl.BlockSpec(memory_space=pltpu.VMEM),
        scratch_shapes=[
            pltpu.SemaphoreType.DMA((n,)),
            pltpu.SemaphoreType.DMA((n,)),
            pltpu.SemaphoreType.DMA,
        ],
        compiler_params=pltpu.CompilerParams(collective_id=ident, has_side_effects=True),
    )(source)


def exchange(blocks, ident):
    return send(blocks, blocks.shape, False, ident)


def gather(block, ident):
    return send(block, (lax.axis_size("ep"),) + block.shape, True, ident)


def transposed(left, right):
    return lax.dot_general(left, right, (((1,), (1,)), ((), ())), preferred_element_type=jnp.float32)


def state_kernel(per_group, decay, inputs, write, read, carried, updated, mixed):
    row, part = pl.program_id(0), pl.program_id(1)
    heads = carried.shape[1]
    scaled = inputs[0, 0]
    lane = lax.broadcasted_iota(jnp.int32, scaled.shape, 1)
    total = jnp.zeros(scaled.shape, jnp.float32)
    entries = carried.shape[3]
    head_dim = carried.shape[2]
    for group in range(heads // per_group):
        write_row = write[0, 0, group : group + 1]
        spread = jnp.broadcast_to(read[0, 0, group : group + 1], (entries, entries))
        spread_high = spread.astype(jnp.bfloat16)
        spread_low = (spread - spread_high.astype(jnp.float32)).astype(jnp.bfloat16)
        pieces = []
        for head in range(group * per_group, (group + 1) * per_group):
            fresh = (
                carried[0, head] * decay[row, part * heads + head]
                + scaled[:, head : head + 1] * write_row
            )
            updated[0, head] = fresh
            pieces.append(fresh)
        stacked = jnp.concatenate(pieces, axis=0)
        high = stacked.astype(jnp.bfloat16)
        low = (stacked - high.astype(jnp.float32)).astype(jnp.bfloat16)
        columns = transposed(high, spread_high) + transposed(low, spread_high) + transposed(high, spread_low)
        for place in range(per_group):
            head = group * per_group + place
            column = columns[place * head_dim : (place + 1) * head_dim, :heads]
            total = jnp.where(lane == head, column, total)
    mixed[0, 0] = total


def state_step(state, decay_rate, scaled, write_vec, read_vec):
    rows, head_count, head_dim, entries = state.shape
    groups = write_vec.shape[1]
    parts = 2
    heads = head_count // parts
    inputs = scaled.reshape(rows, parts, heads, head_dim).transpose(0, 1, 3, 2)
    vec_shape = (rows, parts, groups // parts, entries)
    part_spec = lambda *dims: pl.BlockSpec((1, 1) + dims, lambda row, part: (row, part, 0, 0))
    state_spec = pl.BlockSpec((1, heads, head_dim, entries), lambda row, part: (row, part, 0, 0))
    next_state, mixed = pl.pallas_call(
        functools.partial(state_kernel, head_count // groups),
        grid=(rows, parts),
        out_shape=(
            jax.ShapeDtypeStruct(state.shape, jnp.float32),
            jax.ShapeDtypeStruct(inputs.shape, jnp.float32),
        ),
        in_specs=[
            pl.BlockSpec(memory_space=pltpu.SMEM),
            part_spec(head_dim, heads),
            part_spec(groups // parts, entries),
            part_spec(groups // parts, entries),
            state_spec,
        ],
        out_specs=(state_spec, part_spec(head_dim, heads)),
    )(decay_rate, inputs, write_vec.reshape(vec_shape), read_vec.reshape(vec_shape), state)
    return next_state, mixed.transpose(0, 1, 3, 2).reshape(rows, head_count, head_dim)


def shards(
    hidden,
    conv_window,
    ssm_state,
    gate_proj,
    input_proj,
    write_proj,
    read_proj,
    step_proj,
    step_bias,
    decay_log,
    decay_shift,
    skip_scale,
    conv_taps,
    conv_bias,
    mix_gain,
    group_gain,
    out_proj,
    ffn_gain,
    router,
    expert_ids,
    expert_gate,
    expert_up,
    expert_down,
    shared_gate,
    shared_up,
    shared_down,
):
    local_rows = hidden.shape[0]
    device_index = lax.axis_index("ep")
    width = hidden.shape[1]
    first_row = device_index * local_rows
    gathered = gather(hidden, 0).reshape(-1, width)
    gathered_wide = gathered.astype(jnp.float32)
    normed = (gathered_wide * row_scale(gathered_wide) * mix_gain).astype(jnp.bfloat16)
    parts = [matmul(normed, proj).astype(jnp.bfloat16) for proj in (gate_proj, input_proj, write_proj, read_proj)]
    outbound = jnp.concatenate(parts, axis=1)
    arrived = exchange(outbound.reshape(-1, local_rows, outbound.shape[1]), 1)
    rows, offset = [], 0
    for part in parts:
        piece = arrived[:, :, offset : offset + part.shape[1]]
        rows.append(piece.transpose(1, 0, 2).reshape(local_rows, -1))
        offset += part.shape[1]
    gate_rows, input_rows, write_rows, read_rows = rows
    hidden_wide = hidden.astype(jnp.float32)
    normed_local = (hidden_wide * row_scale(hidden_wide) * mix_gain).astype(jnp.bfloat16)
    step_raw = matmul(normed_local, step_proj)
    inner_width = gate_rows.shape[1]
    state_span = GROUPS * STATE
    head_count = step_bias.shape[0]
    fresh_row = jnp.concatenate([input_rows, write_rows, read_rows], axis=1)
    window = jnp.concatenate([conv_window, fresh_row[:, None, :]], axis=1)
    convolved = jax.nn.silu(
        jnp.sum(window.astype(jnp.float32) * conv_taps.astype(jnp.float32)[None], axis=1)
        + conv_bias
    )
    head_input = convolved[:, :inner_width].reshape(local_rows, head_count, HEAD_DIM)
    write_vec = convolved[:, inner_width : inner_width + state_span].reshape(
        local_rows, GROUPS, STATE
    )
    read_vec = convolved[:, inner_width + state_span :].reshape(local_rows, GROUPS, STATE)
    step_size = jax.nn.softplus(step_raw + step_bias)
    decay_rate = jnp.exp(decay_shift - step_size * jnp.exp(decay_log))
    next_state, mixed_out = state_step(
        ssm_state, decay_rate, step_size[:, :, None] * head_input, write_vec, read_vec
    )
    mixed_out = mixed_out + skip_scale[None, :, None] * head_input
    mixed_out = mixed_out.reshape(local_rows, inner_width).astype(jnp.bfloat16)
    gated_out = mixed_out.astype(jnp.float32) * jax.nn.silu(gate_rows.astype(jnp.float32))
    blocks = gated_out.reshape(local_rows, GROUPS, -1)
    gated_out = ((blocks * row_scale(blocks)).reshape(local_rows, inner_width) * group_gain).astype(
        jnp.bfloat16
    )
    col_width = out_proj.shape[1]
    resid_cols = lax.dynamic_slice_in_dim(gathered_wide, device_index * col_width, col_width, 1)
    resid_part = (
        resid_cols + matmul(gather(gated_out, 2).reshape(-1, inner_width), out_proj)
    ).astype(jnp.bfloat16)
    resid_all = gather(resid_part, 3).transpose(1, 0, 2).reshape(-1, width)
    gain_part = lax.dynamic_slice_in_dim(ffn_gain, device_index * col_width, col_width, 0)
    shared_part = (resid_part.astype(jnp.float32) * gain_part).astype(jnp.bfloat16)
    shared_pre = jnp.concatenate(
        [matmul(shared_part, shared_gate), matmul(shared_part, shared_up)], axis=1
    ).astype(jnp.bfloat16)
    resid_all_wide = resid_all.astype(jnp.float32)
    scale_all = row_scale(resid_all_wide)
    routed_all = (resid_all_wide * scale_all * ffn_gain).astype(jnp.bfloat16)
    result = expert_result(routed_all, expert_gate[0], expert_up[0], expert_down[0])
    back = exchange(
        jnp.concatenate([result, shared_pre], axis=1).reshape(
            -1, local_rows, width + shared_pre.shape[1]
        ),
        4,
    ).astype(jnp.float32)
    resid_wide = lax.dynamic_slice_in_dim(resid_all_wide, first_row, local_rows, 0)
    norm_scale = lax.dynamic_slice_in_dim(scale_all, first_row, local_rows, 0)
    routed_in = lax.dynamic_slice_in_dim(routed_all, first_row, local_rows, 0)
    scores = jax.nn.sigmoid(matmul(routed_in, router))
    chosen = jnp.any(
        expert_ids[:, :, None] == jnp.arange(router.shape[1], dtype=jnp.int32)[None, None, :], axis=1
    )
    scores = jnp.where(chosen, scores, 0.0)
    weights = routed_scale * scores / jnp.sum(scores, axis=1, keepdims=True)
    routed = jnp.sum(back[:, :, :width] * weights.T[:, :, None], axis=0)
    shared_sum = jnp.sum(back[:, :, width:], axis=0)
    hidden_units = shared_down.shape[0]
    shared_hidden = (
        jax.nn.silu(norm_scale * shared_sum[:, :hidden_units])
        * (norm_scale * shared_sum[:, hidden_units:])
    ).astype(jnp.bfloat16)
    layer_out = (resid_wide + routed + matmul(shared_hidden, shared_down)).astype(jnp.bfloat16)
    return (layer_out, next_state, window[:, 1:])


def dot_t(left, right):
    return lax.dot_general(left, right, (((1,), (1,)), ((), ())), preferred_element_type=jnp.float32)


def dot_0(left, right):
    return lax.dot_general(left, right, (((0,), (0,)), ((), ())), preferred_element_type=jnp.float32)


def silu(v):
    return v / (1.0 + jnp.exp(-v))


def split2(v):
    high = v.astype(jnp.bfloat16)
    return high, (v - high.astype(jnp.float32)).astype(jnp.bfloat16)


class Args(typing.NamedTuple):
    hidden: typing.Any
    conv_window: typing.Any
    ssm_state: typing.Any
    gate_proj: typing.Any
    input_proj: typing.Any
    write_t: typing.Any
    read_t: typing.Any
    step_t: typing.Any
    step_bias: typing.Any
    decay_log: typing.Any
    decay_shift: typing.Any
    skip_scale: typing.Any
    conv_taps: typing.Any
    conv_bias: typing.Any
    mix_gain: typing.Any
    group_gain: typing.Any
    out_proj: typing.Any
    ffn_gain: typing.Any
    router_t: typing.Any
    expert_ids: typing.Any
    expert_gate: typing.Any
    expert_up: typing.Any
    expert_down: typing.Any
    shared_gate: typing.Any
    shared_up: typing.Any
    shared_down: typing.Any


def layer_kernel(n, rows, *refs):
    count = len(Args._fields)
    hbm = Args(*refs[:count])
    layer_out, next_state, next_window = refs[count : count + 3]
    vm = Args(*refs[count + 3 : 2 * count + 3])
    (
        src1, land1, src2, land2, src_g, land_g, src3, land3, src4, land4, src5, land5, src6, land6,
        fold1, fold3, fold5, x_all, x_low, p_all, gate_all, extra, g_all, g_low, h_all, flag0, flag2, part48,
        acc_gate, acc_up, base, cols, y_all, fresh, xv, wv, rv, step_x, skip_x,
        decay_col, decayed, window, slots, served_f, vec_proj,
        in_sem, send_sem, ring_sem, part_sem, whole_sem,
    ) = refs[2 * count + 3 :]
    me = lax.axis_index("ep")
    f32, bf16 = jnp.float32, jnp.bfloat16
    width = vm.hidden.shape[1]
    inner = cols.shape[1]
    total = n * rows
    heads = hbm.step_bias.shape[1]
    head_dim = inner // heads
    groups = GROUPS
    per_group = heads // groups
    span = inner // groups
    state = STATE
    gate_cols = hbm.gate_proj.shape[1]
    vec_cols = hbm.write_t.shape[0]
    col_width = hbm.out_proj.shape[1]
    shared_units = hbm.shared_gate.shape[1]

    def flipped(value):
        other = me
        bit = 1
        while bit < n:
            if value & bit:
                other = other + bit - 2 * bit * lax.rem(me // bit, 2)
            bit *= 2
        return other

    far_first = tuple(range(n - 1, 0, -1))
    partner = flipped(1)

    barrier = pltpu.get_barrier_semaphore()
    for step in far_first:
        pl.semaphore_signal(
            barrier, inc=1, device_id={"ep": flipped(step)}, device_id_type=pl.DeviceIdType.MESH
        )
    loads = Args(
        *[pltpu.make_async_copy(there, here, in_sem.at[at]) for at, (there, here) in enumerate(zip(hbm, vm))]
    )
    for one in (
        loads.hidden,
        loads.mix_gain,
        loads.expert_ids,
        loads.gate_proj,
        loads.input_proj,
        loads.write_t,
        loads.read_t,
        loads.step_t,
        loads.step_bias,
        loads.decay_log,
        loads.decay_shift,
        loads.skip_scale,
        loads.conv_window,
        loads.conv_taps,
        loads.conv_bias,
        loads.ssm_state,
        loads.group_gain,
        loads.out_proj,
        loads.shared_gate,
        loads.shared_up,
        loads.ffn_gain,
        loads.expert_gate,
        loads.expert_up,
        loads.expert_down,
        loads.router_t,
        loads.shared_down,
    ):
        one.start()

    def need(*these):
        for one in these:
            one.wait()

    def remote(source, target_ref, sends, arrives, target):
        return pltpu.make_async_remote_copy(
            src_ref=source,
            dst_ref=target_ref,
            send_sem=sends,
            recv_sem=arrives,
            device_id={"ep": target},
            device_id_type=pl.DeviceIdType.MESH,
        )

    blocks = []

    def sends(phase, landed):
        blocks.append((phase, landed))
        return send_sem.at[phase]

    def all_blocks(landed, sem, arrives):
        many = landed.at[pl.ds(0, n - 1)]
        return remote(many, many, sem, arrives, partner)

    def spread(phase, ring, source, landed):
        sem = sends(phase, landed)
        out = {}
        for step in range(n - 2, -1, -2):
            out[step] = remote(source, landed.at[me], sem, ring_sem.at[ring, step + 1], flipped(step + 1))
            out[step].start()
        return out

    def collect(phase, ring, landed, out, take):
        passed = [(partner, out[0])]
        for step in range(2, n, 2):
            out[step].wait_recv()
            owner = flipped(step + 1)
            block = landed.at[owner]
            one = remote(block, block, send_sem.at[phase], ring_sem.at[ring, step], partner)
            one.start()
            passed.append((flipped(step), one))
            take(owner, 0)
        return passed

    def finish(passed, take):
        for owner, one in passed:
            one.wait_recv()
            take(owner, 0 if owner is partner else 1)

    def scatter(phase, source, landed, sem):
        sent = sends(phase, landed)
        for step in far_first:
            to = flipped(step)
            remote(source.at[to], landed.at[me], sent, sem, to).start()

    def arrived(part, landed, place):
        @pl.when(me != place)
        def _():
            block = landed.at[place]
            remote(block, block, send_sem.at[0], part_sem.at[part, place], place).wait_recv()

    def arrived_all(which, landed):
        all_blocks(landed, send_sem.at[0], whole_sem.at[which]).wait_recv()

    def folded(value, buffer):
        wide = buffer.shape[1]
        rest = wide // rows
        buffer[0:rows] = value[:, :wide]
        for row in range(rows):
            buffer[rows : rows + 1, row * rest : (row + 1) * rest] = value[row : row + 1, wide:]
        return buffer[...].astype(bf16)

    def unfolded(landed, owner, kind, target):
        piece = landed[owner].astype(f32)
        wide = piece.shape[1]
        rest = wide // rows
        chip = owner // 2
        target[chip, 4 * kind : 4 * kind + rows, :wide] = piece[0:rows]
        for row in range(rows):
            target[chip, 4 * kind + row : 4 * kind + row + 1, wide:] = piece[
                rows : rows + 1, row * rest : (row + 1) * rest
            ]

    def in_order(value):
        tiles = value.reshape(n // 2, 8, value.shape[1])
        turned = jnp.concatenate([tiles[:, 4:], tiles[:, :4]], axis=1)
        return jnp.where(lax.rem(me, 2) == 1, tiles, turned).reshape(value.shape)

    need(loads.hidden, loads.mix_gain, loads.expert_ids)
    own = vm.hidden[...].astype(f32)
    scale = lax.rsqrt(jnp.mean(own * own, axis=-1, keepdims=True) + epsilon)
    normed = (own * scale * vm.mix_gain[...]).astype(bf16)
    packed = folded(normed.astype(f32), fold1)
    src1[...] = packed
    land1[me] = packed
    pl.semaphore_wait(barrier, n - 1)
    rows1 = spread(0, 0, src1, land1)

    lane = lax.broadcasted_iota(jnp.int32, (rows, 128), 1)
    ids = vm.expert_ids[...]
    chosen = jnp.zeros((rows, 128), f32)
    for k in range(ids.shape[1]):
        chosen = jnp.where(lane == ids[:, k : k + 1], 1.0, chosen)
    for place in range(n):
        for row in range(rows):
            extra[place, rows : rows + 1, row * col_width : (row + 1) * col_width] = own[
                row : row + 1, place * col_width : (place + 1) * col_width
            ]
    need(loads.step_t, loads.step_bias, loads.decay_log, loads.decay_shift, loads.skip_scale)
    raw = dot_t(normed, vm.step_t[...]) + vm.step_bias[...]
    step_size = jnp.maximum(raw, 0.0) + jnp.log1p(jnp.exp(-jnp.abs(raw)))
    decay = jnp.exp(vm.decay_shift[...] - step_size * jnp.exp(vm.decay_log[...]))
    skip = vm.skip_scale[...]
    low_half = lax.broadcasted_iota(jnp.int32, (rows, 128), 1) < head_dim
    for pair in range(heads // 2):
        at = slice(pair * 128, (pair + 1) * 128)
        first = jnp.broadcast_to(step_size[:, 2 * pair : 2 * pair + 1], (rows, 128))
        second = jnp.broadcast_to(step_size[:, 2 * pair + 1 : 2 * pair + 2], (rows, 128))
        step_x[:, at] = jnp.where(low_half, first, second)
        first = jnp.broadcast_to(skip[:, 2 * pair : 2 * pair + 1], (1, 128))
        second = jnp.broadcast_to(skip[:, 2 * pair + 1 : 2 * pair + 2], (1, 128))
        skip_x[:, at] = jnp.where(low_half[0:1], first, second)
    for row in range(rows):
        spread_row = jnp.broadcast_to(jnp.concatenate([decay[row : row + 1]] * 2, axis=1), (128, 128))
        turned = spread_row.T
        for group in range(groups):
            decay_col[row * groups + group] = turned[group * per_group : (group + 1) * per_group]

    need(loads.conv_window, loads.conv_taps, loads.conv_bias)
    taps = vm.conv_taps[...].astype(f32)
    for row in range(rows):
        old = vm.conv_window[row].astype(f32)
        base[row : row + 1] = (
            jnp.sum(old * taps[:3], axis=0, keepdims=True) + vm.conv_bias[...]
        )
        window[row, 0:2] = old[1:3]

    need(loads.write_t, loads.read_t)
    vec_proj[...] = jnp.concatenate([vm.write_t[...], vm.read_t[...]], axis=0).T
    unfolded(land1, me, 1, x_all)
    take1 = lambda owner, kind: unfolded(land1, owner, kind, x_all)
    finish(collect(0, 0, land1, rows1, take1), take1)
    need(loads.gate_proj, loads.input_proj)
    x_low[...] = x_all[...].reshape(x_low.shape).astype(bf16)
    p_all[:, :gate_cols] = in_order(matmul(x_low[...], vm.input_proj[...]))
    p_all[:, gate_cols:] = in_order(matmul(x_low[...], vec_proj[...]))
    own_part = lax.broadcasted_iota(jnp.int32, extra.shape[1:], 0) < rows
    for place in range(n):
        src2[place] = jnp.where(own_part, p_all[4 * place : 4 * place + 4], extra[place]).astype(bf16)
    scatter(1, src2, land2, part_sem.at[0, me])
    land2[me] = src2[me]
    gate_all[...] = in_order(matmul(x_low[...], vm.gate_proj[...]))
    ends = jnp.concatenate([chosen[0:1], chosen[2:3]], axis=1)
    ends = jnp.broadcast_to(ends, (rows + 1, ends.shape[1]))
    own_part = lax.broadcasted_iota(jnp.int32, ends.shape, 0) < rows
    for place in range(n):
        src_g[place] = jnp.where(own_part, gate_all[4 * place : 4 * place + 4], ends).astype(bf16)
    scatter(2, src_g, land_g, whole_sem.at[0])
    land_g[me] = src_g[me]

    need(loads.ssm_state)

    def decay_group(at, carry):
        columns = decay_col[at]
        for head in range(per_group):
            part = slice(head * head_dim, (head + 1) * head_dim)
            value = vm.ssm_state[at, part] * columns[head : head + 1]
            next_state[at, part] = value
        decayed[at] = next_state[at].T.astype(bf16)
        return carry

    lax.fori_loop(0, rows * groups, decay_group, 0)

    half = vec_cols
    for place in range(0, n, 2):
        last = []
        for one in (place, place + 1):
            arrived(0, land2, one)
            whole = land2[one].astype(f32)
            piece = whole[0:rows]
            fresh[:, one * gate_cols : (one + 1) * gate_cols] = piece[:, :gate_cols]
            last.append(piece[:, gate_cols:])
            for row in range(rows):
                h_all[4 * one + row : 4 * one + row + 1] = whole[
                    rows : rows + 1, row * col_width : (row + 1) * col_width
                ]
        low = lax.broadcasted_iota(jnp.int32, last[0].shape, 1) < half
        at = slice(inner + place * half, inner + (place + 2) * half)
        fresh[:, at] = jnp.where(low, last[0], pltpu.roll(last[1], half, 1))
        at = slice(at.start + groups * state, at.stop + groups * state)
        fresh[:, at] = jnp.where(low, pltpu.roll(last[0], half, 1), last[1])
    convolved = silu(base[...] + fresh[...] * taps[3:4])
    head_input = convolved[:, :inner]
    xv[...] = head_input
    for group in range(groups):
        at = slice(inner + group * state, inner + (group + 1) * state)
        write = convolved[:, at]
        read = convolved[:, at.start + groups * state : at.stop + groups * state]
        wv[group] = write
        rv[group] = read
    def mix(group):
        high, low = split2(rv[group])
        for row in range(rows):
            left = jnp.concatenate([high[row : row + 1], low[row : row + 1]], axis=0)
            both = matmul(left, decayed[row * groups + group])
            y_all[row : row + 1, group * span : (group + 1) * span] = both[0:1] + both[1:2]

    def gated(group):
        at = slice(group * span, (group + 1) * span)
        overlap = jnp.sum(wv[group] * rv[group], axis=1, keepdims=True)
        mixed = y_all[:, at] + xv[:, at] * (step_x[:, at] * overlap + skip_x[:, at])
        mixed = mixed.astype(bf16).astype(f32) * silu(cols[:, at])
        mixed = mixed * lax.rsqrt(jnp.mean(mixed * mixed, axis=-1, keepdims=True) + epsilon)
        y_all[:, at] = mixed * vm.group_gain[:, at]

    def share(part):
        packed = folded(y_all[:, part * half_inner : (part + 1) * half_inner], fold3)
        src3[part] = packed
        land3[part, me] = packed
        return spread(3 + part, 1 + part, src3.at[part], land3.at[part])

    half_inner = inner // 2
    for group in range(groups // 2):
        mix(group)
    need(loads.group_gain)
    arrived_all(0, land_g)
    for place in range(n):
        whole = land_g[place].astype(f32)
        cols[:, place * gate_cols : (place + 1) * gate_cols] = whole[0:rows]
        flag0[place : place + 1] = whole[rows : rows + 1, :128]
        flag2[place : place + 1] = whole[rows : rows + 1, 128:]
    for group in range(groups // 2):
        gated(group)
    rows3 = [share(0)]
    for group in range(groups // 2, groups):
        mix(group)
        gated(group)
    rows3.append(share(1))

    for group in range(groups):
        at = slice(group * span, (group + 1) * span)
        high, low = split2(xv[:, at] * step_x[:, at])
        left = jnp.concatenate([high.astype(f32), low.astype(f32), high.astype(f32)], axis=0).astype(bf16)
        w_high, w_low = split2(wv[group])
        right = jnp.concatenate([w_high.astype(f32), w_high.astype(f32), w_low.astype(f32)], axis=0)
        owner = lax.rem(lax.broadcasted_iota(jnp.int32, right.shape, 0), rows)
        for row in range(rows):
            picked = jnp.where(owner == row, right, 0.0).astype(bf16)
            place = row * groups + group
            next_state[place] = next_state[place] + dot_0(left, picked)
    for row in range(rows):
        window[row, 2:3] = fresh[row : row + 1]
        next_window[row] = window[row].astype(bf16)

    slot_row = lax.broadcasted_iota(jnp.int32, (2 * n, total), 0)
    slot_lane = lax.broadcasted_iota(jnp.int32, (2 * n, total), 1)
    first_row = (slot_row // 2) * rows
    even = slot_row % 2 == 0
    outer = jnp.where(even, first_row, first_row + 2)
    whose = lax.broadcasted_iota(jnp.int32, (2 * n, n), 1) == lax.broadcasted_iota(jnp.int32, (2 * n, n), 0) // 2
    whose = jnp.where(whose, 1.0, 0.0).astype(bf16)
    even_row = lax.broadcasted_iota(jnp.int32, (2 * n, 128), 0) % 2 == 0
    flag = jnp.where(
        even_row, matmul(whose, flag0[...].astype(bf16)), matmul(whose, flag2[...].astype(bf16))
    )
    flag = jnp.where(lax.broadcasted_iota(jnp.int32, flag.shape, 1) == me, flag, 0.0)
    flag = jnp.sum(flag, axis=1, keepdims=True)
    source_row = jnp.where(flag > 0.5, outer, first_row + 1)
    select = jnp.where(slot_lane == source_row, 1.0, 0.0).astype(bf16)

    take3 = [lambda owner, kind, part=part: unfolded(land3.at[part], owner, kind, g_all.at[part]) for part in range(2)]
    passed3 = []
    for part in range(2):
        take3[part](me, 1)
        passed3.append(collect(3 + part, 1 + part, land3.at[part], rows3[part], take3[part]))
    need(loads.out_proj)
    resid_f = jnp.zeros(h_all.shape, f32)
    for part in range(2):
        finish(passed3[part], take3[part])
        g_low[...] = g_all[part].reshape(g_low.shape).astype(bf16)
        resid_f = resid_f + matmul(g_low[...], vm.out_proj[part * half_inner : (part + 1) * half_inner])
    need(loads.shared_gate, loads.shared_up, loads.ffn_gain)
    resid_f = in_order(resid_f) + h_all[...]
    for place in range(n):
        part48[place * rows : (place + 1) * rows] = resid_f[4 * place : 4 * place + rows]
    resid_part = part48[...].astype(bf16)
    src4[...] = resid_part
    land4[me] = resid_part
    rows4 = spread(5, 3, src4, land4)
    gain_part = vm.ffn_gain[:, pl.ds(pl.multiple_of(me * col_width, col_width), col_width)]
    shared_part = (resid_part.astype(f32) * gain_part).astype(bf16)
    slots[:, :shared_units] = matmul(shared_part, vm.shared_gate[...])
    slots[:, shared_units:] = matmul(shared_part, vm.shared_up[...])
    for place in range(n):
        src5[place] = folded(slots[place * rows : (place + 1) * rows], fold5.at[place])
    scatter(6, src5, land5, whole_sem.at[1])
    land5[me] = src5[me]

    need(loads.expert_gate, loads.expert_up, loads.expert_down)
    acc_gate[...] = jnp.zeros_like(acc_gate)
    acc_up[...] = jnp.zeros_like(acc_up)
    squares = [jnp.zeros((total, col_width), f32)]

    def add_block(owner, kind=0):
        piece = land4[owner].astype(f32)
        squares[0] = squares[0] + piece * piece
        at = pl.ds(pl.multiple_of(owner * col_width, col_width), col_width)
        scaled = (piece * vm.ffn_gain[:, at]).astype(bf16)
        acc_gate[...] += matmul(scaled, vm.expert_gate[at])
        acc_up[...] += matmul(scaled, vm.expert_up[at])

    add_block(me)
    finish(collect(5, 3, land4, rows4, add_block), add_block)
    scale_all = lax.rsqrt(jnp.sum(squares[0], axis=1, keepdims=True) / width + epsilon)
    hidden_units = (silu(acc_gate[...] * scale_all) * (acc_up[...] * scale_all)).astype(bf16)
    served = matmul(select, hidden_units).astype(bf16)
    half_width = width // 2
    for part in range(2):
        served_f[...] = matmul(served, vm.expert_down[:, part * half_width : (part + 1) * half_width])
        for place in range(n):
            src6[part, place] = served_f[2 * place : 2 * place + 2].astype(bf16)
        scatter(7 + part, src6.at[part], land6.at[part], part_sem.at[1, me] if part else whole_sem.at[2])
        land6[part, me] = src6[part, me]

    need(loads.router_t, loads.shared_down)
    own_row = lax.broadcasted_iota(jnp.int32, (rows, total), 0) + me * rows
    pick = jnp.where(lax.broadcasted_iota(jnp.int32, (rows, total), 1) == own_row, 1.0, 0.0).astype(bf16)
    for place in range(n):
        at = slice(place * col_width, (place + 1) * col_width)
        y_all[:, at] = matmul(pick, land4[place])
    resid_own = y_all[:, :width]
    norm_scale = lax.rsqrt(jnp.mean(resid_own * resid_own, axis=-1, keepdims=True) + epsilon)
    routed_own = (resid_own * norm_scale * vm.ffn_gain[...]).astype(bf16)
    scores = 1.0 / (1.0 + jnp.exp(-dot_t(routed_own, vm.router_t[...])))
    kept = chosen[:, :n]
    scores = jnp.where(kept > 0.5, scores, 0.0)
    weights = routed_scale * scores / jnp.sum(scores, axis=1, keepdims=True)
    outer_w = jnp.concatenate([weights[0:1], weights[2:3]], axis=0)
    middle = weights[1:2]
    inner_w = jnp.concatenate([middle * (1.0 - kept[0:1]), middle * kept[0:1]], axis=0)
    shared = jnp.zeros(fold5.shape[1:], f32)
    arrived_all(1, land5)
    for place in range(n):
        shared = shared + land5[place].astype(f32)
    wide = shared.shape[1]
    rest = wide // rows
    cols[:, :wide] = shared[0:rows]
    for row in range(rows):
        cols[row : row + 1, wide : wide + rest] = shared[rows : rows + 1, row * rest : (row + 1) * rest]
    shared = cols[:, : wide + rest] * norm_scale
    shared_hidden = (silu(shared[:, :shared_units]) * shared[:, shared_units:]).astype(bf16)
    start = resid_own + matmul(shared_hidden, vm.shared_down[...])
    y_all[:, :width] = start
    for part in range(2):
        ends = jnp.zeros((2, half_width), f32)
        mid = jnp.zeros((2, half_width), f32)
        if part == 0:
            arrived_all(2, land6.at[0])
        for place in range(n):
            if part:
                arrived(1, land6.at[1], place)
            piece = land6[part, place].astype(f32)
            ends = ends + piece * outer_w[:, place : place + 1]
            mid = mid + piece * inner_w[:, place : place + 1]
        at = slice(part * half_width, (part + 1) * half_width)
        xv[0:1, at] = ends[0:1]
        xv[1:2, at] = mid[0:1] + mid[1:2]
        xv[2:3, at] = ends[1:2]
    layer_out[...] = (y_all[:, :width] + xv[:, :width]).astype(bf16)
    for phase, landed in blocks:
        all_blocks(landed, send_sem.at[phase], whole_sem.at[0]).wait_send()


def store_kernel(layer_out, next_state, next_window, layer_hbm, state_hbm, window_hbm, sems):
    for at in range(next_state.shape[0]):
        pltpu.make_async_copy(next_state.at[at], state_hbm.at[at], sems.at[0]).start()
    small = [
        pltpu.make_async_copy(layer_out, layer_hbm, sems.at[1]),
        pltpu.make_async_copy(next_window, window_hbm, sems.at[2]),
    ]
    for one in small:
        one.start()
    for one in small:
        one.wait()
    pltpu.make_async_copy(next_state, state_hbm, sems.at[0]).wait()


def one_kernel(*args):
    named = Args(*args)
    n = lax.axis_size("ep")
    rows, width = named.hidden.shape
    inner = named.gate_proj.shape[1] * n
    total = n * rows
    heads = named.step_bias.shape[0]
    flat = lambda one: one.reshape(1, -1)
    named = named._replace(
        write_t=named.write_t.T,
        read_t=named.read_t.T,
        step_t=named.step_t.T,
        router_t=named.router_t.T,
        step_bias=flat(named.step_bias),
        decay_log=flat(named.decay_log),
        skip_scale=flat(named.skip_scale),
        conv_bias=flat(named.conv_bias),
        mix_gain=flat(named.mix_gain),
        group_gain=flat(named.group_gain),
        ffn_gain=flat(named.ffn_gain),
        expert_gate=named.expert_gate[0],
        expert_up=named.expert_up[0],
        expert_down=named.expert_down[0],
    )
    state_shape = named.ssm_state.shape
    span = inner // GROUPS
    named = named._replace(ssm_state=named.ssm_state.reshape(rows * GROUPS, span, STATE))
    conv_dim = named.conv_bias.shape[1]
    cols = 2 * named.gate_proj.shape[1] + 2 * named.write_t.shape[0]
    gate_cols = named.gate_proj.shape[1]
    col_width = named.out_proj.shape[1]
    shared_units = named.shared_gate.shape[1]
    bf16, f32 = jnp.bfloat16, jnp.float32
    V = pltpu.VMEM
    scratch = [V(one.shape, one.dtype) for one in named]
    units = 2 * shared_units
    scratch += [
        V((4, width * 3 // 4), bf16), V((n, 4, width * 3 // 4), bf16),
        V((n, 4, cols - gate_cols), bf16), V((n, 4, cols - gate_cols), bf16),
        V((n, 4, gate_cols), bf16), V((n, 4, gate_cols), bf16),
        V((2, 4, inner * 3 // 8), bf16), V((2, n, 4, inner * 3 // 8), bf16),
        V((total, col_width), bf16), V((n, total, col_width), bf16),
        V((n, 4, units * 3 // 4), bf16), V((n, 4, units * 3 // 4), bf16),
        V((2, n, 2, width // 2), bf16), V((2, n, 2, width // 2), bf16),
        V((4, width * 3 // 4), f32), V((4, inner * 3 // 8), f32), V((n, 4, units * 3 // 4), f32),
        V((n // 2, 8, width), f32), V((n * 4, width), bf16), V((n * 4, cols - gate_cols), f32),
        V((n * 4, gate_cols), f32), V((n, 4, cols - gate_cols), f32),
        V((2, n // 2, 8, inner // 2), f32), V((n * 4, inner // 2), bf16), V((n * 4, col_width), f32),
        V((n, 128), f32), V((n, 128), f32), V((total, col_width), f32),
        V((total, shared_units), f32), V((total, shared_units), f32),
        V((rows, conv_dim), f32), V((rows, inner), f32), V((rows, inner), f32), V((rows, conv_dim), f32),
        V((rows, inner), f32), V((GROUPS, rows, STATE), f32), V((GROUPS, rows, STATE), f32),
        V((rows, inner), f32), V((1, inner), f32),
        V((rows * GROUPS, heads // GROUPS, 128), f32), V((rows * GROUPS, STATE, span), bf16),
        V((rows, 3, conv_dim), f32), V((total, units), f32), V((2 * n, width // 2), f32),
        V((width, cols - 2 * gate_cols), bf16),
        pltpu.SemaphoreType.DMA((len(named),)),
        pltpu.SemaphoreType.DMA((9,)),
        pltpu.SemaphoreType.DMA((4, n)),
        pltpu.SemaphoreType.DMA((2, n)),
        pltpu.SemaphoreType.DMA((3,)),
    ]
    layer_out, next_state, next_window = pl.pallas_call(
        functools.partial(layer_kernel, n, rows),
        out_shape=(
            pltpu.VMEM((rows, width), bf16),
            pltpu.VMEM(named.ssm_state.shape, f32),
            pltpu.VMEM(named.conv_window.shape, bf16),
        ),
        in_specs=[pl.BlockSpec(memory_space=pltpu.HBM)] * len(named),
        out_specs=tuple(pl.BlockSpec(memory_space=pltpu.VMEM) for _ in range(3)),
        scratch_shapes=scratch,
        compiler_params=pltpu.CompilerParams(
            collective_id=0, has_side_effects=True, vmem_limit_bytes=36 * 1024 * 1024
        ),
    )(*[pltpu.with_memory_space_constraint(one, pltpu.HBM) for one in named])
    outs = (layer_out, next_state, next_window)
    layer_out, next_state, next_window = pl.pallas_call(
        store_kernel,
        out_shape=tuple(jax.ShapeDtypeStruct(one.shape, one.dtype) for one in outs),
        in_specs=[pl.BlockSpec(memory_space=pltpu.VMEM)] * 3,
        out_specs=tuple(pl.BlockSpec(memory_space=pltpu.HBM) for _ in range(3)),
        scratch_shapes=[pltpu.SemaphoreType.DMA((3,))],
        compiler_params=pltpu.CompilerParams(vmem_limit_bytes=1024 * 1024),
    )(*outs)
    return layer_out, next_state.reshape(state_shape), next_window


def fits(args):
    named = Args(*args)
    n = lax.axis_size("ep")
    return (
        named.hidden.shape[0] == 3
        and n & (n - 1) == 0
        and 2 <= n <= 128
        and named.hidden.shape[1] % 512 == 0
        and named.gate_proj.shape[1] == 256
        and named.gate_proj.shape[0] * 2 == named.group_gain.shape[0]
        and named.expert_gate.shape[2] == named.shared_gate.shape[1]
        and named.shared_gate.shape[1] % 256 == 0
        and named.hidden.shape[1] <= named.group_gain.shape[0]
        and named.out_proj.shape[1] == 128
        and named.gate_proj.shape[1] % 128 == 0
        and named.write_t.shape[1] == 64
        and named.expert_gate.shape[0] == 1
        and named.router_t.shape[1] == n
        and HEAD_DIM * 2 == 128
    )


def body(*args):
    return one_kernel(*args) if fits(args) else shards(*args)


def solution(mesh):
    placed = (
        P(("grp", "ep"), None),
        P(("grp", "ep"), None, None),
        P(("grp", "ep"), None, None, None),
        P(None, "ep"),
        P(None, "ep"),
        P(None, "ep"),
        P(None, "ep"),
        P(),
        P(),
        P(),
        P(("grp", "ep"), None),
        P(),
        P(),
        P(),
        P(),
        P(),
        P(None, "ep"),
        P(),
        P(),
        P(("grp", "ep"), None),
        P("ep", None, None),
        P("ep", None, None),
        P("ep", None, None),
        P("ep", None),
        P("ep", None),
        P(),
    )
    return jax.shard_map(
        body,
        mesh=mesh,
        in_specs=placed,
        out_specs=(
            P(("grp", "ep"), None),
            P(("grp", "ep"), None, None, None),
            P(("grp", "ep"), None, None),
        ),
        check_vma=False,
    )
```

```python
import functools
import typing

import jax
import jax.numpy as jnp
from jax import lax
from jax.experimental import pallas as pl
from jax.experimental.pallas import tpu as pltpu
from jax.sharding import PartitionSpec as P

HEAD_DIM = 64
GROUPS = 8
STATE = 128


epsilon = 1e-06
routed_scale = 2.5


def row_scale(values):
    return lax.rsqrt(jnp.mean(values * values, axis=-1, keepdims=True) + epsilon)


def matmul(left, right):
    return jnp.dot(left, right, preferred_element_type=jnp.float32)


def expert_result(rows_in, weight_gate, weight_up, weight_down):
    expert_hidden = (jax.nn.silu(matmul(rows_in, weight_gate)) * matmul(rows_in, weight_up)).astype(
        jnp.bfloat16
    )
    return matmul(expert_hidden, weight_down).astype(jnp.bfloat16)


def exchange_kernel(n, spread, source, landed, send_sem, recv_sem, own_sem):
    me = lax.axis_index("ep")
    barrier = pltpu.get_barrier_semaphore()
    for step in range(1, n):
        pl.semaphore_signal(
            barrier, inc=1, device_id={"ep": lax.rem(me + step, n)}, device_id_type=pl.DeviceIdType.MESH
        )
    own = pltpu.make_async_copy(source if spread else source.at[me], landed.at[me], own_sem)
    own.start()
    pl.semaphore_wait(barrier, n - 1)
    copies = []
    for step in range(1, n):
        target = lax.rem(me + step, n)
        copy = pltpu.make_async_remote_copy(
            src_ref=source if spread else source.at[target],
            dst_ref=landed.at[me],
            send_sem=send_sem.at[step],
            recv_sem=recv_sem.at[step],
            device_id={"ep": target},
            device_id_type=pl.DeviceIdType.MESH,
        )
        copy.start()
        copies.append(copy)
    own.wait()
    for copy in copies:
        copy.wait()


def send(source, shape, spread, ident):
    n = shape[0]
    return pl.pallas_call(
        functools.partial(exchange_kernel, n, spread),
        out_shape=jax.ShapeDtypeStruct(shape, source.dtype),
        in_specs=[pl.BlockSpec(memory_space=pltpu.VMEM)],
        out_specs=pl.BlockSpec(memory_space=pltpu.VMEM),
        scratch_shapes=[
            pltpu.SemaphoreType.DMA((n,)),
            pltpu.SemaphoreType.DMA((n,)),
            pltpu.SemaphoreType.DMA,
        ],
        compiler_params=pltpu.CompilerParams(collective_id=ident, has_side_effects=True),
    )(source)


def exchange(blocks, ident):
    return send(blocks, blocks.shape, False, ident)


def gather(block, ident):
    return send(block, (lax.axis_size("ep"),) + block.shape, True, ident)


def transposed(left, right):
    return lax.dot_general(left, right, (((1,), (1,)), ((), ())), preferred_element_type=jnp.float32)


def state_kernel(per_group, decay, inputs, write, read, carried, updated, mixed):
    row, part = pl.program_id(0), pl.program_id(1)
    heads = carried.shape[1]
    scaled = inputs[0, 0]
    lane = lax.broadcasted_iota(jnp.int32, scaled.shape, 1)
    total = jnp.zeros(scaled.shape, jnp.float32)
    entries = carried.shape[3]
    head_dim = carried.shape[2]
    for group in range(heads // per_group):
        write_row = write[0, 0, group : group + 1]
        spread = jnp.broadcast_to(read[0, 0, group : group + 1], (entries, entries))
        spread_high = spread.astype(jnp.bfloat16)
        spread_low = (spread - spread_high.astype(jnp.float32)).astype(jnp.bfloat16)
        pieces = []
        for head in range(group * per_group, (group + 1) * per_group):
            fresh = (
                carried[0, head] * decay[row, part * heads + head]
                + scaled[:, head : head + 1] * write_row
            )
            updated[0, head] = fresh
            pieces.append(fresh)
        stacked = jnp.concatenate(pieces, axis=0)
        high = stacked.astype(jnp.bfloat16)
        low = (stacked - high.astype(jnp.float32)).astype(jnp.bfloat16)
        columns = transposed(high, spread_high) + transposed(low, spread_high) + transposed(high, spread_low)
        for place in range(per_group):
            head = group * per_group + place
            column = columns[place * head_dim : (place + 1) * head_dim, :heads]
            total = jnp.where(lane == head, column, total)
    mixed[0, 0] = total


def state_step(state, decay_rate, scaled, write_vec, read_vec):
    rows, head_count, head_dim, entries = state.shape
    groups = write_vec.shape[1]
    parts = 2
    heads = head_count // parts
    inputs = scaled.reshape(rows, parts, heads, head_dim).transpose(0, 1, 3, 2)
    vec_shape = (rows, parts, groups // parts, entries)
    part_spec = lambda *dims: pl.BlockSpec((1, 1) + dims, lambda row, part: (row, part, 0, 0))
    state_spec = pl.BlockSpec((1, heads, head_dim, entries), lambda row, part: (row, part, 0, 0))
    next_state, mixed = pl.pallas_call(
        functools.partial(state_kernel, head_count // groups),
        grid=(rows, parts),
        out_shape=(
            jax.ShapeDtypeStruct(state.shape, jnp.float32),
            jax.ShapeDtypeStruct(inputs.shape, jnp.float32),
        ),
        in_specs=[
            pl.BlockSpec(memory_space=pltpu.SMEM),
            part_spec(head_dim, heads),
            part_spec(groups // parts, entries),
            part_spec(groups // parts, entries),
            state_spec,
        ],
        out_specs=(state_spec, part_spec(head_dim, heads)),
    )(decay_rate, inputs, write_vec.reshape(vec_shape), read_vec.reshape(vec_shape), state)
    return next_state, mixed.transpose(0, 1, 3, 2).reshape(rows, head_count, head_dim)


def shards(
    hidden,
    conv_window,
    ssm_state,
    gate_proj,
    input_proj,
    write_proj,
    read_proj,
    step_proj,
    step_bias,
    decay_log,
    decay_shift,
    skip_scale,
    conv_taps,
    conv_bias,
    mix_gain,
    group_gain,
    out_proj,
    ffn_gain,
    router,
    expert_ids,
    expert_gate,
    expert_up,
    expert_down,
    shared_gate,
    shared_up,
    shared_down,
):
    local_rows = hidden.shape[0]
    device_index = lax.axis_index("ep")
    width = hidden.shape[1]
    first_row = device_index * local_rows
    gathered = gather(hidden, 0).reshape(-1, width)
    gathered_wide = gathered.astype(jnp.float32)
    normed = (gathered_wide * row_scale(gathered_wide) * mix_gain).astype(jnp.bfloat16)
    parts = [matmul(normed, proj).astype(jnp.bfloat16) for proj in (gate_proj, input_proj, write_proj, read_proj)]
    outbound = jnp.concatenate(parts, axis=1)
    arrived = exchange(outbound.reshape(-1, local_rows, outbound.shape[1]), 1)
    rows, offset = [], 0
    for part in parts:
        piece = arrived[:, :, offset : offset + part.shape[1]]
        rows.append(piece.transpose(1, 0, 2).reshape(local_rows, -1))
        offset += part.shape[1]
    gate_rows, input_rows, write_rows, read_rows = rows
    hidden_wide = hidden.astype(jnp.float32)
    normed_local = (hidden_wide * row_scale(hidden_wide) * mix_gain).astype(jnp.bfloat16)
    step_raw = matmul(normed_local, step_proj)
    inner_width = gate_rows.shape[1]
    state_span = GROUPS * STATE
    head_count = step_bias.shape[0]
    fresh_row = jnp.concatenate([input_rows, write_rows, read_rows], axis=1)
    window = jnp.concatenate([conv_window, fresh_row[:, None, :]], axis=1)
    convolved = jax.nn.silu(
        jnp.sum(window.astype(jnp.float32) * conv_taps.astype(jnp.float32)[None], axis=1)
        + conv_bias
    )
    head_input = convolved[:, :inner_width].reshape(local_rows, head_count, HEAD_DIM)
    write_vec = convolved[:, inner_width : inner_width + state_span].reshape(
        local_rows, GROUPS, STATE
    )
    read_vec = convolved[:, inner_width + state_span :].reshape(local_rows, GROUPS, STATE)
    step_size = jax.nn.softplus(step_raw + step_bias)
    decay_rate = jnp.exp(decay_shift - step_size * jnp.exp(decay_log))
    next_state, mixed_out = state_step(
        ssm_state, decay_rate, step_size[:, :, None] * head_input, write_vec, read_vec
    )
    mixed_out = mixed_out + skip_scale[None, :, None] * head_input
    mixed_out = mixed_out.reshape(local_rows, inner_width).astype(jnp.bfloat16)
    gated_out = mixed_out.astype(jnp.float32) * jax.nn.silu(gate_rows.astype(jnp.float32))
    blocks = gated_out.reshape(local_rows, GROUPS, -1)
    gated_out = ((blocks * row_scale(blocks)).reshape(local_rows, inner_width) * group_gain).astype(
        jnp.bfloat16
    )
    col_width = out_proj.shape[1]
    resid_cols = lax.dynamic_slice_in_dim(gathered_wide, device_index * col_width, col_width, 1)
    resid_part = (
        resid_cols + matmul(gather(gated_out, 2).reshape(-1, inner_width), out_proj)
    ).astype(jnp.bfloat16)
    resid_all = gather(resid_part, 3).transpose(1, 0, 2).reshape(-1, width)
    gain_part = lax.dynamic_slice_in_dim(ffn_gain, device_index * col_width, col_width, 0)
    shared_part = (resid_part.astype(jnp.float32) * gain_part).astype(jnp.bfloat16)
    shared_pre = jnp.concatenate(
        [matmul(shared_part, shared_gate), matmul(shared_part, shared_up)], axis=1
    ).astype(jnp.bfloat16)
    resid_all_wide = resid_all.astype(jnp.float32)
    scale_all = row_scale(resid_all_wide)
    routed_all = (resid_all_wide * scale_all * ffn_gain).astype(jnp.bfloat16)
    result = expert_result(routed_all, expert_gate[0], expert_up[0], expert_down[0])
    back = exchange(
        jnp.concatenate([result, shared_pre], axis=1).reshape(
            -1, local_rows, width + shared_pre.shape[1]
        ),
        4,
    ).astype(jnp.float32)
    resid_wide = lax.dynamic_slice_in_dim(resid_all_wide, first_row, local_rows, 0)
    norm_scale = lax.dynamic_slice_in_dim(scale_all, first_row, local_rows, 0)
    routed_in = lax.dynamic_slice_in_dim(routed_all, first_row, local_rows, 0)
    scores = jax.nn.sigmoid(matmul(routed_in, router))
    chosen = jnp.any(
        expert_ids[:, :, None] == jnp.arange(router.shape[1], dtype=jnp.int32)[None, None, :], axis=1
    )
    scores = jnp.where(chosen, scores, 0.0)
    weights = routed_scale * scores / jnp.sum(scores, axis=1, keepdims=True)
    routed = jnp.sum(back[:, :, :width] * weights.T[:, :, None], axis=0)
    shared_sum = jnp.sum(back[:, :, width:], axis=0)
    hidden_units = shared_down.shape[0]
    shared_hidden = (
        jax.nn.silu(norm_scale * shared_sum[:, :hidden_units])
        * (norm_scale * shared_sum[:, hidden_units:])
    ).astype(jnp.bfloat16)
    layer_out = (resid_wide + routed + matmul(shared_hidden, shared_down)).astype(jnp.bfloat16)
    return (layer_out, next_state, window[:, 1:])


def dot_t(left, right):
    return lax.dot_general(left, right, (((1,), (1,)), ((), ())), preferred_element_type=jnp.float32)


def dot_0(left, right):
    return lax.dot_general(left, right, (((0,), (0,)), ((), ())), preferred_element_type=jnp.float32)


def silu(v):
    return v / (1.0 + jnp.exp(-v))


def split2(v):
    high = v.astype(jnp.bfloat16)
    return high, (v - high.astype(jnp.float32)).astype(jnp.bfloat16)


class Args(typing.NamedTuple):
    hidden: typing.Any
    conv_window: typing.Any
    ssm_state: typing.Any
    gate_proj: typing.Any
    input_proj: typing.Any
    write_t: typing.Any
    read_t: typing.Any
    step_t: typing.Any
    step_bias: typing.Any
    decay_log: typing.Any
    decay_shift: typing.Any
    skip_scale: typing.Any
    conv_taps: typing.Any
    conv_bias: typing.Any
    mix_gain: typing.Any
    group_gain: typing.Any
    out_proj: typing.Any
    ffn_gain: typing.Any
    router_t: typing.Any
    expert_ids: typing.Any
    expert_gate: typing.Any
    expert_up: typing.Any
    expert_down: typing.Any
    shared_gate: typing.Any
    shared_up: typing.Any
    shared_down: typing.Any


def layer_kernel(n, rows, *refs):
    count = len(Args._fields)
    hbm = Args(*refs[:count])
    layer_out, next_state, next_window = refs[count : count + 3]
    vm = Args(*refs[count + 3 : 2 * count + 3])
    (
        src1, land1, src2, land2, src_g, land_g, src3, land3, src4, land4, src5, land5, src6, land6,
        fold1, fold3, fold5, x_all, x_low, p_all, gate_all, extra, g_all, g_low, h_all, flag0, flag2, part48,
        acc_gate, acc_up, base, cols, y_all, fresh, xv, wv, rv, step_x, skip_x,
        decay_col, decayed, window, slots, served_f, vec_proj,
        in_sem, send_sem, ring_sem, part_sem, whole_sem,
    ) = refs[2 * count + 3 :]
    me = lax.axis_index("ep")
    f32, bf16 = jnp.float32, jnp.bfloat16
    width = vm.hidden.shape[1]
    inner = cols.shape[1]
    total = n * rows
    heads = hbm.step_bias.shape[1]
    head_dim = inner // heads
    groups = GROUPS
    per_group = heads // groups
    span = inner // groups
    state = STATE
    gate_cols = hbm.gate_proj.shape[1]
    vec_cols = hbm.write_t.shape[0]
    col_width = hbm.out_proj.shape[1]
    shared_units = hbm.shared_gate.shape[1]

    def flipped(value):
        other = me
        bit = 1
        while bit < n:
            if value & bit:
                other = other + bit - 2 * bit * lax.rem(me // bit, 2)
            bit *= 2
        return other

    far_first = tuple(range(n - 1, 0, -1))
    partner = flipped(1)

    barrier = pltpu.get_barrier_semaphore()
    for step in far_first:
        pl.semaphore_signal(
            barrier, inc=1, device_id={"ep": flipped(step)}, device_id_type=pl.DeviceIdType.MESH
        )
    def load(name, at):
        return pltpu.make_async_copy(getattr(hbm, name), getattr(vm, name), in_sem.at[at])

    first = (
        "hidden",
        "mix_gain",
        "expert_ids",
        "write_t",
        "read_t",
        "step_t",
        "step_bias",
        "decay_log",
        "decay_shift",
        "skip_scale",
        "input_proj",
        "gate_proj",
        "conv_window",
        "conv_taps",
        "conv_bias",
        "ssm_state",
    )
    later = (
        "group_gain",
        "out_proj",
        "ffn_gain",
        "shared_gate",
        "shared_up",
        "expert_gate",
        "expert_up",
        "expert_down",
        "router_t",
        "shared_down",
    )
    loads = {name: load(name, at) for at, name in enumerate(first)}
    for one in loads.values():
        one.start()
    loads.update({name: load(name, at) for at, name in enumerate(later)})
    loads = Args(**loads)

    def need(*these):
        for one in these:
            one.wait()

    def remote(source, target_ref, sends, arrives, target):
        return pltpu.make_async_remote_copy(
            src_ref=source,
            dst_ref=target_ref,
            send_sem=sends,
            recv_sem=arrives,
            device_id={"ep": target},
            device_id_type=pl.DeviceIdType.MESH,
        )

    blocks = {}

    def drained(phase):
        if phase in blocks:
            all_blocks(blocks.pop(phase), send_sem.at[phase], whole_sem.at[0]).wait_send()

    def sends(phase, landed):
        drained(phase)
        blocks[phase] = landed
        return send_sem.at[phase]

    def all_blocks(landed, sem, arrives):
        many = landed.at[pl.ds(0, n - 1)]
        return remote(many, many, sem, arrives, partner)

    def spread(phase, ring, source, landed):
        sem = sends(phase, landed)
        out = {}
        for step in range(n - 2, -1, -2):
            out[step] = remote(source, landed.at[me], sem, ring_sem.at[ring, step], flipped(step + 1))
            out[step].start()
        return out

    def collect(phase, ring, landed, out, take):
        passed = [(partner, out[0])]
        for step in range(2, n, 2):
            out[step].wait_recv()
            owner = flipped(step + 1)
            block = landed.at[owner]
            one = remote(block, block, send_sem.at[phase], ring_sem.at[ring, step - 1], partner)
            one.start()
            passed.append((flipped(step), one))
            take(owner, 0)
        return passed

    def finish(passed, take):
        for owner, one in passed:
            one.wait_recv()
            take(owner, 0 if owner is partner else 1)

    def scatter(phase, source, landed, sem):
        sent = sends(phase, landed)
        for step in far_first:
            to = flipped(step)
            remote(source.at[to], landed.at[me], sent, sem, to).start()

    span_z = min(n, 4)

    def arrived(landed, place):
        def wait(many):
            some = landed.at[pl.ds(place, many)]
            remote(some, some, send_sem.at[0], part_sem.at[place // span_z], partner).wait_recv()

        @pl.when(me // span_z != place // span_z)
        def _():
            wait(span_z)

        @pl.when(me // span_z == place // span_z)
        def _():
            wait(span_z - 1)

    def arrived_all(which, landed):
        all_blocks(landed, send_sem.at[0], whole_sem.at[which]).wait_recv()

    def folded(value, buffer):
        wide = buffer.shape[1]
        rest = wide // rows
        buffer[0:rows] = value[:, :wide]
        for row in range(rows):
            buffer[rows : rows + 1, row * rest : (row + 1) * rest] = value[row : row + 1, wide:]
        return buffer[...].astype(bf16)

    def unfolded(landed, owner, kind, target):
        piece = landed[owner].astype(f32)
        wide = piece.shape[1]
        rest = wide // rows
        chip = owner // 2
        target[chip, 4 * kind : 4 * kind + rows, :wide] = piece[0:rows]
        for row in range(rows):
            target[chip, 4 * kind + row : 4 * kind + row + 1, wide:] = piece[
                rows : rows + 1, row * rest : (row + 1) * rest
            ]

    def in_order(value):
        tiles = value.reshape(n // 2, 8, value.shape[1])
        turned = jnp.concatenate([tiles[:, 4:], tiles[:, :4]], axis=1)
        return jnp.where(lax.rem(me, 2) == 1, tiles, turned).reshape(value.shape)

    need(loads.hidden, loads.mix_gain, loads.expert_ids)
    own = vm.hidden[...].astype(f32)
    scale = lax.rsqrt(jnp.mean(own * own, axis=-1, keepdims=True) + epsilon)
    normed = (own * scale * vm.mix_gain[...]).astype(bf16)
    packed = folded(normed.astype(f32), fold1)
    src1[...] = packed
    land1[me] = packed
    pl.semaphore_wait(barrier, n - 1)
    rows1 = spread(0, 0, src1, land1)

    lane = lax.broadcasted_iota(jnp.int32, (rows, 128), 1)
    ids = vm.expert_ids[...]
    chosen = jnp.zeros((rows, 128), f32)
    for k in range(ids.shape[1]):
        chosen = jnp.where(lane == ids[:, k : k + 1], 1.0, chosen)
    for place in range(n):
        for row in range(rows):
            extra[place, rows : rows + 1, row * col_width : (row + 1) * col_width] = own[
                row : row + 1, place * col_width : (place + 1) * col_width
            ]
    need(loads.step_t, loads.step_bias, loads.decay_log, loads.decay_shift, loads.skip_scale)
    raw = dot_t(normed, vm.step_t[...]) + vm.step_bias[...]
    step_size = jnp.maximum(raw, 0.0) + jnp.log1p(jnp.exp(-jnp.abs(raw)))
    decay = jnp.exp(vm.decay_shift[...] - step_size * jnp.exp(vm.decay_log[...]))
    skip = vm.skip_scale[...]
    low_half = lax.broadcasted_iota(jnp.int32, (rows, 128), 1) < head_dim
    for pair in range(heads // 2):
        at = slice(pair * 128, (pair + 1) * 128)
        first = jnp.broadcast_to(step_size[:, 2 * pair : 2 * pair + 1], (rows, 128))
        second = jnp.broadcast_to(step_size[:, 2 * pair + 1 : 2 * pair + 2], (rows, 128))
        step_x[:, at] = jnp.where(low_half, first, second)
        first = jnp.broadcast_to(skip[:, 2 * pair : 2 * pair + 1], (1, 128))
        second = jnp.broadcast_to(skip[:, 2 * pair + 1 : 2 * pair + 2], (1, 128))
        skip_x[:, at] = jnp.where(low_half[0:1], first, second)
    for row in range(rows):
        spread_row = jnp.broadcast_to(jnp.concatenate([decay[row : row + 1]] * 2, axis=1), (128, 128))
        turned = spread_row.T
        for group in range(groups):
            decay_col[row * groups + group] = turned[group * per_group : (group + 1) * per_group]

    need(loads.conv_window, loads.conv_taps, loads.conv_bias)
    taps = vm.conv_taps[...].astype(f32)
    for row in range(rows):
        old = vm.conv_window[row].astype(f32)
        base[row : row + 1] = (
            jnp.sum(old * taps[:3], axis=0, keepdims=True) + vm.conv_bias[...]
        )
        window[row, 0:2] = old[1:3]

    need(loads.write_t, loads.read_t)
    for name in later:
        getattr(loads, name).start()
    vec_proj[...] = jnp.concatenate([vm.write_t[...], vm.read_t[...]], axis=0).T
    unfolded(land1, me, 1, x_all)
    take1 = lambda owner, kind: unfolded(land1, owner, kind, x_all)
    finish(collect(0, 0, land1, rows1, take1), take1)
    need(loads.gate_proj, loads.input_proj)
    x_low[...] = x_all[...].reshape(x_low.shape).astype(bf16)
    p_all[:, :gate_cols] = in_order(matmul(x_low[...], vm.input_proj[...]))
    p_all[:, gate_cols:] = in_order(matmul(x_low[...], vec_proj[...]))
    own_part = lax.broadcasted_iota(jnp.int32, extra.shape[1:], 0) < rows
    for place in range(n):
        src2[place] = jnp.where(own_part, p_all[4 * place : 4 * place + 4], extra[place]).astype(bf16)
    scatter(1, src2, land2, part_sem.at[me // span_z])
    land2[me] = src2[me]
    gate_all[...] = in_order(matmul(x_low[...], vm.gate_proj[...]))
    ends = jnp.concatenate([chosen[0:1], chosen[2:3]], axis=1)
    ends = jnp.broadcast_to(ends, (rows + 1, ends.shape[1]))
    own_part = lax.broadcasted_iota(jnp.int32, ends.shape, 0) < rows
    for place in range(n):
        src_g[place] = jnp.where(own_part, gate_all[4 * place : 4 * place + 4], ends).astype(bf16)
    scatter(2, src_g, land_g, whole_sem.at[0])
    land_g[me] = src_g[me]

    need(loads.ssm_state)

    def decay_group(at, carry):
        columns = decay_col[at]
        for head in range(per_group):
            part = slice(head * head_dim, (head + 1) * head_dim)
            value = vm.ssm_state[at, part] * columns[head : head + 1]
            next_state[at, part] = value
        decayed[at] = next_state[at].T.astype(bf16)
        return carry

    lax.fori_loop(0, rows * groups, decay_group, 0)

    half = vec_cols
    for place in range(0, n, 2):
        last = []
        for one in (place, place + 1):
            if one % span_z == 0:
                arrived(land2, one)
            whole = land2[one].astype(f32)
            piece = whole[0:rows]
            fresh[:, one * gate_cols : (one + 1) * gate_cols] = piece[:, :gate_cols]
            last.append(piece[:, gate_cols:])
            for row in range(rows):
                h_all[4 * one + row : 4 * one + row + 1] = whole[
                    rows : rows + 1, row * col_width : (row + 1) * col_width
                ]
        low = lax.broadcasted_iota(jnp.int32, last[0].shape, 1) < half
        at = slice(inner + place * half, inner + (place + 2) * half)
        fresh[:, at] = jnp.where(low, last[0], pltpu.roll(last[1], half, 1))
        at = slice(at.start + groups * state, at.stop + groups * state)
        fresh[:, at] = jnp.where(low, pltpu.roll(last[0], half, 1), last[1])
    convolved = silu(base[...] + fresh[...] * taps[3:4])
    head_input = convolved[:, :inner]
    xv[...] = head_input
    for group in range(groups):
        at = slice(inner + group * state, inner + (group + 1) * state)
        write = convolved[:, at]
        read = convolved[:, at.start + groups * state : at.stop + groups * state]
        wv[group] = write
        rv[group] = read
    def mix(group):
        high, low = split2(rv[group])
        for row in range(rows):
            left = jnp.concatenate([high[row : row + 1], low[row : row + 1]], axis=0)
            both = matmul(left, decayed[row * groups + group])
            y_all[row : row + 1, group * span : (group + 1) * span] = both[0:1] + both[1:2]

    def gated(group):
        at = slice(group * span, (group + 1) * span)
        overlap = jnp.sum(wv[group] * rv[group], axis=1, keepdims=True)
        mixed = y_all[:, at] + xv[:, at] * (step_x[:, at] * overlap + skip_x[:, at])
        mixed = mixed.astype(bf16).astype(f32) * silu(cols[:, at])
        mixed = mixed * lax.rsqrt(jnp.mean(mixed * mixed, axis=-1, keepdims=True) + epsilon)
        y_all[:, at] = mixed * vm.group_gain[:, at]

    def share(part):
        packed = folded(y_all[:, part * half_inner : (part + 1) * half_inner], fold3)
        src3[part] = packed
        land3[part, me] = packed
        return spread(3 + part, part, src3.at[part], land3.at[part])

    half_inner = inner // 2
    for group in range(groups // 2):
        mix(group)
    need(loads.group_gain)
    arrived_all(0, land_g)
    for place in range(n):
        whole = land_g[place].astype(f32)
        cols[:, place * gate_cols : (place + 1) * gate_cols] = whole[0:rows]
        flag0[place : place + 1] = whole[rows : rows + 1, :128]
        flag2[place : place + 1] = whole[rows : rows + 1, 128:]
    for group in range(groups // 2):
        gated(group)
    rows3 = [share(0)]
    for group in range(groups // 2, groups):
        mix(group)
        gated(group)
    rows3.append(share(1))

    for group in range(groups):
        at = slice(group * span, (group + 1) * span)
        high, low = split2(xv[:, at] * step_x[:, at])
        left = jnp.concatenate([high.astype(f32), low.astype(f32), high.astype(f32)], axis=0).astype(bf16)
        w_high, w_low = split2(wv[group])
        right = jnp.concatenate([w_high.astype(f32), w_high.astype(f32), w_low.astype(f32)], axis=0)
        owner = lax.rem(lax.broadcasted_iota(jnp.int32, right.shape, 0), rows)
        for row in range(rows):
            picked = jnp.where(owner == row, right, 0.0).astype(bf16)
            place = row * groups + group
            next_state[place] = next_state[place] + dot_0(left, picked)
    for row in range(rows):
        window[row, 2:3] = fresh[row : row + 1]
        next_window[row] = window[row].astype(bf16)

    slot_row = lax.broadcasted_iota(jnp.int32, (2 * n, total), 0)
    slot_lane = lax.broadcasted_iota(jnp.int32, (2 * n, total), 1)
    first_row = (slot_row // 2) * rows
    even = slot_row % 2 == 0
    outer = jnp.where(even, first_row, first_row + 2)
    whose = lax.broadcasted_iota(jnp.int32, (2 * n, n), 1) == lax.broadcasted_iota(jnp.int32, (2 * n, n), 0) // 2
    whose = jnp.where(whose, 1.0, 0.0).astype(bf16)
    even_row = lax.broadcasted_iota(jnp.int32, (2 * n, 128), 0) % 2 == 0
    flag = jnp.where(
        even_row, matmul(whose, flag0[...].astype(bf16)), matmul(whose, flag2[...].astype(bf16))
    )
    flag = jnp.where(lax.broadcasted_iota(jnp.int32, flag.shape, 1) == me, flag, 0.0)
    flag = jnp.sum(flag, axis=1, keepdims=True)
    source_row = jnp.where(flag > 0.5, outer, first_row + 1)
    select = jnp.where(slot_lane == source_row, 1.0, 0.0).astype(bf16)

    take3 = [lambda owner, kind, part=part: unfolded(land3.at[part], owner, kind, g_all.at[part]) for part in range(2)]
    passed3 = []
    for part in range(2):
        take3[part](me, 1)
        passed3.append(collect(3 + part, part, land3.at[part], rows3[part], take3[part]))
    need(loads.out_proj)
    resid_f = jnp.zeros(h_all.shape, f32)
    for part in range(2):
        finish(passed3[part], take3[part])
        g_low[...] = g_all[part].reshape(g_low.shape).astype(bf16)
        resid_f = resid_f + matmul(g_low[...], vm.out_proj[part * half_inner : (part + 1) * half_inner])
    need(loads.shared_gate, loads.shared_up, loads.ffn_gain)
    resid_f = in_order(resid_f) + h_all[...]
    for place in range(n):
        part48[place * rows : (place + 1) * rows] = resid_f[4 * place : 4 * place + rows]
    resid_part = part48[...].astype(bf16)
    src4[...] = resid_part
    land4[me] = resid_part
    rows4 = spread(0, 2, src4, land4)
    gain_part = vm.ffn_gain[:, pl.ds(pl.multiple_of(me * col_width, col_width), col_width)]
    shared_part = (resid_part.astype(f32) * gain_part).astype(bf16)
    slots[:, :shared_units] = matmul(shared_part, vm.shared_gate[...])
    slots[:, shared_units:] = matmul(shared_part, vm.shared_up[...])
    for place in range(n):
        src5[place] = folded(slots[place * rows : (place + 1) * rows], fold5.at[place])
    scatter(1, src5, land5, whole_sem.at[0])
    land5[me] = src5[me]

    need(loads.expert_gate, loads.expert_up, loads.expert_down)
    acc_gate[...] = jnp.zeros_like(acc_gate)
    acc_up[...] = jnp.zeros_like(acc_up)
    squares = [jnp.zeros((total, col_width), f32)]

    def add_block(owner, kind=0):
        piece = land4[owner].astype(f32)
        squares[0] = squares[0] + piece * piece
        at = pl.ds(pl.multiple_of(owner * col_width, col_width), col_width)
        scaled = (piece * vm.ffn_gain[:, at]).astype(bf16)
        acc_gate[...] += matmul(scaled, vm.expert_gate[at])
        acc_up[...] += matmul(scaled, vm.expert_up[at])

    add_block(me)
    finish(collect(0, 2, land4, rows4, add_block), add_block)
    scale_all = lax.rsqrt(jnp.sum(squares[0], axis=1, keepdims=True) / width + epsilon)
    hidden_units = (silu(acc_gate[...] * scale_all) * (acc_up[...] * scale_all)).astype(bf16)
    served = matmul(select, hidden_units).astype(bf16)
    half_width = width // 2
    for part in range(2):
        served_f[...] = matmul(served, vm.expert_down[:, part * half_width : (part + 1) * half_width])
        for place in range(n):
            src6[part, place] = served_f[2 * place : 2 * place + 2].astype(bf16)
        scatter(2 + part, src6.at[part], land6.at[part], part_sem.at[me // span_z] if part else whole_sem.at[1])
        land6[part, me] = src6[part, me]

    need(loads.router_t, loads.shared_down)
    own_row = lax.broadcasted_iota(jnp.int32, (rows, total), 0) + me * rows
    pick = jnp.where(lax.broadcasted_iota(jnp.int32, (rows, total), 1) == own_row, 1.0, 0.0).astype(bf16)
    for place in range(n):
        at = slice(place * col_width, (place + 1) * col_width)
        y_all[:, at] = matmul(pick, land4[place])
    resid_own = y_all[:, :width]
    norm_scale = lax.rsqrt(jnp.mean(resid_own * resid_own, axis=-1, keepdims=True) + epsilon)
    routed_own = (resid_own * norm_scale * vm.ffn_gain[...]).astype(bf16)
    scores = 1.0 / (1.0 + jnp.exp(-dot_t(routed_own, vm.router_t[...])))
    kept = chosen[:, :n]
    scores = jnp.where(kept > 0.5, scores, 0.0)
    weights = routed_scale * scores / jnp.sum(scores, axis=1, keepdims=True)
    outer_w = jnp.concatenate([weights[0:1], weights[2:3]], axis=0)
    middle = weights[1:2]
    inner_w = jnp.concatenate([middle * (1.0 - kept[0:1]), middle * kept[0:1]], axis=0)
    shared = jnp.zeros(fold5.shape[1:], f32)
    arrived_all(0, land5)
    for place in range(n):
        shared = shared + land5[place].astype(f32)
    wide = shared.shape[1]
    rest = wide // rows
    cols[:, :wide] = shared[0:rows]
    for row in range(rows):
        cols[row : row + 1, wide : wide + rest] = shared[rows : rows + 1, row * rest : (row + 1) * rest]
    shared = cols[:, : wide + rest] * norm_scale
    shared_hidden = (silu(shared[:, :shared_units]) * shared[:, shared_units:]).astype(bf16)
    start = resid_own + matmul(shared_hidden, vm.shared_down[...])
    y_all[:, :width] = start
    for part in range(2):
        ends = jnp.zeros((2, half_width), f32)
        mid = jnp.zeros((2, half_width), f32)
        if part == 0:
            arrived_all(1, land6.at[0])
        for place in range(n):
            if part and place % span_z == 0:
                arrived(land6.at[1], place)
            piece = land6[part, place].astype(f32)
            ends = ends + piece * outer_w[:, place : place + 1]
            mid = mid + piece * inner_w[:, place : place + 1]
        at = slice(part * half_width, (part + 1) * half_width)
        xv[0:1, at] = ends[0:1]
        xv[1:2, at] = mid[0:1] + mid[1:2]
        xv[2:3, at] = ends[1:2]
    layer_out[...] = (y_all[:, :width] + xv[:, :width]).astype(bf16)
    for phase in tuple(blocks):
        drained(phase)


def store_kernel(layer_out, next_state, next_window, layer_hbm, state_hbm, window_hbm, sems):
    for at in range(next_state.shape[0]):
        pltpu.make_async_copy(next_state.at[at], state_hbm.at[at], sems.at[0]).start()
    small = [
        pltpu.make_async_copy(layer_out, layer_hbm, sems.at[1]),
        pltpu.make_async_copy(next_window, window_hbm, sems.at[2]),
    ]
    for one in small:
        one.start()
    for one in small:
        one.wait()
    pltpu.make_async_copy(next_state, state_hbm, sems.at[0]).wait()


def one_kernel(*args):
    named = Args(*args)
    n = lax.axis_size("ep")
    rows, width = named.hidden.shape
    inner = named.gate_proj.shape[1] * n
    total = n * rows
    heads = named.step_bias.shape[0]
    flat = lambda one: one.reshape(1, -1)
    named = named._replace(
        write_t=named.write_t.T,
        read_t=named.read_t.T,
        step_t=named.step_t.T,
        router_t=named.router_t.T,
        step_bias=flat(named.step_bias),
        decay_log=flat(named.decay_log),
        skip_scale=flat(named.skip_scale),
        conv_bias=flat(named.conv_bias),
        mix_gain=flat(named.mix_gain),
        group_gain=flat(named.group_gain),
        ffn_gain=flat(named.ffn_gain),
        expert_gate=named.expert_gate[0],
        expert_up=named.expert_up[0],
        expert_down=named.expert_down[0],
    )
    state_shape = named.ssm_state.shape
    span = inner // GROUPS
    named = named._replace(ssm_state=named.ssm_state.reshape(rows * GROUPS, span, STATE))
    conv_dim = named.conv_bias.shape[1]
    cols = 2 * named.gate_proj.shape[1] + 2 * named.write_t.shape[0]
    gate_cols = named.gate_proj.shape[1]
    col_width = named.out_proj.shape[1]
    shared_units = named.shared_gate.shape[1]
    bf16, f32 = jnp.bfloat16, jnp.float32
    V = pltpu.VMEM
    scratch = [V(one.shape, one.dtype) for one in named]
    units = 2 * shared_units
    scratch += [
        V((4, width * 3 // 4), bf16), V((n, 4, width * 3 // 4), bf16),
        V((n, 4, cols - gate_cols), bf16), V((n, 4, cols - gate_cols), bf16),
        V((n, 4, gate_cols), bf16), V((n, 4, gate_cols), bf16),
        V((2, 4, inner * 3 // 8), bf16), V((2, n, 4, inner * 3 // 8), bf16),
        V((total, col_width), bf16), V((n, total, col_width), bf16),
        V((n, 4, units * 3 // 4), bf16), V((n, 4, units * 3 // 4), bf16),
        V((2, n, 2, width // 2), bf16), V((2, n, 2, width // 2), bf16),
        V((4, width * 3 // 4), f32), V((4, inner * 3 // 8), f32), V((n, 4, units * 3 // 4), f32),
        V((n // 2, 8, width), f32), V((n * 4, width), bf16), V((n * 4, cols - gate_cols), f32),
        V((n * 4, gate_cols), f32), V((n, 4, cols - gate_cols), f32),
        V((2, n // 2, 8, inner // 2), f32), V((n * 4, inner // 2), bf16), V((n * 4, col_width), f32),
        V((n, 128), f32), V((n, 128), f32), V((total, col_width), f32),
        V((total, shared_units), f32), V((total, shared_units), f32),
        V((rows, conv_dim), f32), V((rows, inner), f32), V((rows, inner), f32), V((rows, conv_dim), f32),
        V((rows, inner), f32), V((GROUPS, rows, STATE), f32), V((GROUPS, rows, STATE), f32),
        V((rows, inner), f32), V((1, inner), f32),
        V((rows * GROUPS, heads // GROUPS, 128), f32), V((rows * GROUPS, STATE, span), bf16),
        V((rows, 3, conv_dim), f32), V((total, units), f32), V((2 * n, width // 2), f32),
        V((width, cols - 2 * gate_cols), bf16),
        pltpu.SemaphoreType.DMA((16,)),
        pltpu.SemaphoreType.DMA((5,)),
        pltpu.SemaphoreType.DMA((3, n - 1)),
        pltpu.SemaphoreType.DMA((max(1, n // 4),)),
        pltpu.SemaphoreType.DMA((2,)),
    ]
    layer_out, next_state, next_window = pl.pallas_call(
        functools.partial(layer_kernel, n, rows),
        out_shape=(
            pltpu.VMEM((rows, width), bf16),
            pltpu.VMEM(named.ssm_state.shape, f32),
            pltpu.VMEM(named.conv_window.shape, bf16),
        ),
        in_specs=[pl.BlockSpec(memory_space=pltpu.HBM)] * len(named),
        out_specs=tuple(pl.BlockSpec(memory_space=pltpu.VMEM) for _ in range(3)),
        scratch_shapes=scratch,
        compiler_params=pltpu.CompilerParams(
            collective_id=0, has_side_effects=True, vmem_limit_bytes=36 * 1024 * 1024
        ),
    )(*[pltpu.with_memory_space_constraint(one, pltpu.HBM) for one in named])
    outs = (layer_out, next_state, next_window)
    layer_out, next_state, next_window = pl.pallas_call(
        store_kernel,
        out_shape=tuple(jax.ShapeDtypeStruct(one.shape, one.dtype) for one in outs),
        in_specs=[pl.BlockSpec(memory_space=pltpu.VMEM)] * 3,
        out_specs=tuple(pl.BlockSpec(memory_space=pltpu.HBM) for _ in range(3)),
        scratch_shapes=[pltpu.SemaphoreType.DMA((3,))],
        compiler_params=pltpu.CompilerParams(vmem_limit_bytes=1024 * 1024),
    )(*outs)
    return layer_out, next_state.reshape(state_shape), next_window


def fits(args):
    named = Args(*args)
    n = lax.axis_size("ep")
    return (
        named.hidden.shape[0] == 3
        and n & (n - 1) == 0
        and 2 <= n <= 128
        and named.hidden.shape[1] % 512 == 0
        and named.gate_proj.shape[1] == 256
        and named.gate_proj.shape[0] * 2 == named.group_gain.shape[0]
        and named.expert_gate.shape[2] == named.shared_gate.shape[1]
        and named.shared_gate.shape[1] % 256 == 0
        and named.hidden.shape[1] <= named.group_gain.shape[0]
        and named.out_proj.shape[1] == 128
        and named.gate_proj.shape[1] % 128 == 0
        and named.write_t.shape[1] == 64
        and named.expert_gate.shape[0] == 1
        and named.router_t.shape[1] == n
        and HEAD_DIM * 2 == 128
    )


def body(*args):
    return one_kernel(*args) if fits(args) else shards(*args)


def solution(mesh):
    placed = (
        P(("grp", "ep"), None),
        P(("grp", "ep"), None, None),
        P(("grp", "ep"), None, None, None),
        P(None, "ep"),
        P(None, "ep"),
        P(None, "ep"),
        P(None, "ep"),
        P(),
        P(),
        P(),
        P(("grp", "ep"), None),
        P(),
        P(),
        P(),
        P(),
        P(),
        P(None, "ep"),
        P(),
        P(),
        P(("grp", "ep"), None),
        P("ep", None, None),
        P("ep", None, None),
        P("ep", None, None),
        P("ep", None),
        P("ep", None),
        P(),
    )
    return jax.shard_map(
        body,
        mesh=mesh,
        in_specs=placed,
        out_specs=(
            P(("grp", "ep"), None),
            P(("grp", "ep"), None, None, None),
            P(("grp", "ep"), None, None),
        ),
        check_vma=False,
    )
```

```python
import functools
import typing

import jax
import jax.numpy as jnp
from jax import lax
from jax.experimental import pallas as pl
from jax.experimental.pallas import tpu as pltpu
from jax.sharding import PartitionSpec as P

HEAD_DIM = 64
GROUPS = 8
STATE = 128


epsilon = 1e-06
routed_scale = 2.5


def row_scale(values):
    return lax.rsqrt(jnp.mean(values * values, axis=-1, keepdims=True) + epsilon)


def matmul(left, right):
    return jnp.dot(left, right, preferred_element_type=jnp.float32)


def expert_result(rows_in, weight_gate, weight_up, weight_down):
    expert_hidden = (jax.nn.silu(matmul(rows_in, weight_gate)) * matmul(rows_in, weight_up)).astype(
        jnp.bfloat16
    )
    return matmul(expert_hidden, weight_down).astype(jnp.bfloat16)


def exchange_kernel(n, spread, source, landed, send_sem, recv_sem, own_sem):
    me = lax.axis_index("ep")
    barrier = pltpu.get_barrier_semaphore()
    for step in range(1, n):
        pl.semaphore_signal(
            barrier, inc=1, device_id={"ep": lax.rem(me + step, n)}, device_id_type=pl.DeviceIdType.MESH
        )
    own = pltpu.make_async_copy(source if spread else source.at[me], landed.at[me], own_sem)
    own.start()
    pl.semaphore_wait(barrier, n - 1)
    copies = []
    for step in range(1, n):
        target = lax.rem(me + step, n)
        copy = pltpu.make_async_remote_copy(
            src_ref=source if spread else source.at[target],
            dst_ref=landed.at[me],
            send_sem=send_sem.at[step],
            recv_sem=recv_sem.at[step],
            device_id={"ep": target},
            device_id_type=pl.DeviceIdType.MESH,
        )
        copy.start()
        copies.append(copy)
    own.wait()
    for copy in copies:
        copy.wait()


def send(source, shape, spread, ident):
    n = shape[0]
    return pl.pallas_call(
        functools.partial(exchange_kernel, n, spread),
        out_shape=jax.ShapeDtypeStruct(shape, source.dtype),
        in_specs=[pl.BlockSpec(memory_space=pltpu.VMEM)],
        out_specs=pl.BlockSpec(memory_space=pltpu.VMEM),
        scratch_shapes=[
            pltpu.SemaphoreType.DMA((n,)),
            pltpu.SemaphoreType.DMA((n,)),
            pltpu.SemaphoreType.DMA,
        ],
        compiler_params=pltpu.CompilerParams(collective_id=ident, has_side_effects=True),
    )(source)


def exchange(blocks, ident):
    return send(blocks, blocks.shape, False, ident)


def gather(block, ident):
    return send(block, (lax.axis_size("ep"),) + block.shape, True, ident)


def transposed(left, right):
    return lax.dot_general(left, right, (((1,), (1,)), ((), ())), preferred_element_type=jnp.float32)


def state_kernel(per_group, decay, inputs, write, read, carried, updated, mixed):
    row, part = pl.program_id(0), pl.program_id(1)
    heads = carried.shape[1]
    scaled = inputs[0, 0]
    lane = lax.broadcasted_iota(jnp.int32, scaled.shape, 1)
    total = jnp.zeros(scaled.shape, jnp.float32)
    entries = carried.shape[3]
    head_dim = carried.shape[2]
    for group in range(heads // per_group):
        write_row = write[0, 0, group : group + 1]
        spread = jnp.broadcast_to(read[0, 0, group : group + 1], (entries, entries))
        spread_high = spread.astype(jnp.bfloat16)
        spread_low = (spread - spread_high.astype(jnp.float32)).astype(jnp.bfloat16)
        pieces = []
        for head in range(group * per_group, (group + 1) * per_group):
            fresh = (
                carried[0, head] * decay[row, part * heads + head]
                + scaled[:, head : head + 1] * write_row
            )
            updated[0, head] = fresh
            pieces.append(fresh)
        stacked = jnp.concatenate(pieces, axis=0)
        high = stacked.astype(jnp.bfloat16)
        low = (stacked - high.astype(jnp.float32)).astype(jnp.bfloat16)
        columns = transposed(high, spread_high) + transposed(low, spread_high) + transposed(high, spread_low)
        for place in range(per_group):
            head = group * per_group + place
            column = columns[place * head_dim : (place + 1) * head_dim, :heads]
            total = jnp.where(lane == head, column, total)
    mixed[0, 0] = total


def state_step(state, decay_rate, scaled, write_vec, read_vec):
    rows, head_count, head_dim, entries = state.shape
    groups = write_vec.shape[1]
    parts = 2
    heads = head_count // parts
    inputs = scaled.reshape(rows, parts, heads, head_dim).transpose(0, 1, 3, 2)
    vec_shape = (rows, parts, groups // parts, entries)
    part_spec = lambda *dims: pl.BlockSpec((1, 1) + dims, lambda row, part: (row, part, 0, 0))
    state_spec = pl.BlockSpec((1, heads, head_dim, entries), lambda row, part: (row, part, 0, 0))
    next_state, mixed = pl.pallas_call(
        functools.partial(state_kernel, head_count // groups),
        grid=(rows, parts),
        out_shape=(
            jax.ShapeDtypeStruct(state.shape, jnp.float32),
            jax.ShapeDtypeStruct(inputs.shape, jnp.float32),
        ),
        in_specs=[
            pl.BlockSpec(memory_space=pltpu.SMEM),
            part_spec(head_dim, heads),
            part_spec(groups // parts, entries),
            part_spec(groups // parts, entries),
            state_spec,
        ],
        out_specs=(state_spec, part_spec(head_dim, heads)),
    )(decay_rate, inputs, write_vec.reshape(vec_shape), read_vec.reshape(vec_shape), state)
    return next_state, mixed.transpose(0, 1, 3, 2).reshape(rows, head_count, head_dim)


def shards(
    hidden,
    conv_window,
    ssm_state,
    gate_proj,
    input_proj,
    write_proj,
    read_proj,
    step_proj,
    step_bias,
    decay_log,
    decay_shift,
    skip_scale,
    conv_taps,
    conv_bias,
    mix_gain,
    group_gain,
    out_proj,
    ffn_gain,
    router,
    expert_ids,
    expert_gate,
    expert_up,
    expert_down,
    shared_gate,
    shared_up,
    shared_down,
):
    local_rows = hidden.shape[0]
    device_index = lax.axis_index("ep")
    width = hidden.shape[1]
    first_row = device_index * local_rows
    gathered = gather(hidden, 0).reshape(-1, width)
    gathered_wide = gathered.astype(jnp.float32)
    normed = (gathered_wide * row_scale(gathered_wide) * mix_gain).astype(jnp.bfloat16)
    parts = [matmul(normed, proj).astype(jnp.bfloat16) for proj in (gate_proj, input_proj, write_proj, read_proj)]
    outbound = jnp.concatenate(parts, axis=1)
    arrived = exchange(outbound.reshape(-1, local_rows, outbound.shape[1]), 1)
    rows, offset = [], 0
    for part in parts:
        piece = arrived[:, :, offset : offset + part.shape[1]]
        rows.append(piece.transpose(1, 0, 2).reshape(local_rows, -1))
        offset += part.shape[1]
    gate_rows, input_rows, write_rows, read_rows = rows
    hidden_wide = hidden.astype(jnp.float32)
    normed_local = (hidden_wide * row_scale(hidden_wide) * mix_gain).astype(jnp.bfloat16)
    step_raw = matmul(normed_local, step_proj)
    inner_width = gate_rows.shape[1]
    state_span = GROUPS * STATE
    head_count = step_bias.shape[0]
    fresh_row = jnp.concatenate([input_rows, write_rows, read_rows], axis=1)
    window = jnp.concatenate([conv_window, fresh_row[:, None, :]], axis=1)
    convolved = jax.nn.silu(
        jnp.sum(window.astype(jnp.float32) * conv_taps.astype(jnp.float32)[None], axis=1)
        + conv_bias
    )
    head_input = convolved[:, :inner_width].reshape(local_rows, head_count, HEAD_DIM)
    write_vec = convolved[:, inner_width : inner_width + state_span].reshape(
        local_rows, GROUPS, STATE
    )
    read_vec = convolved[:, inner_width + state_span :].reshape(local_rows, GROUPS, STATE)
    step_size = jax.nn.softplus(step_raw + step_bias)
    decay_rate = jnp.exp(decay_shift - step_size * jnp.exp(decay_log))
    next_state, mixed_out = state_step(
        ssm_state, decay_rate, step_size[:, :, None] * head_input, write_vec, read_vec
    )
    mixed_out = mixed_out + skip_scale[None, :, None] * head_input
    mixed_out = mixed_out.reshape(local_rows, inner_width).astype(jnp.bfloat16)
    gated_out = mixed_out.astype(jnp.float32) * jax.nn.silu(gate_rows.astype(jnp.float32))
    blocks = gated_out.reshape(local_rows, GROUPS, -1)
    gated_out = ((blocks * row_scale(blocks)).reshape(local_rows, inner_width) * group_gain).astype(
        jnp.bfloat16
    )
    col_width = out_proj.shape[1]
    resid_cols = lax.dynamic_slice_in_dim(gathered_wide, device_index * col_width, col_width, 1)
    resid_part = (
        resid_cols + matmul(gather(gated_out, 2).reshape(-1, inner_width), out_proj)
    ).astype(jnp.bfloat16)
    resid_all = gather(resid_part, 3).transpose(1, 0, 2).reshape(-1, width)
    gain_part = lax.dynamic_slice_in_dim(ffn_gain, device_index * col_width, col_width, 0)
    shared_part = (resid_part.astype(jnp.float32) * gain_part).astype(jnp.bfloat16)
    shared_pre = jnp.concatenate(
        [matmul(shared_part, shared_gate), matmul(shared_part, shared_up)], axis=1
    ).astype(jnp.bfloat16)
    resid_all_wide = resid_all.astype(jnp.float32)
    scale_all = row_scale(resid_all_wide)
    routed_all = (resid_all_wide * scale_all * ffn_gain).astype(jnp.bfloat16)
    result = expert_result(routed_all, expert_gate[0], expert_up[0], expert_down[0])
    back = exchange(
        jnp.concatenate([result, shared_pre], axis=1).reshape(
            -1, local_rows, width + shared_pre.shape[1]
        ),
        4,
    ).astype(jnp.float32)
    resid_wide = lax.dynamic_slice_in_dim(resid_all_wide, first_row, local_rows, 0)
    norm_scale = lax.dynamic_slice_in_dim(scale_all, first_row, local_rows, 0)
    routed_in = lax.dynamic_slice_in_dim(routed_all, first_row, local_rows, 0)
    scores = jax.nn.sigmoid(matmul(routed_in, router))
    chosen = jnp.any(
        expert_ids[:, :, None] == jnp.arange(router.shape[1], dtype=jnp.int32)[None, None, :], axis=1
    )
    scores = jnp.where(chosen, scores, 0.0)
    weights = routed_scale * scores / jnp.sum(scores, axis=1, keepdims=True)
    routed = jnp.sum(back[:, :, :width] * weights.T[:, :, None], axis=0)
    shared_sum = jnp.sum(back[:, :, width:], axis=0)
    hidden_units = shared_down.shape[0]
    shared_hidden = (
        jax.nn.silu(norm_scale * shared_sum[:, :hidden_units])
        * (norm_scale * shared_sum[:, hidden_units:])
    ).astype(jnp.bfloat16)
    layer_out = (resid_wide + routed + matmul(shared_hidden, shared_down)).astype(jnp.bfloat16)
    return (layer_out, next_state, window[:, 1:])


def dot_t(left, right):
    return lax.dot_general(left, right, (((1,), (1,)), ((), ())), preferred_element_type=jnp.float32)


def dot_0(left, right):
    return lax.dot_general(left, right, (((0,), (0,)), ((), ())), preferred_element_type=jnp.float32)


def silu(v):
    return v / (1.0 + jnp.exp(-v))


def split2(v):
    high = v.astype(jnp.bfloat16)
    return high, (v - high.astype(jnp.float32)).astype(jnp.bfloat16)


class Args(typing.NamedTuple):
    hidden: typing.Any
    conv_window: typing.Any
    ssm_state: typing.Any
    gate_proj: typing.Any
    input_proj: typing.Any
    write_t: typing.Any
    read_t: typing.Any
    step_t: typing.Any
    step_bias: typing.Any
    decay_log: typing.Any
    decay_shift: typing.Any
    skip_scale: typing.Any
    conv_taps: typing.Any
    conv_bias: typing.Any
    mix_gain: typing.Any
    group_gain: typing.Any
    out_proj: typing.Any
    ffn_gain: typing.Any
    router_t: typing.Any
    expert_ids: typing.Any
    expert_gate: typing.Any
    expert_up: typing.Any
    expert_down: typing.Any
    shared_gate: typing.Any
    shared_up: typing.Any
    shared_down: typing.Any


def layer_kernel(n, rows, *refs):
    count = len(Args._fields)
    hbm = Args(*refs[:count])
    layer_out, next_state, next_window = refs[count : count + 3]
    vm = Args(*refs[count + 3 : 2 * count + 3])
    (
        src1, land1, src2, land2, src_g, land_g, src3, land3, src4, land4, src5, land5, src6, land6,
        fold1, fold3, fold5, x_all, x_low, p_all, gate_all, g_all, g_low, h_all, flag0, flag2, part48,
        acc_gate, acc_up, base, cols, y_all, fresh, xv, wv, rv, step_x, skip_x,
        decay_col, decayed, window, slots, served_f, vec_proj,
        src_h, land_h, mate_proj, mate_gate, mate_up, in_sem, send_sem, ring_sem, part_sem, whole_sem, mate_sem,
    ) = refs[2 * count + 3 :]
    me = lax.axis_index("ep")
    f32, bf16 = jnp.float32, jnp.bfloat16
    width = vm.hidden.shape[1]
    inner = cols.shape[1]
    total = n * rows
    heads = hbm.step_bias.shape[1]
    head_dim = inner // heads
    groups = GROUPS
    per_group = heads // groups
    span = inner // groups
    state = STATE
    gate_cols = hbm.gate_proj.shape[1]
    vec_cols = hbm.write_t.shape[0]
    col_width = hbm.out_proj.shape[1]
    shared_units = hbm.shared_gate.shape[1]

    def flipped(value):
        other = me
        bit = 1
        while bit < n:
            if value & bit:
                other = other + bit - 2 * bit * lax.rem(me // bit, 2)
            bit *= 2
        return other

    far_first = tuple(range(n - 1, 0, -1))
    partner = flipped(1)

    barrier = pltpu.get_barrier_semaphore()
    for step in far_first:
        pl.semaphore_signal(
            barrier, inc=1, device_id={"ep": flipped(step)}, device_id_type=pl.DeviceIdType.MESH
        )
    def load(name, at):
        return pltpu.make_async_copy(getattr(hbm, name), getattr(vm, name), in_sem.at[at])

    first = (
        "hidden",
        "mix_gain",
        "expert_ids",
        "write_t",
        "read_t",
        "step_t",
        "step_bias",
        "decay_log",
        "decay_shift",
        "skip_scale",
        "input_proj",
        "gate_proj",
        "conv_window",
        "conv_taps",
        "conv_bias",
        "ssm_state",
    )
    later = (
        "group_gain",
        "out_proj",
        "ffn_gain",
        "shared_gate",
        "shared_up",
        "expert_gate",
        "expert_up",
        "expert_down",
        "router_t",
        "shared_down",
    )
    loads = {name: load(name, at) for at, name in enumerate(first)}
    for one in loads.values():
        one.start()
    loads.update({name: load(name, at) for at, name in enumerate(later)})
    loads = Args(**loads)

    def need(*these):
        for one in these:
            one.wait()

    def remote(source, target_ref, sends, arrives, target):
        return pltpu.make_async_remote_copy(
            src_ref=source,
            dst_ref=target_ref,
            send_sem=sends,
            recv_sem=arrives,
            device_id={"ep": target},
            device_id_type=pl.DeviceIdType.MESH,
        )

    blocks = {}

    def drained(phase):
        if phase in blocks:
            landed, count = blocks.pop(phase)
            all_blocks(landed, send_sem.at[phase], whole_sem.at[0], count).wait_send()

    def sends(phase, landed, count=n - 1):
        drained(phase)
        blocks[phase] = (landed, count)
        return send_sem.at[phase]

    def all_blocks(landed, sem, arrives, count=n - 1):
        many = landed.at[pl.ds(0, count)]
        return remote(many, many, sem, arrives, partner)

    def spread(phase, ring, source, landed):
        sem = sends(phase, landed)
        out = {}
        for step in range(n - 2, -1, -2):
            out[step] = remote(source, landed.at[me], sem, ring_sem.at[ring, step], flipped(step + 1))
            out[step].start()
        return out

    def across(phase, source_of, target_ref, landed, sem_of):
        sem = sends(phase, landed, n // 2)
        for step in range(n - 1, 0, -2):
            to = flipped(step)
            remote(source_of(to), target_ref, sem, sem_of(step), to).start()

    def collect(phase, ring, landed, out, take):
        passed = [(partner, out[0])]
        for step in range(2, n, 2):
            out[step].wait_recv()
            owner = flipped(step + 1)
            block = landed.at[owner]
            one = remote(block, block, send_sem.at[phase], ring_sem.at[ring, step - 1], partner)
            one.start()
            passed.append((flipped(step), one))
            take(owner, 0)
        return passed

    def finish(passed, take):
        for owner, one in passed:
            one.wait_recv()
            take(owner, 0 if owner is partner else 1)

    def scatter(phase, source, landed, sem):
        sent = sends(phase, landed)
        for step in far_first:
            to = flipped(step)
            remote(source.at[to], landed.at[me], sent, sem, to).start()

    span_z = min(n, 4)

    def arrived(landed, place):
        def wait(many):
            some = landed.at[pl.ds(place, many)]
            remote(some, some, send_sem.at[0], part_sem.at[place // span_z], partner).wait_recv()

        @pl.when(me // span_z != place // span_z)
        def _():
            wait(span_z)

        @pl.when(me // span_z == place // span_z)
        def _():
            wait(span_z - 1)

    def arrived_all(which, landed, count=n - 1):
        all_blocks(landed, send_sem.at[0], whole_sem.at[which], count).wait_recv()

    def folded(value, buffer):
        wide = buffer.shape[1]
        rest = wide // rows
        buffer[0:rows] = value[:, :wide]
        for row in range(rows):
            buffer[rows : rows + 1, row * rest : (row + 1) * rest] = value[row : row + 1, wide:]
        return buffer[...].astype(bf16)

    def unfolded(landed, owner, kind, target):
        piece = landed[owner].astype(f32)
        wide = piece.shape[1]
        rest = wide // rows
        chip = owner // 2
        target[chip, 4 * kind : 4 * kind + rows, :wide] = piece[0:rows]
        for row in range(rows):
            target[chip, 4 * kind + row : 4 * kind + row + 1, wide:] = piece[
                rows : rows + 1, row * rest : (row + 1) * rest
            ]

    def in_order(value):
        tiles = value.reshape(n // 2, 8, value.shape[1])
        turned = jnp.concatenate([tiles[:, 4:], tiles[:, :4]], axis=1)
        return jnp.where(lax.rem(me, 2) == 1, tiles, turned).reshape(value.shape)

    need(loads.hidden, loads.mix_gain, loads.expert_ids)
    own = vm.hidden[...].astype(f32)
    scale = lax.rsqrt(jnp.mean(own * own, axis=-1, keepdims=True) + epsilon)
    normed = (own * scale * vm.mix_gain[...]).astype(bf16)
    packed = folded(normed.astype(f32), fold1)
    src1[...] = packed
    land1[me] = packed
    pl.semaphore_wait(barrier, n - 1)
    rows1 = spread(0, 0, src1, land1)
    mates = [
        remote(there, here, mate_sem.at[2 * at], mate_sem.at[2 * at + 1], partner)
        for at, (there, here) in enumerate(
            ((hbm.out_proj, mate_proj), (hbm.shared_gate, mate_gate), (hbm.shared_up, mate_up))
        )
    ]
    for one in mates:
        one.start()

    lane = lax.broadcasted_iota(jnp.int32, (rows, 128), 1)
    ids = vm.expert_ids[...]
    chosen = jnp.zeros((rows, 128), f32)
    for k in range(ids.shape[1]):
        chosen = jnp.where(lane == ids[:, k : k + 1], 1.0, chosen)
    duo = 2 * col_width
    core = lax.rem(me, 2)
    for chip in range(n // 2):
        src_h[chip] = vm.hidden[:, chip * duo : (chip + 1) * duo]
    need(loads.step_t, loads.step_bias, loads.decay_log, loads.decay_shift, loads.skip_scale)
    raw = dot_t(normed, vm.step_t[...]) + vm.step_bias[...]
    step_size = jnp.maximum(raw, 0.0) + jnp.log1p(jnp.exp(-jnp.abs(raw)))
    decay = jnp.exp(vm.decay_shift[...] - step_size * jnp.exp(vm.decay_log[...]))
    skip = vm.skip_scale[...]
    low_half = lax.broadcasted_iota(jnp.int32, (rows, 128), 1) < head_dim
    for pair in range(heads // 2):
        at = slice(pair * 128, (pair + 1) * 128)
        first = jnp.broadcast_to(step_size[:, 2 * pair : 2 * pair + 1], (rows, 128))
        second = jnp.broadcast_to(step_size[:, 2 * pair + 1 : 2 * pair + 2], (rows, 128))
        step_x[:, at] = jnp.where(low_half, first, second)
        first = jnp.broadcast_to(skip[:, 2 * pair : 2 * pair + 1], (1, 128))
        second = jnp.broadcast_to(skip[:, 2 * pair + 1 : 2 * pair + 2], (1, 128))
        skip_x[:, at] = jnp.where(low_half[0:1], first, second)
    for row in range(rows):
        spread_row = jnp.broadcast_to(jnp.concatenate([decay[row : row + 1]] * 2, axis=1), (128, 128))
        turned = spread_row.T
        for group in range(groups):
            decay_col[row * groups + group] = turned[group * per_group : (group + 1) * per_group]

    need(loads.conv_window, loads.conv_taps, loads.conv_bias)
    taps = vm.conv_taps[...].astype(f32)
    for row in range(rows):
        old = vm.conv_window[row].astype(f32)
        base[row : row + 1] = (
            jnp.sum(old * taps[:3], axis=0, keepdims=True) + vm.conv_bias[...]
        )
        window[row, 0:2] = old[1:3]

    need(loads.write_t, loads.read_t)
    for name in later:
        getattr(loads, name).start()
    vec_proj[...] = jnp.concatenate([vm.write_t[...], vm.read_t[...]], axis=0).T
    unfolded(land1, me, 1, x_all)
    take1 = lambda owner, kind: unfolded(land1, owner, kind, x_all)
    finish(collect(0, 0, land1, rows1, take1), take1)
    need(loads.gate_proj, loads.input_proj)
    x_low[...] = x_all[...].reshape(x_low.shape).astype(bf16)
    p_all[:, :gate_cols] = in_order(matmul(x_low[...], vm.input_proj[...]))
    p_all[:, gate_cols:] = in_order(matmul(x_low[...], vec_proj[...]))
    for place in range(n):
        src2[place] = p_all[4 * place : 4 * place + 4].astype(bf16)
    scatter(1, src2, land2, part_sem.at[me // span_z])
    land2[me] = src2[me]
    gate_all[...] = in_order(matmul(x_low[...], vm.gate_proj[...]))
    ends = jnp.concatenate([chosen[0:1], chosen[2:3]], axis=1)
    ends = jnp.broadcast_to(ends, (rows + 1, ends.shape[1]))
    own_part = lax.broadcasted_iota(jnp.int32, ends.shape, 0) < rows
    for place in range(n):
        src_g[place] = jnp.where(own_part, gate_all[4 * place : 4 * place + 4], ends).astype(bf16)
    scatter(2, src_g, land_g, whole_sem.at[0])
    land_g[me] = src_g[me]
    across(4, lambda to: src_h.at[to // 2], land_h.at[me // 2], land_h, lambda step: whole_sem.at[2])

    need(loads.ssm_state)

    def decay_group(at, carry):
        columns = decay_col[at]
        for head in range(per_group):
            part = slice(head * head_dim, (head + 1) * head_dim)
            value = vm.ssm_state[at, part] * columns[head : head + 1]
            next_state[at, part] = value
        decayed[at] = next_state[at].T.astype(bf16)
        return carry

    lax.fori_loop(0, rows * groups, decay_group, 0)

    half = vec_cols
    for place in range(0, n, 2):
        last = []
        for one in (place, place + 1):
            if one % span_z == 0:
                arrived(land2, one)
            whole = land2[one].astype(f32)
            piece = whole[0:rows]
            fresh[:, one * gate_cols : (one + 1) * gate_cols] = piece[:, :gate_cols]
            last.append(piece[:, gate_cols:])
        low = lax.broadcasted_iota(jnp.int32, last[0].shape, 1) < half
        at = slice(inner + place * half, inner + (place + 2) * half)
        fresh[:, at] = jnp.where(low, last[0], pltpu.roll(last[1], half, 1))
        at = slice(at.start + groups * state, at.stop + groups * state)
        fresh[:, at] = jnp.where(low, pltpu.roll(last[0], half, 1), last[1])
    convolved = silu(base[...] + fresh[...] * taps[3:4])
    head_input = convolved[:, :inner]
    xv[...] = head_input
    for group in range(groups):
        at = slice(inner + group * state, inner + (group + 1) * state)
        write = convolved[:, at]
        read = convolved[:, at.start + groups * state : at.stop + groups * state]
        wv[group] = write
        rv[group] = read
    def mix(group):
        high, low = split2(rv[group])
        for row in range(rows):
            left = jnp.concatenate([high[row : row + 1], low[row : row + 1]], axis=0)
            both = matmul(left, decayed[row * groups + group])
            y_all[row : row + 1, group * span : (group + 1) * span] = both[0:1] + both[1:2]

    def gated(group):
        at = slice(group * span, (group + 1) * span)
        overlap = jnp.sum(wv[group] * rv[group], axis=1, keepdims=True)
        mixed = y_all[:, at] + xv[:, at] * (step_x[:, at] * overlap + skip_x[:, at])
        mixed = mixed.astype(bf16).astype(f32) * silu(cols[:, at])
        mixed = mixed * lax.rsqrt(jnp.mean(mixed * mixed, axis=-1, keepdims=True) + epsilon)
        y_all[:, at] = mixed * vm.group_gain[:, at]

    def share(part):
        packed = folded(y_all[:, part * half_inner : (part + 1) * half_inner], fold3)
        src3[part] = packed
        across(
            5 + part,
            lambda to: src3.at[part],
            land3.at[part, me // 2],
            land3.at[part],
            lambda step: ring_sem.at[part, step - 1],
        )

    half_inner = inner // 2
    for group in range(groups // 2):
        mix(group)
    need(loads.group_gain)
    arrived_all(0, land_g)
    for place in range(n):
        whole = land_g[place].astype(f32)
        cols[:, place * gate_cols : (place + 1) * gate_cols] = whole[0:rows]
        flag0[place : place + 1] = whole[rows : rows + 1, :128]
        flag2[place : place + 1] = whole[rows : rows + 1, 128:]
    for group in range(groups // 2):
        gated(group)
    share(0)
    for group in range(groups // 2, groups):
        mix(group)
        gated(group)
    share(1)

    for group in range(groups):
        at = slice(group * span, (group + 1) * span)
        high, low = split2(xv[:, at] * step_x[:, at])
        left = jnp.concatenate([high.astype(f32), low.astype(f32), high.astype(f32)], axis=0).astype(bf16)
        w_high, w_low = split2(wv[group])
        right = jnp.concatenate([w_high.astype(f32), w_high.astype(f32), w_low.astype(f32)], axis=0)
        owner = lax.rem(lax.broadcasted_iota(jnp.int32, right.shape, 0), rows)
        for row in range(rows):
            picked = jnp.where(owner == row, right, 0.0).astype(bf16)
            place = row * groups + group
            next_state[place] = next_state[place] + dot_0(left, picked)
    for row in range(rows):
        window[row, 2:3] = fresh[row : row + 1]
        next_window[row] = window[row].astype(bf16)

    slot_row = lax.broadcasted_iota(jnp.int32, (2 * n, total), 0)
    slot_lane = lax.broadcasted_iota(jnp.int32, (2 * n, total), 1)
    half_rows = total // 2
    first_row = (slot_row // 2) % 2 * half_rows + slot_row // 4 * rows
    even = slot_row % 2 == 0
    outer = jnp.where(even, first_row, first_row + 2)
    whose = lax.broadcasted_iota(jnp.int32, (2 * n, n), 1) == lax.broadcasted_iota(jnp.int32, (2 * n, n), 0) // 2
    whose = jnp.where(whose, 1.0, 0.0).astype(bf16)
    even_row = lax.broadcasted_iota(jnp.int32, (2 * n, 128), 0) % 2 == 0
    flag = jnp.where(
        even_row, matmul(whose, flag0[...].astype(bf16)), matmul(whose, flag2[...].astype(bf16))
    )
    flag = jnp.where(lax.broadcasted_iota(jnp.int32, flag.shape, 1) == me, flag, 0.0)
    flag = jnp.sum(flag, axis=1, keepdims=True)
    source_row = jnp.where(flag > 0.5, outer, first_row + 1)
    select = jnp.where(slot_lane == source_row, 1.0, 0.0).astype(bf16)

    arrived_all(2, land_h, n // 2)
    for chip in range(n // 2):
        h_all[chip * rows : (chip + 1) * rows] = land_h[chip].astype(f32)
    need(loads.out_proj)
    mates[0].wait_recv()
    resid_f = [jnp.zeros((n * 4, col_width), f32)] * 2
    for part in range(2):
        for step in range(1, n, 2):
            chip = flipped(step) // 2
            block = land3.at[part, chip]
            remote(block, block, send_sem.at[0], ring_sem.at[part, step - 1], partner).wait_recv()
            piece = block[...].astype(f32)
            wide = piece.shape[1]
            rest = wide // rows
            g_all[part, chip, 0:rows, :wide] = piece[0:rows]
            for row in range(rows):
                g_all[part, chip, row : row + 1, wide:] = piece[rows : rows + 1, row * rest : (row + 1) * rest]
        g_low[...] = g_all[part].reshape(g_low.shape).astype(bf16)
        at = slice(part * half_inner, (part + 1) * half_inner)
        resid_f = [
            resid_f[0] + matmul(g_low[...], vm.out_proj[at]),
            resid_f[1] + matmul(g_low[...], mate_proj[at]),
        ]
    need(loads.shared_gate, loads.shared_up, loads.ffn_gain)
    for which, place in enumerate((core, 1 - core)):
        for chip in range(n // 2):
            part48[which, chip * rows : (chip + 1) * rows] = resid_f[which][8 * chip : 8 * chip + rows]
    swap = lambda left, right: jnp.where(core == 0, jnp.concatenate([left, right], axis=1), jnp.concatenate([right, left], axis=1))
    resid_part = (swap(part48[0], part48[1]) + h_all[...]).astype(bf16)
    src4[...] = resid_part
    land4[me] = resid_part
    rows4 = spread(0, 2, src4, land4)
    gain_part = vm.ffn_gain[:, pl.ds(pl.multiple_of(me // 2 * duo, duo), duo)]
    shared_part = (resid_part.astype(f32) * gain_part).astype(bf16)
    mates[1].wait_recv()
    mates[2].wait_recv()
    lower, upper = shared_part[:, :col_width], shared_part[:, col_width:]
    mine = jnp.where(core == 0, lower.astype(f32), upper.astype(f32)).astype(bf16)
    other = jnp.where(core == 0, upper.astype(f32), lower.astype(f32)).astype(bf16)
    slots[:, :shared_units] = matmul(mine, vm.shared_gate[...]) + matmul(other, mate_gate[...])
    slots[:, shared_units:] = matmul(mine, vm.shared_up[...]) + matmul(other, mate_up[...])
    for chip in range(n // 2):
        src5[chip] = folded(slots[chip * rows : (chip + 1) * rows], fold5.at[chip])
    across(1, lambda to: src5.at[to // 2], land5.at[me // 2], land5, lambda step: whole_sem.at[0])

    need(loads.expert_gate, loads.expert_up, loads.expert_down)
    acc_gate[...] = jnp.zeros_like(acc_gate)
    acc_up[...] = jnp.zeros_like(acc_up)
    squares = [jnp.zeros((total, duo), f32)]

    def chip_rows(chip):
        return jnp.concatenate([land4[2 * chip + 1].astype(f32), land4[2 * chip].astype(f32)], axis=0)

    def add_chip(owner, kind):
        chip = owner // 2
        piece = chip_rows(chip)
        squares[0] = squares[0] + piece * piece
        at = pl.ds(pl.multiple_of(chip * duo, duo), duo)
        scaled = (piece * vm.ffn_gain[:, at]).astype(bf16)
        acc_gate[...] += matmul(scaled, vm.expert_gate[at])
        acc_up[...] += matmul(scaled, vm.expert_up[at])

    finish(collect(0, 2, land4, rows4, lambda owner, kind: None), add_chip)
    scale_all = lax.rsqrt(jnp.sum(squares[0], axis=1, keepdims=True) / width + epsilon)
    hidden_units = (silu(acc_gate[...] * scale_all) * (acc_up[...] * scale_all)).astype(bf16)
    served = matmul(select, hidden_units).astype(bf16)
    half_width = width // 2
    for part in range(2):
        served_f[...] = matmul(served, vm.expert_down[:, part * half_width : (part + 1) * half_width])
        for place in range(n):
            src6[part, place] = served_f[2 * place : 2 * place + 2].astype(bf16)
        scatter(2 + part, src6.at[part], land6.at[part], part_sem.at[me // span_z] if part else whole_sem.at[1])
        land6[part, me] = src6[part, me]

    need(loads.router_t, loads.shared_down)
    own_row = lax.broadcasted_iota(jnp.int32, (rows, total), 0) + core * half_rows + me // 2 * rows
    pick = jnp.where(lax.broadcasted_iota(jnp.int32, (rows, total), 1) == own_row, 1.0, 0.0).astype(bf16)
    for chip in range(n // 2):
        y_all[:, chip * duo : (chip + 1) * duo] = matmul(pick, chip_rows(chip).astype(bf16))
    resid_own = y_all[:, :width]
    norm_scale = lax.rsqrt(jnp.mean(resid_own * resid_own, axis=-1, keepdims=True) + epsilon)
    routed_own = (resid_own * norm_scale * vm.ffn_gain[...]).astype(bf16)
    scores = 1.0 / (1.0 + jnp.exp(-dot_t(routed_own, vm.router_t[...])))
    kept = chosen[:, :n]
    scores = jnp.where(kept > 0.5, scores, 0.0)
    weights = routed_scale * scores / jnp.sum(scores, axis=1, keepdims=True)
    outer_w = jnp.concatenate([weights[0:1], weights[2:3]], axis=0)
    middle = weights[1:2]
    inner_w = jnp.concatenate([middle * (1.0 - kept[0:1]), middle * kept[0:1]], axis=0)
    shared = jnp.zeros(fold5.shape[1:], f32)
    arrived_all(0, land5, n // 2)
    for chip in range(n // 2):
        shared = shared + land5[chip].astype(f32)
    wide = shared.shape[1]
    rest = wide // rows
    cols[:, :wide] = shared[0:rows]
    for row in range(rows):
        cols[row : row + 1, wide : wide + rest] = shared[rows : rows + 1, row * rest : (row + 1) * rest]
    shared = cols[:, : wide + rest] * norm_scale
    shared_hidden = (silu(shared[:, :shared_units]) * shared[:, shared_units:]).astype(bf16)
    start = resid_own + matmul(shared_hidden, vm.shared_down[...])
    y_all[:, :width] = start
    for part in range(2):
        ends = jnp.zeros((2, half_width), f32)
        mid = jnp.zeros((2, half_width), f32)
        if part == 0:
            arrived_all(1, land6.at[0])
        for place in range(n):
            if part and place % span_z == 0:
                arrived(land6.at[1], place)
            piece = land6[part, place].astype(f32)
            ends = ends + piece * outer_w[:, place : place + 1]
            mid = mid + piece * inner_w[:, place : place + 1]
        at = slice(part * half_width, (part + 1) * half_width)
        xv[0:1, at] = ends[0:1]
        xv[1:2, at] = mid[0:1] + mid[1:2]
        xv[2:3, at] = ends[1:2]
    layer_out[...] = (y_all[:, :width] + xv[:, :width]).astype(bf16)
    for phase in tuple(blocks):
        drained(phase)
    for one in mates:
        one.wait_send()


def store_kernel(layer_out, next_state, next_window, layer_hbm, state_hbm, window_hbm, sems):
    for at in range(next_state.shape[0]):
        pltpu.make_async_copy(next_state.at[at], state_hbm.at[at], sems.at[0]).start()
    small = [
        pltpu.make_async_copy(layer_out, layer_hbm, sems.at[1]),
        pltpu.make_async_copy(next_window, window_hbm, sems.at[2]),
    ]
    for one in small:
        one.start()
    for one in small:
        one.wait()
    pltpu.make_async_copy(next_state, state_hbm, sems.at[0]).wait()


def one_kernel(*args):
    named = Args(*args)
    n = lax.axis_size("ep")
    rows, width = named.hidden.shape
    inner = named.gate_proj.shape[1] * n
    total = n * rows
    heads = named.step_bias.shape[0]
    flat = lambda one: one.reshape(1, -1)
    named = named._replace(
        write_t=named.write_t.T,
        read_t=named.read_t.T,
        step_t=named.step_t.T,
        router_t=named.router_t.T,
        step_bias=flat(named.step_bias),
        decay_log=flat(named.decay_log),
        skip_scale=flat(named.skip_scale),
        conv_bias=flat(named.conv_bias),
        mix_gain=flat(named.mix_gain),
        group_gain=flat(named.group_gain),
        ffn_gain=flat(named.ffn_gain),
        expert_gate=named.expert_gate[0],
        expert_up=named.expert_up[0],
        expert_down=named.expert_down[0],
    )
    state_shape = named.ssm_state.shape
    span = inner // GROUPS
    named = named._replace(ssm_state=named.ssm_state.reshape(rows * GROUPS, span, STATE))
    conv_dim = named.conv_bias.shape[1]
    cols = 2 * named.gate_proj.shape[1] + 2 * named.write_t.shape[0]
    gate_cols = named.gate_proj.shape[1]
    col_width = named.out_proj.shape[1]
    shared_units = named.shared_gate.shape[1]
    bf16, f32 = jnp.bfloat16, jnp.float32
    V = pltpu.VMEM
    scratch = [V(one.shape, one.dtype) for one in named]
    units = 2 * shared_units
    scratch += [
        V((4, width * 3 // 4), bf16), V((n, 4, width * 3 // 4), bf16),
        V((n, 4, cols - gate_cols), bf16), V((n, 4, cols - gate_cols), bf16),
        V((n, 4, gate_cols), bf16), V((n, 4, gate_cols), bf16),
        V((2, 4, inner * 3 // 8), bf16), V((2, n // 2, 4, inner * 3 // 8), bf16),
        V((total // 2, 2 * col_width), bf16), V((n, total // 2, 2 * col_width), bf16),
        V((n // 2, 4, units * 3 // 4), bf16), V((n // 2, 4, units * 3 // 4), bf16),
        V((2, n, 2, width // 2), bf16), V((2, n, 2, width // 2), bf16),
        V((4, width * 3 // 4), f32), V((4, inner * 3 // 8), f32), V((n // 2, 4, units * 3 // 4), f32),
        V((n // 2, 8, width), f32), V((n * 4, width), bf16), V((n * 4, cols - gate_cols), f32),
        V((n * 4, gate_cols), f32),
        V((2, n // 2, 8, inner // 2), f32), V((n * 4, inner // 2), bf16), V((total // 2, 2 * col_width), f32),
        V((n, 128), f32), V((n, 128), f32), V((2, total // 2, col_width), f32),
        V((total, shared_units), f32), V((total, shared_units), f32),
        V((rows, conv_dim), f32), V((rows, inner), f32), V((rows, inner), f32), V((rows, conv_dim), f32),
        V((rows, inner), f32), V((GROUPS, rows, STATE), f32), V((GROUPS, rows, STATE), f32),
        V((rows, inner), f32), V((1, inner), f32),
        V((rows * GROUPS, heads // GROUPS, 128), f32), V((rows * GROUPS, STATE, span), bf16),
        V((rows, 3, conv_dim), f32), V((total // 2, units), f32), V((2 * n, width // 2), f32),
        V((width, cols - 2 * gate_cols), bf16),
        V((n // 2, rows, 2 * col_width), bf16), V((n // 2, rows, 2 * col_width), bf16),
        V(named.out_proj.shape, bf16), V(named.shared_gate.shape, bf16), V(named.shared_up.shape, bf16),
        pltpu.SemaphoreType.DMA((16,)),
        pltpu.SemaphoreType.DMA((7,)),
        pltpu.SemaphoreType.DMA((3, n - 1)),
        pltpu.SemaphoreType.DMA((max(1, n // 4),)),
        pltpu.SemaphoreType.DMA((3,)),
        pltpu.SemaphoreType.DMA((6,)),
    ]
    layer_out, next_state, next_window = pl.pallas_call(
        functools.partial(layer_kernel, n, rows),
        out_shape=(
            pltpu.VMEM((rows, width), bf16),
            pltpu.VMEM(named.ssm_state.shape, f32),
            pltpu.VMEM(named.conv_window.shape, bf16),
        ),
        in_specs=[pl.BlockSpec(memory_space=pltpu.HBM)] * len(named),
        out_specs=tuple(pl.BlockSpec(memory_space=pltpu.VMEM) for _ in range(3)),
        scratch_shapes=scratch,
        compiler_params=pltpu.CompilerParams(
            collective_id=0, has_side_effects=True, vmem_limit_bytes=36 * 1024 * 1024
        ),
    )(*[pltpu.with_memory_space_constraint(one, pltpu.HBM) for one in named])
    outs = (layer_out, next_state, next_window)
    layer_out, next_state, next_window = pl.pallas_call(
        store_kernel,
        out_shape=tuple(jax.ShapeDtypeStruct(one.shape, one.dtype) for one in outs),
        in_specs=[pl.BlockSpec(memory_space=pltpu.VMEM)] * 3,
        out_specs=tuple(pl.BlockSpec(memory_space=pltpu.HBM) for _ in range(3)),
        scratch_shapes=[pltpu.SemaphoreType.DMA((3,))],
        compiler_params=pltpu.CompilerParams(vmem_limit_bytes=1024 * 1024),
    )(*outs)
    return layer_out, next_state.reshape(state_shape), next_window


def fits(args):
    named = Args(*args)
    n = lax.axis_size("ep")
    return (
        named.hidden.shape[0] == 3
        and n & (n - 1) == 0
        and 2 <= n <= 128
        and named.hidden.shape[1] % 512 == 0
        and named.gate_proj.shape[1] == 256
        and named.gate_proj.shape[0] * 2 == named.group_gain.shape[0]
        and named.expert_gate.shape[2] == named.shared_gate.shape[1]
        and named.shared_gate.shape[1] % 256 == 0
        and named.hidden.shape[1] <= named.group_gain.shape[0]
        and named.out_proj.shape[1] == 128
        and named.gate_proj.shape[1] % 128 == 0
        and named.write_t.shape[1] == 64
        and named.expert_gate.shape[0] == 1
        and named.router_t.shape[1] == n
        and HEAD_DIM * 2 == 128
    )


def body(*args):
    return one_kernel(*args) if fits(args) else shards(*args)


def solution(mesh):
    placed = (
        P(("grp", "ep"), None),
        P(("grp", "ep"), None, None),
        P(("grp", "ep"), None, None, None),
        P(None, "ep"),
        P(None, "ep"),
        P(None, "ep"),
        P(None, "ep"),
        P(),
        P(),
        P(),
        P(("grp", "ep"), None),
        P(),
        P(),
        P(),
        P(),
        P(),
        P(None, "ep"),
        P(),
        P(),
        P(("grp", "ep"), None),
        P("ep", None, None),
        P("ep", None, None),
        P("ep", None, None),
        P("ep", None),
        P("ep", None),
        P(),
    )
    return jax.shard_map(
        body,
        mesh=mesh,
        in_specs=placed,
        out_specs=(
            P(("grp", "ep"), None),
            P(("grp", "ep"), None, None, None),
            P(("grp", "ep"), None, None),
        ),
        check_vma=False,
    )
```

```python
import functools
import typing

import jax
import jax.numpy as jnp
from jax import lax
from jax.experimental import pallas as pl
from jax.experimental.pallas import tpu as pltpu
from jax.sharding import PartitionSpec as P

HEAD_DIM = 64
GROUPS = 8
STATE = 128


epsilon = 1e-06
routed_scale = 2.5


def row_scale(values):
    return lax.rsqrt(jnp.mean(values * values, axis=-1, keepdims=True) + epsilon)


def matmul(left, right):
    return jnp.dot(left, right, preferred_element_type=jnp.float32)


def expert_result(rows_in, weight_gate, weight_up, weight_down):
    expert_hidden = (jax.nn.silu(matmul(rows_in, weight_gate)) * matmul(rows_in, weight_up)).astype(
        jnp.bfloat16
    )
    return matmul(expert_hidden, weight_down).astype(jnp.bfloat16)


def exchange_kernel(n, spread, source, landed, send_sem, recv_sem, own_sem):
    me = lax.axis_index("ep")
    barrier = pltpu.get_barrier_semaphore()
    for step in range(1, n):
        pl.semaphore_signal(
            barrier, inc=1, device_id={"ep": lax.rem(me + step, n)}, device_id_type=pl.DeviceIdType.MESH
        )
    own = pltpu.make_async_copy(source if spread else source.at[me], landed.at[me], own_sem)
    own.start()
    pl.semaphore_wait(barrier, n - 1)
    copies = []
    for step in range(1, n):
        target = lax.rem(me + step, n)
        copy = pltpu.make_async_remote_copy(
            src_ref=source if spread else source.at[target],
            dst_ref=landed.at[me],
            send_sem=send_sem.at[step],
            recv_sem=recv_sem.at[step],
            device_id={"ep": target},
            device_id_type=pl.DeviceIdType.MESH,
        )
        copy.start()
        copies.append(copy)
    own.wait()
    for copy in copies:
        copy.wait()


def send(source, shape, spread, ident):
    n = shape[0]
    return pl.pallas_call(
        functools.partial(exchange_kernel, n, spread),
        out_shape=jax.ShapeDtypeStruct(shape, source.dtype),
        in_specs=[pl.BlockSpec(memory_space=pltpu.VMEM)],
        out_specs=pl.BlockSpec(memory_space=pltpu.VMEM),
        scratch_shapes=[
            pltpu.SemaphoreType.DMA((n,)),
            pltpu.SemaphoreType.DMA((n,)),
            pltpu.SemaphoreType.DMA,
        ],
        compiler_params=pltpu.CompilerParams(collective_id=ident, has_side_effects=True),
    )(source)


def exchange(blocks, ident):
    return send(blocks, blocks.shape, False, ident)


def gather(block, ident):
    return send(block, (lax.axis_size("ep"),) + block.shape, True, ident)


def transposed(left, right):
    return lax.dot_general(left, right, (((1,), (1,)), ((), ())), preferred_element_type=jnp.float32)


def state_kernel(per_group, decay, inputs, write, read, carried, updated, mixed):
    row, part = pl.program_id(0), pl.program_id(1)
    heads = carried.shape[1]
    scaled = inputs[0, 0]
    lane = lax.broadcasted_iota(jnp.int32, scaled.shape, 1)
    total = jnp.zeros(scaled.shape, jnp.float32)
    entries = carried.shape[3]
    head_dim = carried.shape[2]
    for group in range(heads // per_group):
        write_row = write[0, 0, group : group + 1]
        spread = jnp.broadcast_to(read[0, 0, group : group + 1], (entries, entries))
        spread_high = spread.astype(jnp.bfloat16)
        spread_low = (spread - spread_high.astype(jnp.float32)).astype(jnp.bfloat16)
        pieces = []
        for head in range(group * per_group, (group + 1) * per_group):
            fresh = (
                carried[0, head] * decay[row, part * heads + head]
                + scaled[:, head : head + 1] * write_row
            )
            updated[0, head] = fresh
            pieces.append(fresh)
        stacked = jnp.concatenate(pieces, axis=0)
        high = stacked.astype(jnp.bfloat16)
        low = (stacked - high.astype(jnp.float32)).astype(jnp.bfloat16)
        columns = transposed(high, spread_high) + transposed(low, spread_high) + transposed(high, spread_low)
        for place in range(per_group):
            head = group * per_group + place
            column = columns[place * head_dim : (place + 1) * head_dim, :heads]
            total = jnp.where(lane == head, column, total)
    mixed[0, 0] = total


def state_step(state, decay_rate, scaled, write_vec, read_vec):
    rows, head_count, head_dim, entries = state.shape
    groups = write_vec.shape[1]
    parts = 2
    heads = head_count // parts
    inputs = scaled.reshape(rows, parts, heads, head_dim).transpose(0, 1, 3, 2)
    vec_shape = (rows, parts, groups // parts, entries)
    part_spec = lambda *dims: pl.BlockSpec((1, 1) + dims, lambda row, part: (row, part, 0, 0))
    state_spec = pl.BlockSpec((1, heads, head_dim, entries), lambda row, part: (row, part, 0, 0))
    next_state, mixed = pl.pallas_call(
        functools.partial(state_kernel, head_count // groups),
        grid=(rows, parts),
        out_shape=(
            jax.ShapeDtypeStruct(state.shape, jnp.float32),
            jax.ShapeDtypeStruct(inputs.shape, jnp.float32),
        ),
        in_specs=[
            pl.BlockSpec(memory_space=pltpu.SMEM),
            part_spec(head_dim, heads),
            part_spec(groups // parts, entries),
            part_spec(groups // parts, entries),
            state_spec,
        ],
        out_specs=(state_spec, part_spec(head_dim, heads)),
    )(decay_rate, inputs, write_vec.reshape(vec_shape), read_vec.reshape(vec_shape), state)
    return next_state, mixed.transpose(0, 1, 3, 2).reshape(rows, head_count, head_dim)


def shards(
    hidden,
    conv_window,
    ssm_state,
    gate_proj,
    input_proj,
    write_proj,
    read_proj,
    step_proj,
    step_bias,
    decay_log,
    decay_shift,
    skip_scale,
    conv_taps,
    conv_bias,
    mix_gain,
    group_gain,
    out_proj,
    ffn_gain,
    router,
    expert_ids,
    expert_gate,
    expert_up,
    expert_down,
    shared_gate,
    shared_up,
    shared_down,
):
    local_rows = hidden.shape[0]
    device_index = lax.axis_index("ep")
    width = hidden.shape[1]
    first_row = device_index * local_rows
    gathered = gather(hidden, 0).reshape(-1, width)
    gathered_wide = gathered.astype(jnp.float32)
    normed = (gathered_wide * row_scale(gathered_wide) * mix_gain).astype(jnp.bfloat16)
    parts = [matmul(normed, proj).astype(jnp.bfloat16) for proj in (gate_proj, input_proj, write_proj, read_proj)]
    outbound = jnp.concatenate(parts, axis=1)
    arrived = exchange(outbound.reshape(-1, local_rows, outbound.shape[1]), 1)
    rows, offset = [], 0
    for part in parts:
        piece = arrived[:, :, offset : offset + part.shape[1]]
        rows.append(piece.transpose(1, 0, 2).reshape(local_rows, -1))
        offset += part.shape[1]
    gate_rows, input_rows, write_rows, read_rows = rows
    hidden_wide = hidden.astype(jnp.float32)
    normed_local = (hidden_wide * row_scale(hidden_wide) * mix_gain).astype(jnp.bfloat16)
    step_raw = matmul(normed_local, step_proj)
    inner_width = gate_rows.shape[1]
    state_span = GROUPS * STATE
    head_count = step_bias.shape[0]
    fresh_row = jnp.concatenate([input_rows, write_rows, read_rows], axis=1)
    window = jnp.concatenate([conv_window, fresh_row[:, None, :]], axis=1)
    convolved = jax.nn.silu(
        jnp.sum(window.astype(jnp.float32) * conv_taps.astype(jnp.float32)[None], axis=1)
        + conv_bias
    )
    head_input = convolved[:, :inner_width].reshape(local_rows, head_count, HEAD_DIM)
    write_vec = convolved[:, inner_width : inner_width + state_span].reshape(
        local_rows, GROUPS, STATE
    )
    read_vec = convolved[:, inner_width + state_span :].reshape(local_rows, GROUPS, STATE)
    step_size = jax.nn.softplus(step_raw + step_bias)
    decay_rate = jnp.exp(decay_shift - step_size * jnp.exp(decay_log))
    next_state, mixed_out = state_step(
        ssm_state, decay_rate, step_size[:, :, None] * head_input, write_vec, read_vec
    )
    mixed_out = mixed_out + skip_scale[None, :, None] * head_input
    mixed_out = mixed_out.reshape(local_rows, inner_width).astype(jnp.bfloat16)
    gated_out = mixed_out.astype(jnp.float32) * jax.nn.silu(gate_rows.astype(jnp.float32))
    blocks = gated_out.reshape(local_rows, GROUPS, -1)
    gated_out = ((blocks * row_scale(blocks)).reshape(local_rows, inner_width) * group_gain).astype(
        jnp.bfloat16
    )
    col_width = out_proj.shape[1]
    resid_cols = lax.dynamic_slice_in_dim(gathered_wide, device_index * col_width, col_width, 1)
    resid_part = (
        resid_cols + matmul(gather(gated_out, 2).reshape(-1, inner_width), out_proj)
    ).astype(jnp.bfloat16)
    resid_all = gather(resid_part, 3).transpose(1, 0, 2).reshape(-1, width)
    gain_part = lax.dynamic_slice_in_dim(ffn_gain, device_index * col_width, col_width, 0)
    shared_part = (resid_part.astype(jnp.float32) * gain_part).astype(jnp.bfloat16)
    shared_pre = jnp.concatenate(
        [matmul(shared_part, shared_gate), matmul(shared_part, shared_up)], axis=1
    ).astype(jnp.bfloat16)
    resid_all_wide = resid_all.astype(jnp.float32)
    scale_all = row_scale(resid_all_wide)
    routed_all = (resid_all_wide * scale_all * ffn_gain).astype(jnp.bfloat16)
    result = expert_result(routed_all, expert_gate[0], expert_up[0], expert_down[0])
    back = exchange(
        jnp.concatenate([result, shared_pre], axis=1).reshape(
            -1, local_rows, width + shared_pre.shape[1]
        ),
        4,
    ).astype(jnp.float32)
    resid_wide = lax.dynamic_slice_in_dim(resid_all_wide, first_row, local_rows, 0)
    norm_scale = lax.dynamic_slice_in_dim(scale_all, first_row, local_rows, 0)
    routed_in = lax.dynamic_slice_in_dim(routed_all, first_row, local_rows, 0)
    scores = jax.nn.sigmoid(matmul(routed_in, router))
    chosen = jnp.any(
        expert_ids[:, :, None] == jnp.arange(router.shape[1], dtype=jnp.int32)[None, None, :], axis=1
    )
    scores = jnp.where(chosen, scores, 0.0)
    weights = routed_scale * scores / jnp.sum(scores, axis=1, keepdims=True)
    routed = jnp.sum(back[:, :, :width] * weights.T[:, :, None], axis=0)
    shared_sum = jnp.sum(back[:, :, width:], axis=0)
    hidden_units = shared_down.shape[0]
    shared_hidden = (
        jax.nn.silu(norm_scale * shared_sum[:, :hidden_units])
        * (norm_scale * shared_sum[:, hidden_units:])
    ).astype(jnp.bfloat16)
    layer_out = (resid_wide + routed + matmul(shared_hidden, shared_down)).astype(jnp.bfloat16)
    return (layer_out, next_state, window[:, 1:])


def dot_t(left, right):
    return lax.dot_general(left, right, (((1,), (1,)), ((), ())), preferred_element_type=jnp.float32)


def dot_0(left, right):
    return lax.dot_general(left, right, (((0,), (0,)), ((), ())), preferred_element_type=jnp.float32)


def silu(v):
    return v / (1.0 + jnp.exp(-v))


def split2(v):
    high = v.astype(jnp.bfloat16)
    return high, (v - high.astype(jnp.float32)).astype(jnp.bfloat16)


class Args(typing.NamedTuple):
    hidden: typing.Any
    conv_window: typing.Any
    ssm_state: typing.Any
    gate_proj: typing.Any
    input_proj: typing.Any
    write_t: typing.Any
    read_t: typing.Any
    step_t: typing.Any
    step_bias: typing.Any
    decay_log: typing.Any
    decay_shift: typing.Any
    skip_scale: typing.Any
    conv_taps: typing.Any
    conv_bias: typing.Any
    mix_gain: typing.Any
    group_gain: typing.Any
    out_proj: typing.Any
    ffn_gain: typing.Any
    router_t: typing.Any
    expert_ids: typing.Any
    expert_gate: typing.Any
    expert_up: typing.Any
    expert_down: typing.Any
    shared_gate: typing.Any
    shared_up: typing.Any
    shared_down: typing.Any


def layer_kernel(n, rows, *refs):
    count = len(Args._fields)
    hbm = Args(*refs[:count])
    layer_out, next_state, next_window = refs[count : count + 3]
    vm = Args(*refs[count + 3 : 2 * count + 3])
    (
        src1, land1, src2, land2, src_g, land_g, src3, land3, src4, land4, src5, land5, src6, land6,
        fold1, fold3, fold5, x_all, x_low, p_all, gate_all, g_all, g_low, h_all, flag0, flag2, part48,
        acc_gate, acc_up, base, cols, y_all, fresh, xv, wv, rv, step_x, skip_x,
        decay_col, decayed, window, slots, served_f, vec_proj,
        src_h, land_h, mate_proj, mate_gate, mate_up, in_sem, send_sem, ring_sem, part_sem, whole_sem, mate_sem, half_sem, by_chip,
    ) = refs[2 * count + 3 :]
    me = lax.axis_index("ep")
    f32, bf16 = jnp.float32, jnp.bfloat16
    width = vm.hidden.shape[1]
    inner = cols.shape[1]
    total = n * rows
    heads = hbm.step_bias.shape[1]
    head_dim = inner // heads
    groups = GROUPS
    per_group = heads // groups
    span = inner // groups
    state = STATE
    gate_cols = hbm.gate_proj.shape[1]
    vec_cols = hbm.write_t.shape[0]
    col_width = hbm.out_proj.shape[1]
    shared_units = hbm.shared_gate.shape[1]

    def flipped(value):
        other = me
        bit = 1
        while bit < n:
            if value & bit:
                other = other + bit - 2 * bit * lax.rem(me // bit, 2)
            bit *= 2
        return other

    far_first = tuple(range(n - 1, 0, -1))
    partner = flipped(1)

    barrier = pltpu.get_barrier_semaphore()
    for step in far_first:
        pl.semaphore_signal(
            barrier, inc=1, device_id={"ep": flipped(step)}, device_id_type=pl.DeviceIdType.MESH
        )
    def load(name, at):
        return pltpu.make_async_copy(getattr(hbm, name), getattr(vm, name), in_sem.at[at])

    first = (
        "hidden",
        "mix_gain",
        "expert_ids",
        "write_t",
        "read_t",
        "step_t",
        "step_bias",
        "decay_log",
        "decay_shift",
        "skip_scale",
        "input_proj",
        "gate_proj",
        "conv_window",
        "conv_taps",
        "conv_bias",
        "ssm_state",
    )
    later = (
        "group_gain",
        "out_proj",
        "ffn_gain",
        "shared_gate",
        "shared_up",
        "expert_gate",
        "expert_up",
        "expert_down",
        "router_t",
        "shared_down",
    )
    loads = {name: load(name, at) for at, name in enumerate(first)}
    for one in loads.values():
        one.start()
    loads.update({name: load(name, at) for at, name in enumerate(later)})
    loads = Args(**loads)

    def need(*these):
        for one in these:
            one.wait()

    def remote(source, target_ref, sends, arrives, target):
        return pltpu.make_async_remote_copy(
            src_ref=source,
            dst_ref=target_ref,
            send_sem=sends,
            recv_sem=arrives,
            device_id={"ep": target},
            device_id_type=pl.DeviceIdType.MESH,
        )

    blocks = {}

    def drained(phase):
        if phase in blocks:
            landed, count = blocks.pop(phase)
            all_blocks(landed, send_sem.at[phase], whole_sem.at[0], count).wait_send()

    def sends(phase, landed, count=n - 1):
        drained(phase)
        blocks[phase] = (landed, count)
        return send_sem.at[phase]

    def all_blocks(landed, sem, arrives, count=n - 1):
        many = landed.at[pl.ds(0, count)]
        return remote(many, many, sem, arrives, partner)

    def spread(phase, ring, source, landed):
        sem = sends(phase, landed)
        out = {}
        for step in range(n - 2, -1, -2):
            out[step] = remote(source, landed.at[me], sem, ring_sem.at[ring, step], flipped(step + 1))
            out[step].start()
        return out

    def across(phase, source_of, target_ref, landed, sem_of):
        sem = sends(phase, landed, n // 2)
        for step in range(n - 1, 0, -2):
            to = flipped(step)
            remote(source_of(to), target_ref, sem, sem_of(step), to).start()

    def collect(phase, ring, landed, out, take):
        passed = [(partner, out[0])]
        for step in range(2, n, 2):
            out[step].wait_recv()
            owner = flipped(step + 1)
            block = landed.at[owner]
            one = remote(block, block, send_sem.at[phase], ring_sem.at[ring, step - 1], partner)
            one.start()
            passed.append((flipped(step), one))
            take(owner, 0)
        return passed

    def finish(passed, take):
        for owner, one in passed:
            one.wait_recv()
            take(owner, 0 if owner is partner else 1)

    def scatter(phase, source, landed, sem):
        sent = sends(phase, landed)
        for step in far_first:
            to = flipped(step)
            remote(source.at[to], landed.at[me], sent, sem, to).start()

    span_z = min(n, 4)

    def arrived(landed, place):
        def wait(many):
            some = landed.at[pl.ds(place, many)]
            remote(some, some, send_sem.at[0], part_sem.at[place // span_z], partner).wait_recv()

        @pl.when(me // span_z != place // span_z)
        def _():
            wait(span_z)

        @pl.when(me // span_z == place // span_z)
        def _():
            wait(span_z - 1)

    def arrived_all(which, landed, count=n - 1):
        all_blocks(landed, send_sem.at[0], whole_sem.at[which], count).wait_recv()

    def folded(value, buffer):
        wide = buffer.shape[1]
        rest = wide // rows
        buffer[0:rows] = value[:, :wide]
        for row in range(rows):
            buffer[rows : rows + 1, row * rest : (row + 1) * rest] = value[row : row + 1, wide:]
        return buffer[...].astype(bf16)

    def unfolded(landed, owner, kind, target):
        piece = landed[owner].astype(f32)
        wide = piece.shape[1]
        rest = wide // rows
        chip = owner // 2
        target[chip, 4 * kind : 4 * kind + rows, :wide] = piece[0:rows]
        for row in range(rows):
            target[chip, 4 * kind + row : 4 * kind + row + 1, wide:] = piece[
                rows : rows + 1, row * rest : (row + 1) * rest
            ]

    def in_order(value):
        tiles = value.reshape(n // 2, 8, value.shape[1])
        turned = jnp.concatenate([tiles[:, 4:], tiles[:, :4]], axis=1)
        return jnp.where(lax.rem(me, 2) == 1, tiles, turned).reshape(value.shape)

    need(loads.hidden, loads.mix_gain, loads.expert_ids)
    own = vm.hidden[...].astype(f32)
    scale = lax.rsqrt(jnp.mean(own * own, axis=-1, keepdims=True) + epsilon)
    normed = (own * scale * vm.mix_gain[...]).astype(bf16)
    packed = folded(normed.astype(f32), fold1)
    src1[...] = packed
    land1[me] = packed
    pl.semaphore_wait(barrier, n - 1)
    rows1 = spread(0, 0, src1, land1)
    mates = [
        remote(there, here, mate_sem.at[2 * at], mate_sem.at[2 * at + 1], partner)
        for at, (there, here) in enumerate(
            ((hbm.out_proj, mate_proj), (hbm.shared_gate, mate_gate), (hbm.shared_up, mate_up))
        )
    ]
    for one in mates:
        one.start()

    lane = lax.broadcasted_iota(jnp.int32, (rows, 128), 1)
    ids = vm.expert_ids[...]
    chosen = jnp.zeros((rows, 128), f32)
    for k in range(ids.shape[1]):
        chosen = jnp.where(lane == ids[:, k : k + 1], 1.0, chosen)
    duo = 2 * col_width
    core = lax.rem(me, 2)
    for chip in range(n // 2):
        src_h[chip] = vm.hidden[:, chip * duo : (chip + 1) * duo]
    need(loads.step_t, loads.step_bias, loads.decay_log, loads.decay_shift, loads.skip_scale)
    raw = dot_t(normed, vm.step_t[...]) + vm.step_bias[...]
    step_size = jnp.maximum(raw, 0.0) + jnp.log1p(jnp.exp(-jnp.abs(raw)))
    decay = jnp.exp(vm.decay_shift[...] - step_size * jnp.exp(vm.decay_log[...]))
    skip = vm.skip_scale[...]
    low_half = lax.broadcasted_iota(jnp.int32, (rows, 128), 1) < head_dim
    for pair in range(heads // 2):
        at = slice(pair * 128, (pair + 1) * 128)
        first = jnp.broadcast_to(step_size[:, 2 * pair : 2 * pair + 1], (rows, 128))
        second = jnp.broadcast_to(step_size[:, 2 * pair + 1 : 2 * pair + 2], (rows, 128))
        step_x[:, at] = jnp.where(low_half, first, second)
        first = jnp.broadcast_to(skip[:, 2 * pair : 2 * pair + 1], (1, 128))
        second = jnp.broadcast_to(skip[:, 2 * pair + 1 : 2 * pair + 2], (1, 128))
        skip_x[:, at] = jnp.where(low_half[0:1], first, second)
    for row in range(rows):
        spread_row = jnp.broadcast_to(jnp.concatenate([decay[row : row + 1]] * 2, axis=1), (128, 128))
        turned = spread_row.T
        for group in range(groups):
            decay_col[row * groups + group] = turned[group * per_group : (group + 1) * per_group]

    need(loads.conv_window, loads.conv_taps, loads.conv_bias)
    taps = vm.conv_taps[...].astype(f32)
    for row in range(rows):
        old = vm.conv_window[row].astype(f32)
        base[row : row + 1] = (
            jnp.sum(old * taps[:3], axis=0, keepdims=True) + vm.conv_bias[...]
        )
        window[row, 0:2] = old[1:3]

    need(loads.write_t, loads.read_t)
    for name in later:
        getattr(loads, name).start()
    vec_proj[...] = jnp.concatenate([vm.write_t[...], vm.read_t[...]], axis=0).T
    unfolded(land1, me, 1, x_all)
    take1 = lambda owner, kind: unfolded(land1, owner, kind, x_all)
    finish(collect(0, 0, land1, rows1, take1), take1)
    need(loads.gate_proj, loads.input_proj)
    x_low[...] = x_all[...].reshape(x_low.shape).astype(bf16)
    p_all[:, :gate_cols] = in_order(matmul(x_low[...], vm.input_proj[...]))
    p_all[:, gate_cols:] = in_order(matmul(x_low[...], vec_proj[...]))
    for place in range(n):
        src2[place] = p_all[4 * place : 4 * place + 4].astype(bf16)
    scatter(1, src2, land2, part_sem.at[me // span_z])
    land2[me] = src2[me]
    gate_all[...] = in_order(matmul(x_low[...], vm.gate_proj[...]))
    ends = jnp.concatenate([chosen[0:1], chosen[2:3]], axis=1)
    ends = jnp.broadcast_to(ends, (rows + 1, ends.shape[1]))
    own_part = lax.broadcasted_iota(jnp.int32, ends.shape, 0) < rows
    for place in range(n):
        src_g[place] = jnp.where(own_part, gate_all[4 * place : 4 * place + 4], ends).astype(bf16)
    scatter(2, src_g, land_g, whole_sem.at[0])
    land_g[me] = src_g[me]
    across(4, lambda to: src_h.at[to // 2], land_h.at[me // 2], land_h, lambda step: whole_sem.at[2])

    need(loads.ssm_state)

    def decay_group(at, carry):
        columns = decay_col[at]
        for head in range(per_group):
            part = slice(head * head_dim, (head + 1) * head_dim)
            value = vm.ssm_state[at, part] * columns[head : head + 1]
            next_state[at, part] = value
        decayed[at] = next_state[at].T.astype(bf16)
        return carry

    lax.fori_loop(0, rows * groups, decay_group, 0)

    half = vec_cols
    for place in range(0, n, 2):
        last = []
        for one in (place, place + 1):
            if one % span_z == 0:
                arrived(land2, one)
            whole = land2[one].astype(f32)
            piece = whole[0:rows]
            fresh[:, one * gate_cols : (one + 1) * gate_cols] = piece[:, :gate_cols]
            last.append(piece[:, gate_cols:])
        low = lax.broadcasted_iota(jnp.int32, last[0].shape, 1) < half
        at = slice(inner + place * half, inner + (place + 2) * half)
        fresh[:, at] = jnp.where(low, last[0], pltpu.roll(last[1], half, 1))
        at = slice(at.start + groups * state, at.stop + groups * state)
        fresh[:, at] = jnp.where(low, pltpu.roll(last[0], half, 1), last[1])
    convolved = silu(base[...] + fresh[...] * taps[3:4])
    head_input = convolved[:, :inner]
    xv[...] = head_input
    for group in range(groups):
        at = slice(inner + group * state, inner + (group + 1) * state)
        write = convolved[:, at]
        read = convolved[:, at.start + groups * state : at.stop + groups * state]
        wv[group] = write
        rv[group] = read
    def mix(group):
        high, low = split2(rv[group])
        for row in range(rows):
            left = jnp.concatenate([high[row : row + 1], low[row : row + 1]], axis=0)
            both = matmul(left, decayed[row * groups + group])
            y_all[row : row + 1, group * span : (group + 1) * span] = both[0:1] + both[1:2]

    def gated(group):
        at = slice(group * span, (group + 1) * span)
        overlap = jnp.sum(wv[group] * rv[group], axis=1, keepdims=True)
        mixed = y_all[:, at] + xv[:, at] * (step_x[:, at] * overlap + skip_x[:, at])
        mixed = mixed.astype(bf16).astype(f32) * silu(cols[:, at])
        mixed = mixed * lax.rsqrt(jnp.mean(mixed * mixed, axis=-1, keepdims=True) + epsilon)
        y_all[:, at] = mixed * vm.group_gain[:, at]

    def share(part):
        packed = folded(y_all[:, part * half_inner : (part + 1) * half_inner], fold3)
        src3[part] = packed
        across(
            5 + part,
            lambda to: src3.at[part],
            land3.at[part, me // 2],
            land3.at[part],
            lambda step: half_sem.at[step // 2] if part else ring_sem.at[0, step - 1],
        )

    half_inner = inner // 2
    for group in range(groups // 2):
        mix(group)
    need(loads.group_gain)
    arrived_all(0, land_g)
    for place in range(n):
        whole = land_g[place].astype(f32)
        cols[:, place * gate_cols : (place + 1) * gate_cols] = whole[0:rows]
        flag0[place : place + 1] = whole[rows : rows + 1, :128]
        flag2[place : place + 1] = whole[rows : rows + 1, 128:]
    for group in range(groups // 2):
        gated(group)
    share(0)
    for group in range(groups // 2, groups):
        mix(group)
        gated(group)
    share(1)

    for group in range(groups):
        at = slice(group * span, (group + 1) * span)
        high, low = split2(xv[:, at] * step_x[:, at])
        left = jnp.concatenate([high.astype(f32), low.astype(f32), high.astype(f32)], axis=0).astype(bf16)
        w_high, w_low = split2(wv[group])
        right = jnp.concatenate([w_high.astype(f32), w_high.astype(f32), w_low.astype(f32)], axis=0)
        owner = lax.rem(lax.broadcasted_iota(jnp.int32, right.shape, 0), rows)
        for row in range(rows):
            picked = jnp.where(owner == row, right, 0.0).astype(bf16)
            place = row * groups + group
            next_state[place] = next_state[place] + dot_0(left, picked)
    for row in range(rows):
        window[row, 2:3] = fresh[row : row + 1]
        next_window[row] = window[row].astype(bf16)

    slot_row = lax.broadcasted_iota(jnp.int32, (2 * n, total), 0)
    slot_lane = lax.broadcasted_iota(jnp.int32, (2 * n, total), 1)
    half_rows = total // 2
    first_row = (slot_row // 2) % 2 * half_rows + slot_row // 4 * rows
    even = slot_row % 2 == 0
    outer = jnp.where(even, first_row, first_row + 2)
    whose = lax.broadcasted_iota(jnp.int32, (2 * n, n), 1) == lax.broadcasted_iota(jnp.int32, (2 * n, n), 0) // 2
    whose = jnp.where(whose, 1.0, 0.0).astype(bf16)
    even_row = lax.broadcasted_iota(jnp.int32, (2 * n, 128), 0) % 2 == 0
    flag = jnp.where(
        even_row, matmul(whose, flag0[...].astype(bf16)), matmul(whose, flag2[...].astype(bf16))
    )
    flag = jnp.where(lax.broadcasted_iota(jnp.int32, flag.shape, 1) == me, flag, 0.0)
    flag = jnp.sum(flag, axis=1, keepdims=True)
    source_row = jnp.where(flag > 0.5, outer, first_row + 1)
    select = jnp.where(slot_lane == source_row, 1.0, 0.0).astype(bf16)

    arrived_all(2, land_h, n // 2)
    for chip in range(n // 2):
        h_all[chip * rows : (chip + 1) * rows] = land_h[chip].astype(f32)
    need(loads.out_proj)
    mates[0].wait_recv()
    resid_f = [jnp.zeros((n * 2, col_width), f32)] * 2
    for part in range(2):
        for step in range(1, n, 2):
            chip = flipped(step) // 2
            block = land3.at[part, chip]
            sem = half_sem.at[step // 2] if part else ring_sem.at[0, step - 1]
            remote(block, block, send_sem.at[0], sem, partner).wait_recv()
            piece = block[...].astype(f32)
            wide = piece.shape[1]
            rest = wide // rows
            tile, low = step // 4, 4 * (step // 2 % 2)
            g_all[part, tile, low : low + rows, :wide] = piece[0:rows]
            for row in range(rows):
                g_all[part, tile, low + row : low + row + 1, wide:] = piece[rows : rows + 1, row * rest : (row + 1) * rest]
        g_low[...] = g_all[part].reshape(g_low.shape).astype(bf16)
        at = slice(part * half_inner, (part + 1) * half_inner)
        resid_f = [
            resid_f[0] + matmul(g_low[...], vm.out_proj[at]),
            resid_f[1] + matmul(g_low[...], mate_proj[at]),
        ]
    need(loads.shared_gate, loads.shared_up, loads.ffn_gain)
    for which, place in enumerate((core, 1 - core)):
        for step in range(1, n, 2):
            by_chip[which, flipped(step) // 2] = resid_f[which][2 * step - 2 : 2 * step + 2]
        for chip in range(n // 2):
            part48[which, chip * rows : (chip + 1) * rows] = by_chip[which, chip, 0:rows]
    swap = lambda left, right: jnp.where(core == 0, jnp.concatenate([left, right], axis=1), jnp.concatenate([right, left], axis=1))
    resid_part = (swap(part48[0], part48[1]) + h_all[...]).astype(bf16)
    src4[...] = resid_part
    land4[me] = resid_part
    rows4 = spread(0, 1, src4, land4)
    gain_part = vm.ffn_gain[:, pl.ds(pl.multiple_of(me // 2 * duo, duo), duo)]
    shared_part = (resid_part.astype(f32) * gain_part).astype(bf16)
    mates[1].wait_recv()
    mates[2].wait_recv()
    lower, upper = shared_part[:, :col_width], shared_part[:, col_width:]
    mine = jnp.where(core == 0, lower.astype(f32), upper.astype(f32)).astype(bf16)
    other = jnp.where(core == 0, upper.astype(f32), lower.astype(f32)).astype(bf16)
    slots[:, :shared_units] = matmul(mine, vm.shared_gate[...]) + matmul(other, mate_gate[...])
    slots[:, shared_units:] = matmul(mine, vm.shared_up[...]) + matmul(other, mate_up[...])
    for chip in range(n // 2):
        src5[chip] = folded(slots[chip * rows : (chip + 1) * rows], fold5.at[chip])
    across(1, lambda to: src5.at[to // 2], land5.at[me // 2], land5, lambda step: whole_sem.at[0])

    need(loads.expert_gate, loads.expert_up, loads.expert_down)
    acc_gate[...] = jnp.zeros_like(acc_gate)
    acc_up[...] = jnp.zeros_like(acc_up)
    squares = [jnp.zeros((total, duo), f32)]

    def chip_rows(chip):
        return jnp.concatenate([land4[2 * chip + 1].astype(f32), land4[2 * chip].astype(f32)], axis=0)

    def add_chip(owner, kind):
        chip = owner // 2
        piece = chip_rows(chip)
        squares[0] = squares[0] + piece * piece
        at = pl.ds(pl.multiple_of(chip * duo, duo), duo)
        scaled = (piece * vm.ffn_gain[:, at]).astype(bf16)
        acc_gate[...] += matmul(scaled, vm.expert_gate[at])
        acc_up[...] += matmul(scaled, vm.expert_up[at])

    finish(collect(0, 1, land4, rows4, lambda owner, kind: None), add_chip)
    scale_all = lax.rsqrt(jnp.sum(squares[0], axis=1, keepdims=True) / width + epsilon)
    hidden_units = (silu(acc_gate[...] * scale_all) * (acc_up[...] * scale_all)).astype(bf16)
    served = matmul(select, hidden_units).astype(bf16)
    half_width = width // 2
    for part in range(2):
        served_f[...] = matmul(served, vm.expert_down[:, part * half_width : (part + 1) * half_width])
        for place in range(n):
            src6[part, place] = served_f[2 * place : 2 * place + 2].astype(bf16)
        scatter(2 + part, src6.at[part], land6.at[part], part_sem.at[me // span_z] if part else whole_sem.at[1])
        land6[part, me] = src6[part, me]

    need(loads.router_t, loads.shared_down)
    own_row = lax.broadcasted_iota(jnp.int32, (rows, total), 0) + core * half_rows + me // 2 * rows
    pick = jnp.where(lax.broadcasted_iota(jnp.int32, (rows, total), 1) == own_row, 1.0, 0.0).astype(bf16)
    for chip in range(n // 2):
        y_all[:, chip * duo : (chip + 1) * duo] = matmul(pick, chip_rows(chip).astype(bf16))
    resid_own = y_all[:, :width]
    norm_scale = lax.rsqrt(jnp.mean(resid_own * resid_own, axis=-1, keepdims=True) + epsilon)
    routed_own = (resid_own * norm_scale * vm.ffn_gain[...]).astype(bf16)
    scores = 1.0 / (1.0 + jnp.exp(-dot_t(routed_own, vm.router_t[...])))
    kept = chosen[:, :n]
    scores = jnp.where(kept > 0.5, scores, 0.0)
    weights = routed_scale * scores / jnp.sum(scores, axis=1, keepdims=True)
    outer_w = jnp.concatenate([weights[0:1], weights[2:3]], axis=0)
    middle = weights[1:2]
    inner_w = jnp.concatenate([middle * (1.0 - kept[0:1]), middle * kept[0:1]], axis=0)
    shared = jnp.zeros(fold5.shape[1:], f32)
    arrived_all(0, land5, n // 2)
    for chip in range(n // 2):
        shared = shared + land5[chip].astype(f32)
    wide = shared.shape[1]
    rest = wide // rows
    cols[:, :wide] = shared[0:rows]
    for row in range(rows):
        cols[row : row + 1, wide : wide + rest] = shared[rows : rows + 1, row * rest : (row + 1) * rest]
    shared = cols[:, : wide + rest] * norm_scale
    shared_hidden = (silu(shared[:, :shared_units]) * shared[:, shared_units:]).astype(bf16)
    start = resid_own + matmul(shared_hidden, vm.shared_down[...])
    y_all[:, :width] = start
    for part in range(2):
        ends = jnp.zeros((2, half_width), f32)
        mid = jnp.zeros((2, half_width), f32)
        if part == 0:
            arrived_all(1, land6.at[0])
        for place in range(n):
            if part and place % span_z == 0:
                arrived(land6.at[1], place)
            piece = land6[part, place].astype(f32)
            ends = ends + piece * outer_w[:, place : place + 1]
            mid = mid + piece * inner_w[:, place : place + 1]
        at = slice(part * half_width, (part + 1) * half_width)
        xv[0:1, at] = ends[0:1]
        xv[1:2, at] = mid[0:1] + mid[1:2]
        xv[2:3, at] = ends[1:2]
    layer_out[...] = (y_all[:, :width] + xv[:, :width]).astype(bf16)
    for phase in tuple(blocks):
        drained(phase)
    for one in mates:
        one.wait_send()


def store_kernel(layer_out, next_state, next_window, layer_hbm, state_hbm, window_hbm, sems):
    for at in range(next_state.shape[0]):
        pltpu.make_async_copy(next_state.at[at], state_hbm.at[at], sems.at[0]).start()
    small = [
        pltpu.make_async_copy(layer_out, layer_hbm, sems.at[1]),
        pltpu.make_async_copy(next_window, window_hbm, sems.at[2]),
    ]
    for one in small:
        one.start()
    for one in small:
        one.wait()
    pltpu.make_async_copy(next_state, state_hbm, sems.at[0]).wait()


def one_kernel(*args):
    named = Args(*args)
    n = lax.axis_size("ep")
    rows, width = named.hidden.shape
    inner = named.gate_proj.shape[1] * n
    total = n * rows
    heads = named.step_bias.shape[0]
    flat = lambda one: one.reshape(1, -1)
    named = named._replace(
        write_t=named.write_t.T,
        read_t=named.read_t.T,
        step_t=named.step_t.T,
        router_t=named.router_t.T,
        step_bias=flat(named.step_bias),
        decay_log=flat(named.decay_log),
        skip_scale=flat(named.skip_scale),
        conv_bias=flat(named.conv_bias),
        mix_gain=flat(named.mix_gain),
        group_gain=flat(named.group_gain),
        ffn_gain=flat(named.ffn_gain),
        expert_gate=named.expert_gate[0],
        expert_up=named.expert_up[0],
        expert_down=named.expert_down[0],
    )
    state_shape = named.ssm_state.shape
    span = inner // GROUPS
    named = named._replace(ssm_state=named.ssm_state.reshape(rows * GROUPS, span, STATE))
    conv_dim = named.conv_bias.shape[1]
    cols = 2 * named.gate_proj.shape[1] + 2 * named.write_t.shape[0]
    gate_cols = named.gate_proj.shape[1]
    col_width = named.out_proj.shape[1]
    shared_units = named.shared_gate.shape[1]
    bf16, f32 = jnp.bfloat16, jnp.float32
    V = pltpu.VMEM
    scratch = [V(one.shape, one.dtype) for one in named]
    units = 2 * shared_units
    scratch += [
        V((4, width * 3 // 4), bf16), V((n, 4, width * 3 // 4), bf16),
        V((n, 4, cols - gate_cols), bf16), V((n, 4, cols - gate_cols), bf16),
        V((n, 4, gate_cols), bf16), V((n, 4, gate_cols), bf16),
        V((2, 4, inner * 3 // 8), bf16), V((2, n // 2, 4, inner * 3 // 8), bf16),
        V((total // 2, 2 * col_width), bf16), V((n, total // 2, 2 * col_width), bf16),
        V((n // 2, 4, units * 3 // 4), bf16), V((n // 2, 4, units * 3 // 4), bf16),
        V((2, n, 2, width // 2), bf16), V((2, n, 2, width // 2), bf16),
        V((4, width * 3 // 4), f32), V((4, inner * 3 // 8), f32), V((n // 2, 4, units * 3 // 4), f32),
        V((n // 2, 8, width), f32), V((n * 4, width), bf16), V((n * 4, cols - gate_cols), f32),
        V((n * 4, gate_cols), f32),
        V((2, n // 4, 8, inner // 2), f32), V((n * 2, inner // 2), bf16), V((total // 2, 2 * col_width), f32),
        V((n, 128), f32), V((n, 128), f32), V((2, total // 2, col_width), f32),
        V((total, shared_units), f32), V((total, shared_units), f32),
        V((rows, conv_dim), f32), V((rows, inner), f32), V((rows, inner), f32), V((rows, conv_dim), f32),
        V((rows, inner), f32), V((GROUPS, rows, STATE), f32), V((GROUPS, rows, STATE), f32),
        V((rows, inner), f32), V((1, inner), f32),
        V((rows * GROUPS, heads // GROUPS, 128), f32), V((rows * GROUPS, STATE, span), bf16),
        V((rows, 3, conv_dim), f32), V((total // 2, units), f32), V((2 * n, width // 2), f32),
        V((width, cols - 2 * gate_cols), bf16),
        V((n // 2, rows, 2 * col_width), bf16), V((n // 2, rows, 2 * col_width), bf16),
        V(named.out_proj.shape, bf16), V(named.shared_gate.shape, bf16), V(named.shared_up.shape, bf16),
        pltpu.SemaphoreType.DMA((16,)),
        pltpu.SemaphoreType.DMA((7,)),
        pltpu.SemaphoreType.DMA((2, n - 1)),
        pltpu.SemaphoreType.DMA((max(1, n // 4),)),
        pltpu.SemaphoreType.DMA((3,)),
        pltpu.SemaphoreType.DMA((6,)),
        pltpu.SemaphoreType.DMA((n // 2,)),
        V((2, n // 2, 4, col_width), f32),
    ]
    layer_out, next_state, next_window = pl.pallas_call(
        functools.partial(layer_kernel, n, rows),
        out_shape=(
            pltpu.VMEM((rows, width), bf16),
            pltpu.VMEM(named.ssm_state.shape, f32),
            pltpu.VMEM(named.conv_window.shape, bf16),
        ),
        in_specs=[pl.BlockSpec(memory_space=pltpu.HBM)] * len(named),
        out_specs=tuple(pl.BlockSpec(memory_space=pltpu.VMEM) for _ in range(3)),
        scratch_shapes=scratch,
        compiler_params=pltpu.CompilerParams(
            collective_id=0, has_side_effects=True, vmem_limit_bytes=36 * 1024 * 1024
        ),
    )(*[pltpu.with_memory_space_constraint(one, pltpu.HBM) for one in named])
    outs = (layer_out, next_state, next_window)
    layer_out, next_state, next_window = pl.pallas_call(
        store_kernel,
        out_shape=tuple(jax.ShapeDtypeStruct(one.shape, one.dtype) for one in outs),
        in_specs=[pl.BlockSpec(memory_space=pltpu.VMEM)] * 3,
        out_specs=tuple(pl.BlockSpec(memory_space=pltpu.HBM) for _ in range(3)),
        scratch_shapes=[pltpu.SemaphoreType.DMA((3,))],
        compiler_params=pltpu.CompilerParams(vmem_limit_bytes=1024 * 1024),
    )(*outs)
    return layer_out, next_state.reshape(state_shape), next_window


def fits(args):
    named = Args(*args)
    n = lax.axis_size("ep")
    return (
        named.hidden.shape[0] == 3
        and n & (n - 1) == 0
        and 2 <= n <= 128
        and named.hidden.shape[1] % 512 == 0
        and named.gate_proj.shape[1] == 256
        and named.gate_proj.shape[0] * 2 == named.group_gain.shape[0]
        and named.expert_gate.shape[2] == named.shared_gate.shape[1]
        and named.shared_gate.shape[1] % 256 == 0
        and named.hidden.shape[1] <= named.group_gain.shape[0]
        and named.out_proj.shape[1] == 128
        and named.gate_proj.shape[1] % 128 == 0
        and named.write_t.shape[1] == 64
        and named.expert_gate.shape[0] == 1
        and named.router_t.shape[1] == n
        and HEAD_DIM * 2 == 128
    )


def body(*args):
    return one_kernel(*args) if fits(args) else shards(*args)


def solution(mesh):
    placed = (
        P(("grp", "ep"), None),
        P(("grp", "ep"), None, None),
        P(("grp", "ep"), None, None, None),
        P(None, "ep"),
        P(None, "ep"),
        P(None, "ep"),
        P(None, "ep"),
        P(),
        P(),
        P(),
        P(("grp", "ep"), None),
        P(),
        P(),
        P(),
        P(),
        P(),
        P(None, "ep"),
        P(),
        P(),
        P(("grp", "ep"), None),
        P("ep", None, None),
        P("ep", None, None),
        P("ep", None, None),
        P("ep", None),
        P("ep", None),
        P(),
    )
    return jax.shard_map(
        body,
        mesh=mesh,
        in_specs=placed,
        out_specs=(
            P(("grp", "ep"), None),
            P(("grp", "ep"), None, None, None),
            P(("grp", "ep"), None, None),
        ),
        check_vma=False,
    )
```
